128 devices in a mesh: sp: 32 (over z, y, core), tp: 4 (over x).
Axes of the slice: x: 4, y: 4, z: 4, core: 2. Of those that a mesh axis runs over, the one named last changes fastest.
Arguments:
- residual: bfloat16 [8192, 2048], P(('sp', 'tp')), may hold values from -6 to 6
- ssm_input: bfloat16 [8192, 2048], P('sp', 'tp'), may hold values from -6 to 6
- pole_real: float32 [128, 64], P('tp'), may hold values from -2 to 0
- pole_imaginary: float32 [128, 64], P('tp'), may hold values from 1 to 100
- step_log: float32 [128], P('tp'), may hold values from -8 to 0
- input_real: float32 [128, 64, 16], P('tp'), may hold values from -1 to 1
- entry_map_quadrature: float32 [128, 64, 16], P('tp'), may hold values from -1 to 1
- output_real: float32 [128, 16, 64], P('tp'), may hold values from -0.5 to 0.5
- output_imaginary: float32 [128, 16, 64], P('tp'), may hold values from -0.5 to 0.5
- added_log_decay: float32 [8192, 128], P('sp', 'tp'), may hold values from -2 to 0
- out_weight: bfloat16 [2048, 2048], P('tp'), may hold values from -0.125 to 0.125
- mix_gain: float32 [2048], replicated, may hold values from 0.1 to 1.9
- gate_weight: bfloat16 [2048, 5632], P('sp', 'tp'), may hold values from -0.125 to 0.125
- up_weight: bfloat16 [2048, 5632], P('sp', 'tp'), may hold values from -0.125 to 0.125
- down_weight: bfloat16 [2048, 5632], P('sp', 'tp'), may hold values from -0.078125 to 0.078125
- pre_gain: float32 [2048], replicated, may hold values from 0.1 to 1.9
- post_gain: float32 [2048], replicated, may hold values from 0.1 to 1.9
Outputs:
- merged: bfloat16 [8192, 2048], P(('sp', 'tp'))
The draws below stay inside these ranges and needn't reach their ends.
All inputs are finite; a program needn't handle non-finite values.
Results may differ from the reference program's by a relative error of at most 0.017.
Values may be sent and summed in bfloat16 or wider, within the bound.
A program may use at most 128 MiB of HBM per device.

```python
import math
import jax
import jax.numpy as jnp
from jax import lax

D = 2048
FF = 5632
SSM_WIDTH = 2048
GROUP_CH = 16
STATE = 64
TOK_DEV = 256
CHANNEL_BUNDLES = 128
SEQUENCE_ITEMS = 8192


def frequency_lookup(key):
    base = jax.random.fold_in(key, 11)
    pick_key, slow_key, quick_random_seed, spread_key = jax.random.split(base, 4)
    slow_count = 5
    slow_flag = jax.random.randint(pick_key, (CHANNEL_BUNDLES,), 0, 10) < slow_count
    slow_rate = jnp.exp(jax.random.uniform(slow_key, (CHANNEL_BUNDLES,), jnp.float32, math.log(0.05), math.log(0.5))) / SEQUENCE_ITEMS
    fast_rate = jnp.exp(jax.random.uniform(quick_random_seed, (CHANNEL_BUNDLES,), jnp.float32, math.log(8.0), math.log(16.0))) / TOK_DEV
    rate = jnp.where(slow_flag, slow_rate, fast_rate)
    dispersion = jnp.exp(jax.random.uniform(spread_key, (CHANNEL_BUNDLES, STATE), jnp.float32, -0.3, 0.3))
    return (rate, dispersion)


def draw_pole_real(key, part):
    rate, dispersion = frequency_lookup(key)
    return -jnp.sqrt(rate)[:, None] * dispersion


def draw_step_log(key, part):
    rate, dispersion = frequency_lookup(key)
    return 0.5 * jnp.log(rate)


def draw_added_log_decay(key, part):
    base = jax.random.fold_in(key, 23)
    level_key, where_key, damping_random_seed = jax.random.split(base, 3)
    block_count = SEQUENCE_ITEMS // TOK_DEV
    level = jax.random.uniform(level_key, (block_count, CHANNEL_BUNDLES), jnp.float32, 0.0, 0.4) / SEQUENCE_ITEMS
    baseline_constant = jnp.repeat(level, TOK_DEV, axis=0)
    locations = jax.random.randint(where_key, (2, CHANNEL_BUNDLES), 0, SEQUENCE_ITEMS)
    damping_charges = jax.random.uniform(damping_random_seed, (2, CHANNEL_BUNDLES), jnp.float32, 0.2, 0.4)
    impulse_slots = jnp.arange(SEQUENCE_ITEMS)[:, None, None] == locations[None]
    impulse_tallies = jnp.sum(jnp.where(impulse_slots, jnp.log1p(-damping_charges)[None], 0.0), axis=1)
    return impulse_tallies - baseline_constant


def steps_of(rng, extent, shards, low, high):
    level, own = 1.0, jax.random.fold_in(rng, 6)
    for dim, blocks in shards:
        steps = jnp.exp(jax.random.uniform(jax.random.fold_in(own, dim), (blocks,), jnp.float32, low / len(shards), high / len(shards)))
        level = level * jnp.repeat(steps, extent[dim] // blocks).reshape([-1 if axis == dim else 1 for axis in range(len(extent))])
    return level


def normal_values(own_key, dims, scale, limit, cuts=(), held_as=jnp.bfloat16):
    entries = scale * jax.random.normal(own_key, dims, jnp.float32)
    if cuts:
        entries = entries * steps_of(own_key, dims, cuts, -0.22, 0.18)
    return jnp.clip(entries, -limit, limit).astype(held_as)


def setup_inputs(seed: int = 0) -> dict:
    key_of = jax.random.split(jax.random.key(seed), 18)
    residual = normal_values(key_of[0], (SEQUENCE_ITEMS, D), 1.0, 6.0, ((0, 128),))
    ssm_input = normal_values(key_of[1], (SEQUENCE_ITEMS, SSM_WIDTH), 1.0, 6.0, ((0, 32), (1, 4)))
    pole_real = draw_pole_real(jax.random.fold_in(key_of[17], 71), 0)
    pole_imaginary = jnp.clip(1.0 + 99.0 * jax.random.uniform(key_of[3], (CHANNEL_BUNDLES, STATE), jnp.float32) ** steps_of(key_of[3], (CHANNEL_BUNDLES, STATE), ((0, 4),), -0.2, 0.2), 1.0, 100.0)
    step_log = draw_step_log(jax.random.fold_in(key_of[17], 71), 0)
    input_real = normal_values(key_of[5], (CHANNEL_BUNDLES, STATE, GROUP_CH), (2 * GROUP_CH) ** -0.5, 1.0, ((0, 4),), jnp.float32)
    entry_map_quadrature = normal_values(key_of[6], (CHANNEL_BUNDLES, STATE, GROUP_CH), (2 * GROUP_CH) ** -0.5, 1.0, ((0, 4),), jnp.float32)
    output_real = normal_values(key_of[7], (CHANNEL_BUNDLES, GROUP_CH, STATE), (2 * STATE) ** -0.5, 0.5, ((0, 4),), jnp.float32)
    output_imaginary = normal_values(key_of[8], (CHANNEL_BUNDLES, GROUP_CH, STATE), (2 * STATE) ** -0.5, 0.5, ((0, 4),), jnp.float32)
    added_log_decay = draw_added_log_decay(jax.random.fold_in(key_of[17], 71), 0)
    out_weight = normal_values(key_of[10], (SSM_WIDTH, D), SSM_WIDTH ** -0.5, 0.125, ((0, 4),))
    mix_gain = jnp.clip(1.0 + 0.18 * jax.random.normal(key_of[11], (D,), jnp.float32), 0.1, 1.9)
    gate_weight = normal_values(key_of[12], (D, FF), D ** -0.5, 0.125, ((0, 32), (1, 4)))
    up_weight = normal_values(key_of[13], (D, FF), D ** -0.5, 0.125, ((0, 32), (1, 4)))
    down_weight = normal_values(key_of[14], (D, FF), FF ** -0.5, 0.078125, ((0, 32), (1, 4)))
    pre_gain = jnp.clip(1.0 + 0.18 * jax.random.normal(key_of[15], (D,), jnp.float32), 0.1, 1.9)
    post_gain = jnp.clip(1.0 + 0.18 * jax.random.normal(key_of[16], (D,), jnp.float32), 0.1, 1.9)
    return {"residual": residual, "ssm_input": ssm_input, "pole_real": pole_real, "pole_imaginary": pole_imaginary, "step_log": step_log, "input_real": input_real, "entry_map_quadrature": entry_map_quadrature, "output_real": output_real, "output_imaginary": output_imaginary, "added_log_decay": added_log_decay, "out_weight": out_weight, "mix_gain": mix_gain, "gate_weight": gate_weight, "up_weight": up_weight, "down_weight": down_weight, "pre_gain": pre_gain, "post_gain": post_gain}


EXACT = lax.Precision.HIGHEST
EPSILON = 1e-06

def rms_scale(values, gain):
    return values * lax.rsqrt(lax.optimization_barrier(jnp.mean(values * values, axis=-1, keepdims=True)) + EPSILON) * gain

def round_half(values):
    return lax.optimization_barrier(values.astype(jnp.bfloat16))

def chain_link(earlier, later):
    decay_real, decay_imaginary, state_real, state_imaginary = earlier
    next_real, next_imaginary, drive_real, drive_imaginary = later
    return (next_real * decay_real - next_imaginary * decay_imaginary, next_real * decay_imaginary + next_imaginary * decay_real, next_real * state_real - next_imaginary * state_imaginary + drive_real, next_real * state_imaginary + next_imaginary * state_real + drive_imaginary)

def local_states(inputs, pole_real, pole_imaginary, step_log, input_real, entry_map_quadrature, added_log_decay):
    row_count = inputs.shape[0]
    groups, hidden_states = pole_real.shape
    width = input_real.shape[2]
    step_size = jnp.exp(step_log)[:, None]
    log_size = pole_real * step_size
    angle = pole_imaginary * step_size
    cosine = jnp.cos(angle)
    sine = jnp.sin(angle)
    lift_real = jnp.expm1(log_size) * cosine - 2.0 * jnp.sin(0.5 * angle) ** 2
    lift_imaginary = jnp.exp(log_size) * sine
    denominator = pole_real * pole_real + pole_imaginary * pole_imaginary
    ratio_real = (lift_real * pole_real + lift_imaginary * pole_imaginary) / denominator
    ratio_imaginary = (lift_imaginary * pole_real - lift_real * pole_imaginary) / denominator
    bar_real = ratio_real[..., None] * input_real - ratio_imaginary[..., None] * entry_map_quadrature
    bar_imaginary = ratio_real[..., None] * entry_map_quadrature + ratio_imaginary[..., None] * input_real
    grouped = inputs.astype(jnp.float32).reshape(row_count, groups, width)
    drive_real = jnp.einsum('gnc,tgc->tgn', bar_real, grouped, precision=EXACT).reshape(row_count, groups * hidden_states)
    drive_imaginary = jnp.einsum('gnc,tgc->tgn', bar_imaginary, grouped, precision=EXACT).reshape(row_count, groups * hidden_states)
    pole_magnitude = jnp.exp(log_size[None] + added_log_decay[:, :, None])
    decay_real = (pole_magnitude * cosine[None]).reshape(row_count, groups * hidden_states)
    decay_imaginary = (pole_magnitude * sine[None]).reshape(row_count, groups * hidden_states)
    return lax.associative_scan(chain_link, (decay_real, decay_imaginary, drive_real, drive_imaginary), axis=0)

def apply_carry(scanned, carry_real, carry_imaginary):
    product_real, product_imaginary, state_real, state_imaginary = scanned
    return (state_real + product_real * carry_real - product_imaginary * carry_imaginary, state_imaginary + product_real * carry_imaginary + product_imaginary * carry_real)

def readout(state_real, state_imaginary, output_real, output_imaginary):
    groups, width, hidden_states = output_real.shape
    row_count = state_real.shape[0]
    real_part = jnp.einsum('gcn,tgn->tgc', output_real, state_real.reshape(row_count, groups, hidden_states), precision=EXACT)
    other_part = jnp.einsum('gcn,tgn->tgc', output_imaginary, state_imaginary.reshape(row_count, groups, hidden_states), precision=EXACT)
    return jax.nn.gelu((real_part - other_part).reshape(row_count, groups * width)).astype(jnp.bfloat16)

def reference(residual, ssm_input, pole_real, pole_imaginary, step_log, input_real, entry_map_quadrature, output_real, output_imaginary, added_log_decay, out_weight, mix_gain, gate_weight, up_weight, down_weight, pre_gain, post_gain):
    block_count = SEQUENCE_ITEMS // TOK_DEV

    def per_block(carry, inputs):
        rows_residual, rows_input, rows_extra = inputs
        scanned = local_states(rows_input, pole_real, pole_imaginary, step_log, input_real, entry_map_quadrature, rows_extra)
        state_real, state_imaginary = apply_carry(scanned, carry[0], carry[1])
        activated = readout(state_real, state_imaginary, output_real, output_imaginary)
        mixed = jnp.dot(activated, out_weight, preferred_element_type=jnp.float32)
        middle = round_half(rows_residual.astype(jnp.float32) + rms_scale(mixed, mix_gain))
        mixer_input = rms_scale(middle.astype(jnp.float32), pre_gain).astype(jnp.bfloat16)
        gate_act = jnp.dot(mixer_input, gate_weight, preferred_element_type=jnp.float32)
        up_act = jnp.dot(mixer_input, up_weight, preferred_element_type=jnp.float32)
        hidden = (jax.nn.silu(gate_act) * up_act).astype(jnp.bfloat16)
        mixer_out = lax.dot_general(hidden, down_weight, (((1,), (1,)), ((), ())), preferred_element_type=jnp.float32)
        merged = (middle.astype(jnp.float32) + 0.5 * rms_scale(mixer_out, post_gain)).astype(jnp.bfloat16)
        return ((state_real[-1], state_imaginary[-1]), merged)
    flat_width = pole_real.shape[0] * pole_real.shape[1]
    initial = (jnp.zeros((flat_width,), jnp.float32), jnp.zeros((flat_width,), jnp.float32))
    _, outputs = lax.scan(per_block, initial, (residual.reshape(block_count, TOK_DEV, D), ssm_input.reshape(block_count, TOK_DEV, SSM_WIDTH), added_log_decay.reshape(block_count, TOK_DEV, CHANNEL_BUNDLES)))
    return outputs.reshape(SEQUENCE_ITEMS, D)
```

```python
import functools

import jax
import jax.numpy as jnp
from jax import lax
from jax.experimental import pallas as pl
from jax.experimental.pallas import tpu as pltpu
from jax.sharding import PartitionSpec as P

EPSILON = 1e-06
EXACT = lax.Precision.HIGHEST
MESH = pl.DeviceIdType.MESH
F32 = jnp.float32
BF16 = jnp.bfloat16
T = 256
G = 32
N = 64
C = 16
GN = G * N
SEGS = 8
STEPS = T // SEGS


def dot(a, b, **kw):
    return jnp.dot(a, b, preferred_element_type=F32, **kw)


def dot_nt(a, b):
    return lax.dot_general(a, b, (((1,), (1,)), ((), ())), preferred_element_type=F32)


def iota(shape, dim):
    return lax.broadcasted_iota(jnp.int32, shape, dim)


def one_hot(mask, dtype):
    return jnp.where(mask, 1.0, 0.0).astype(dtype)


def cmul(ar, ai, br, bi):
    return ar * br - ai * bi, ar * bi + ai * br


def split(v):
    hi = v.astype(BF16)
    return hi, (v - hi.astype(F32)).astype(BF16)


def expm1(x):
    p = 1.0 / 40320.0
    for k in (5040.0, 720.0, 120.0, 24.0, 6.0, 2.0, 1.0):
        p = p * x + 1.0 / k
    return jnp.where(x > -0.5, p * x, jnp.exp(x) - 1.0)


def step_rows(pr_ref, pi_ref, sl_ref):
    tile = one_hot(iota((N, GN), 1) % N == iota((N, GN), 0), F32)
    mine = iota((G, GN), 1) // N == iota((G, GN), 0)
    groups = one_hot(mine, F32)

    def row(ref):
        wide = dot(ref[...], tile, precision=EXACT)
        return jnp.sum(jnp.where(mine, wide, 0.0), axis=0, keepdims=True)

    pr, pi = row(pr_ref), row(pi_ref)
    sl = dot(jnp.broadcast_to(sl_ref[...], (8, G)), groups, precision=EXACT)[0:1]
    step = jnp.exp(sl)
    log_size = pr * step
    angle = pi * step
    cosine, sine = jnp.cos(angle), jnp.sin(angle)
    size = jnp.exp(log_size)
    half = jnp.sin(0.5 * angle)
    lift_r = expm1(log_size) * cosine - 2.0 * half * half
    lift_i = size * sine
    inv = 1.0 / (pr * pr + pi * pi)
    ratio_r = (lift_r * pr + lift_i * pi) * inv
    ratio_i = (lift_i * pr - lift_r * pi) * inv
    return size * cosine, size * sine, ratio_r, ratio_i, groups


def scan_pass(base, e_ref, dr_ref, di_ref, init, store):
    ends = []
    width = GN // 4
    for lc in range(4):
        sl = slice(lc * width, (lc + 1) * width)
        br = jnp.broadcast_to(base[0][:, sl], (SEGS, width))
        bi = jnp.broadcast_to(base[1][:, sl], (SEGS, width))

        def body(i, st):
            sr, si, pe = st
            rows = pl.ds(pl.multiple_of(i * SEGS, SEGS), SEGS)
            e = e_ref[rows, sl]
            ar, ai = br * e, bi * e
            nr = ar * sr - ai * si + dr_ref[rows, sl]
            ni = ar * si + ai * sr + di_ref[rows, sl]
            if store:
                dr_ref[rows, sl] = nr
                di_ref[rows, sl] = ni
                return nr, ni, pe
            return nr, ni, pe * e

        st = (init[0][:, sl], init[1][:, sl], jnp.ones((SEGS, width), F32))
        ends.append(lax.fori_loop(0, STEPS, body, st, unroll=4))
    return [jnp.concatenate([p[k] for p in ends], axis=1) for k in range(3)]


def put_row(ref, slot, part, row):
    for k in range(16):
        ref[slot, part * 16 + k : part * 16 + k + 1, :] = row[:, k * 128 : (k + 1) * 128]


def to_row(block):
    return jnp.concatenate([block[k : k + 1, :] for k in range(16)], axis=1)


def parts_of(ref, slot):
    block = ref[slot]
    return [block[16 * k : 16 * (k + 1), :] for k in range(4)]


def link(first, then):
    ar, ai, sr, si = first
    br, bi, tr, ti = then
    pr, pi = cmul(br, bi, ar, ai)
    ur, ui = cmul(br, bi, sr, si)
    return pr, pi, ur + tr, ui + ti


def choose(cond, a, b):
    return tuple(jnp.where(cond, x, y) for x, y in zip(a, b))


def front_kernel(
    u_ref, a_ref, pr_ref, pi_ref, sl_ref, bre_ref, bim_ref, cre_ref, cim_ref, wo_ref,
    out_ref,
    e_ref, dr_ref, di_ref, act_ref, ra_ref, rb_ref, sa, qa, sb, qb,
):
    sp = lax.axis_index("sp")
    q = sp % 8
    z = sp // 8
    peers_a = [z * 8 + (q + d) % 8 for d in range(1, 8)]
    peers_b = [((z + d) % 4) * 8 + q for d in range(1, 4)]
    barrier = pltpu.get_barrier_semaphore()
    for peer in peers_a + peers_b:
        pl.semaphore_signal(barrier, inc=1, device_id={"sp": peer}, device_id_type=MESH)

    base_r, base_i, ratio_r, ratio_i, groups = step_rows(pr_ref, pi_ref, sl_ref)
    perm = iota((T, T), 1) == (iota((T, T), 0) % SEGS) * STEPS + iota((T, T), 0) // SEGS
    e_small = dot(one_hot(perm, F32), jnp.exp(a_ref[...]), precision=EXACT)
    e_ref[...] = dot(e_small, groups, precision=EXACT)
    u = dot(one_hot(perm, BF16), u_ref[...]).astype(BF16)
    spread = one_hot(iota((C, 256), 1) % C == iota((C, 256), 0), BF16)
    own_b = iota((1024, 256), 0) // N == iota((1024, 256), 1) // C
    for h in range(2):
        gn = slice(h * 1024, (h + 1) * 1024)
        uh = u[:, h * 256 : (h + 1) * 256]
        raw = []
        for ref in (bre_ref, bim_ref):
            acc = None
            for piece in split(ref[gn, :]):
                wide = jnp.where(own_b, dot(piece, spread), 0.0).astype(BF16)
                term = dot_nt(uh, wide)
                acc = term if acc is None else acc + term
            raw.append(acc)
        rr, ri = ratio_r[:, gn], ratio_i[:, gn]
        dr_ref[:, gn] = rr * raw[0] - ri * raw[1]
        di_ref[:, gn] = rr * raw[1] + ri * raw[0]

    zero = jnp.zeros((SEGS, GN), F32)
    end_r, end_i, pe = scan_pass((base_r, base_i), e_ref, dr_ref, di_ref, (zero, zero), False)
    wr, wi = base_r, base_i
    for _ in range(5):
        wr, wi = cmul(wr, wi, wr, wi)
    seg_r, seg_i = wr * pe, wi * pe
    one_row = jnp.ones((1, GN), F32)
    no_row = jnp.zeros((1, GN), F32)
    total = (one_row, no_row, no_row, no_row)
    before = []
    for j in range(SEGS):
        before.append(total)
        total = link(total, (seg_r[j : j + 1], seg_i[j : j + 1], end_r[j : j + 1], end_i[j : j + 1]))
    for k in range(4):
        put_row(ra_ref, 0, k, total[k])

    pl.semaphore_wait(barrier, 10)
    copies = []
    for d in range(1, 8):
        copies.append(pltpu.make_async_remote_copy(
            ra_ref.at[0], ra_ref.at[d], sa.at[d], qa.at[d],
            device_id={"sp": peers_a[d - 1]}, device_id_type=MESH))
        copies[-1].start()
    for copy in copies:
        copy.wait()
    unit = jnp.ones((16, 128), F32)
    null = jnp.zeros((16, 128), F32)
    run = (unit, null, null, null)
    pre_a = run
    for k in range(8):
        pre_a = choose(q == k, run, pre_a)
        run = link(run, parts_of(ra_ref, (q - k + 8) % 8))
    for k in range(4):
        rb_ref[0, 16 * k : 16 * (k + 1), :] = run[k]
    copies = []
    for d in range(1, 4):
        copies.append(pltpu.make_async_remote_copy(
            rb_ref.at[0], rb_ref.at[d], sb.at[d], qb.at[d],
            device_id={"sp": peers_b[d - 1]}, device_id_type=MESH))
        copies[-1].start()
    for copy in copies:
        copy.wait()
    run = (unit, null, null, null)
    pre_b = run
    for k in range(4):
        pre_b = choose(z == k, run, pre_b)
        run = link(run, parts_of(rb_ref, (z - k + 4) % 4))
    carry = link(pre_b, pre_a)
    cr, ci = to_row(carry[2]), to_row(carry[3])
    starts = []
    for k in range(SEGS):
        pr, pi, sr, si = before[k]
        tr, ti = cmul(pr, pi, cr, ci)
        starts.append((tr + sr, ti + si))
    init = [jnp.concatenate([s[k] for s in starts], axis=0) for k in range(2)]
    scan_pass((base_r, base_i), e_ref, dr_ref, di_ref, init, True)

    lay = one_hot(iota((N, 1024), 1) % N == iota((N, 1024), 0), BF16)
    own_c = iota((256, 1024), 0) // C == iota((256, 1024), 1) // N
    for h in range(2):
        gn = slice(h * 1024, (h + 1) * 1024)
        ch = slice(h * 256, (h + 1) * 256)
        y = None
        for s_ref, c_ref, sign in ((dr_ref, cre_ref, 1.0), (di_ref, cim_ref, -1.0)):
            s_hi, s_lo = split(s_ref[:, gn])
            c_hi, c_lo = (
                jnp.where(own_c, dot(piece, lay), 0.0).astype(BF16)
                for piece in split(sign * c_ref[ch, :])
            )
            term = dot_nt(s_hi, c_hi) + dot_nt(s_lo, c_hi) + dot_nt(s_hi, c_lo)
            y = term if y is None else y + term
        act_ref[:, ch] = jax.nn.gelu(y).astype(BF16)
    back = iota((T, T), 0) == (iota((T, T), 1) % SEGS) * STEPS + iota((T, T), 1) // SEGS
    act = dot(one_hot(back, BF16), act_ref[...]).astype(BF16)
    out_ref[...] = dot(act, wo_ref[...]).astype(BF16)


def front(u, a, pr, pi, sl, bre, bim, cre, cim, wo):
    vmem = pl.BlockSpec(memory_space=pltpu.VMEM)
    return pl.pallas_call(
        front_kernel,
        out_shape=jax.ShapeDtypeStruct((T, wo.shape[1]), BF16),
        in_specs=[vmem] * 10,
        out_specs=vmem,
        scratch_shapes=[
            pltpu.VMEM((T, GN), F32),
            pltpu.VMEM((T, GN), F32),
            pltpu.VMEM((T, GN), F32),
            pltpu.VMEM((T, 512), BF16),
            pltpu.VMEM((8, 64, 128), F32),
            pltpu.VMEM((4, 64, 128), F32),
            pltpu.SemaphoreType.DMA((8,)),
            pltpu.SemaphoreType.DMA((8,)),
            pltpu.SemaphoreType.DMA((4,)),
            pltpu.SemaphoreType.DMA((4,)),
        ],
        compiler_params=pltpu.CompilerParams(
            collective_id=0, has_side_effects=True, vmem_limit_bytes=56 * 1024 * 1024
        ),
        name="front",
    )(
        u, a, pr, pi, sl.reshape(1, G), bre.reshape(GN, C), bim.reshape(GN, C),
        cre.reshape(512, N), cim.reshape(512, N), wo,
    )


def from_everyone(shard, axis):
    copies = jnp.broadcast_to(shard, (lax.axis_size(axis), *shard.shape))
    return lax.all_to_all(copies, axis, split_axis=0, concat_axis=0, tiled=True)


def summed_on_arrival(shard, axis):
    count = lax.axis_size(axis)
    blocks = shard.reshape(count, -1, shard.shape[1])
    arrived = lax.all_to_all(blocks, axis, split_axis=0, concat_axis=0, tiled=True)
    return arrived.astype(F32).sum(axis=0)


def rms_scale(values, gain):
    return values * lax.rsqrt(jnp.mean(values * values, axis=-1, keepdims=True) + EPSILON) * gain


def round_half(values):
    return lax.optimization_barrier(values.astype(BF16))


def shards(
    residual, ssm_input, pole_real, pole_imaginary, step_log, input_real, entry_map_quadrature,
    output_real, output_imaginary, added_log_decay, out_weight, mix_gain, gate_weight, up_weight,
    down_weight, pre_gain, post_gain,
):
    partial = front(
        ssm_input, added_log_decay, pole_real, pole_imaginary, step_log, input_real,
        entry_map_quadrature, output_real, output_imaginary, out_weight,
    )
    mixed_own = summed_on_arrival(partial, "tp")
    middle = round_half(residual.astype(F32) + rms_scale(mixed_own, mix_gain))
    normed_own = rms_scale(middle.astype(F32), pre_gain).astype(BF16)
    mixer_input = from_everyone(normed_own, "tp").reshape(T, -1)
    both = jnp.concatenate((gate_weight, up_weight, down_weight), axis=1)
    whole = lax.all_gather(both, "sp", axis=0, tiled=True)
    f = gate_weight.shape[1]
    gate_full, up_full, down_full = whole[:, :f], whole[:, f : 2 * f], whole[:, 2 * f :]
    gate_act = jnp.dot(mixer_input, gate_full, preferred_element_type=F32)
    up_act = jnp.dot(mixer_input, up_full, preferred_element_type=F32)
    hidden = (jax.nn.silu(gate_act) * up_act).astype(BF16)
    mixer_own = summed_on_arrival(dot_nt(hidden, down_full).astype(BF16), "tp")
    merged = middle.astype(F32) + 0.5 * rms_scale(mixer_own, post_gain)
    return merged.astype(BF16)


def solution(mesh):
    return jax.shard_map(
        shards,
        mesh=mesh,
        in_specs=(
            P(("sp", "tp"), None), P("sp", "tp"), P("tp", None), P("tp", None), P("tp"),
            P("tp", None, None), P("tp", None, None), P("tp", None, None), P("tp", None, None),
            P("sp", "tp"), P("tp", None), P(), P("sp", "tp"), P("sp", "tp"), P("sp", "tp"),
            P(), P(),
        ),
        out_specs=P(("sp", "tp"), None),
        check_vma=False,
    )
```

```python
import functools

import jax
import jax.numpy as jnp
from jax import lax
from jax.experimental import pallas as pl
from jax.experimental.pallas import tpu as pltpu
from jax.sharding import PartitionSpec as P

EPSILON = 1e-06
EXACT = lax.Precision.HIGHEST
MESH = pl.DeviceIdType.MESH
F32 = jnp.float32
BF16 = jnp.bfloat16
T = 256
G = 32
N = 64
C = 16
GN = G * N
SEGS = 8
STEPS = T // SEGS
D = 2048
F = 1408
ROWS = 64
HALF = D // 2
TILES = F // 128


def dot(a, b, **kw):
    return jnp.dot(a, b, preferred_element_type=F32, **kw)


def dot_nt(a, b):
    return lax.dot_general(a, b, (((1,), (1,)), ((), ())), preferred_element_type=F32)


def iota(shape, dim):
    return lax.broadcasted_iota(jnp.int32, shape, dim)


def one_hot(mask, dtype):
    return jnp.where(mask, 1.0, 0.0).astype(dtype)


def cmul(ar, ai, br, bi):
    return ar * br - ai * bi, ar * bi + ai * br


def split(v):
    hi = v.astype(BF16)
    return hi, (v - hi.astype(F32)).astype(BF16)


def expm1(x):
    p = 1.0 / 40320.0
    for k in (5040.0, 720.0, 120.0, 24.0, 6.0, 2.0, 1.0):
        p = p * x + 1.0 / k
    return jnp.where(x > -0.5, p * x, jnp.exp(x) - 1.0)


def step_rows(pr_ref, pi_ref, sl_ref):
    tile = one_hot(iota((N, GN), 1) % N == iota((N, GN), 0), F32)
    mine = iota((G, GN), 1) // N == iota((G, GN), 0)
    groups = one_hot(mine, F32)

    def row(ref):
        wide = dot(ref[...], tile, precision=EXACT)
        return jnp.sum(jnp.where(mine, wide, 0.0), axis=0, keepdims=True)

    pr, pi = row(pr_ref), row(pi_ref)
    sl = dot(jnp.broadcast_to(sl_ref[...], (8, G)), groups, precision=EXACT)[0:1]
    step = jnp.exp(sl)
    log_size = pr * step
    angle = pi * step
    cosine, sine = jnp.cos(angle), jnp.sin(angle)
    size = jnp.exp(log_size)
    half = jnp.sin(0.5 * angle)
    lift_r = expm1(log_size) * cosine - 2.0 * half * half
    lift_i = size * sine
    inv = 1.0 / (pr * pr + pi * pi)
    ratio_r = (lift_r * pr + lift_i * pi) * inv
    ratio_i = (lift_i * pr - lift_r * pi) * inv
    return size * cosine, size * sine, ratio_r, ratio_i, groups


def scan_pass(base, e_ref, dr_ref, di_ref, init, store):
    ends = []
    width = GN // 4
    for lc in range(4):
        sl = slice(lc * width, (lc + 1) * width)
        br = jnp.broadcast_to(base[0][:, sl], (SEGS, width))
        bi = jnp.broadcast_to(base[1][:, sl], (SEGS, width))

        def body(i, st):
            sr, si, pe = st
            rows = pl.ds(pl.multiple_of(i * SEGS, SEGS), SEGS)
            e = e_ref[rows, sl]
            ar, ai = br * e, bi * e
            nr = ar * sr - ai * si + dr_ref[rows, sl]
            ni = ar * si + ai * sr + di_ref[rows, sl]
            if store:
                dr_ref[rows, sl] = nr
                di_ref[rows, sl] = ni
                return nr, ni, pe
            return nr, ni, pe * e

        st = (init[0][:, sl], init[1][:, sl], jnp.ones((SEGS, width), F32))
        ends.append(lax.fori_loop(0, STEPS, body, st, unroll=4))
    return [jnp.concatenate([p[k] for p in ends], axis=1) for k in range(3)]


def put_row(ref, slot, part, row):
    for k in range(16):
        ref[slot, part * 16 + k : part * 16 + k + 1, :] = row[:, k * 128 : (k + 1) * 128]


def to_row(block):
    return jnp.concatenate([block[k : k + 1, :] for k in range(16)], axis=1)


def parts_of(ref, slot):
    block = ref[slot]
    return [block[16 * k : 16 * (k + 1), :] for k in range(4)]


def link(first, then):
    ar, ai, sr, si = first
    br, bi, tr, ti = then
    pr, pi = cmul(br, bi, ar, ai)
    ur, ui = cmul(br, bi, sr, si)
    return pr, pi, ur + tr, ui + ti


def choose(cond, a, b):
    return tuple(jnp.where(cond, x, y) for x, y in zip(a, b))


def rms_scale(values, gain):
    return values * lax.rsqrt(jnp.mean(values * values, axis=-1, keepdims=True) + EPSILON) * gain


class Gather:
    def __init__(self, refs, send, recv, sp):
        self.refs, self.send_sem, self.recv_sem = refs, send, recv
        core, y, z = sp % 2, (sp // 2) % 4, sp // 8
        self.core = core
        self.fm, self.sm = 1 + 3 * core, 4 - 3 * core
        f = y + core * (z - y)
        s = z + core * (y - z)
        self.fk = [f, (f + 3) % 4, (f + 1) % 4, (f + 2) % 4]
        self.sk = [s, (s + 3) % 4, (s + 1) % 4, (s + 2) % 4]
        self.f_next, self.f_prev = self.place(2, 0), self.place(1, 0)
        self.s_next, self.s_prev = self.place(0, 2), self.place(0, 1)
        self.partner = sp + 1 - 2 * core
        self.started = []

    def place(self, k, m):
        return 2 * (self.fk[k] * self.fm + self.sk[m] * self.sm) + self.core

    def block(self, p, k, m, half=None):
        start = self.place(k, m) * ROWS
        return self.rows(p, start, half)

    def rows(self, p, start, half):
        if half is None:
            return self.refs[p].at[pl.ds(pl.multiple_of(start, ROWS), ROWS)]
        return self.refs[p].at[pl.ds(pl.multiple_of(start + half * 32, 32), 32)]

    def copy(self, p, slot, ref, dev):
        return pltpu.make_async_remote_copy(
            ref, ref, self.send_sem.at[p, slot], self.recv_sem.at[p, slot],
            device_id={"sp": dev}, device_id_type=MESH)

    def send(self, p, slot, ref, dev):
        copy = self.copy(p, slot, ref, dev)
        copy.start()
        self.started.append(copy)

    def arrive(self, p, slot, ref):
        self.copy(p, slot, ref, self.partner).wait_recv()

    def hand(self, p, k, m):
        self.send(p, 20 + 4 * k + m, self.block(p, k, m), self.partner)

    def along_s(self, p, k):
        ref = self.block(p, k, 0)
        self.send(p, 4 + 4 * k, ref, self.s_next)
        self.send(p, 5 + 4 * k, ref, self.s_prev)

    def onward(self, p, k):
        self.arrive(p, 4 + 4 * k, self.block(p, k, 1))
        self.arrive(p, 5 + 4 * k, self.block(p, k, 2))
        self.send(p, 6 + 4 * k, self.block(p, k, 1, 0), self.s_next)
        self.send(p, 7 + 4 * k, self.block(p, k, 2, 1), self.s_prev)
        self.hand(p, k, 1)
        self.hand(p, k, 2)

    def stage0(self, p):
        own = self.block(p, 0, 0)
        self.send(p, 0, own, self.f_next)
        self.send(p, 1, own, self.f_prev)
        self.along_s(p, 0)
        self.hand(p, 0, 0)

    def stage1(self, p):
        self.arrive(p, 0, self.block(p, 1, 0))
        self.arrive(p, 1, self.block(p, 2, 0))
        self.send(p, 2, self.block(p, 1, 0, 0), self.f_next)
        self.send(p, 3, self.block(p, 2, 0, 1), self.f_prev)
        self.along_s(p, 1)
        self.hand(p, 1, 0)
        self.onward(p, 0)
        self.along_s(p, 2)
        self.hand(p, 2, 0)

    def stage2(self, p):
        self.arrive(p, 2, self.block(p, 3, 0, 0))
        self.arrive(p, 3, self.block(p, 3, 0, 1))
        self.along_s(p, 3)
        self.hand(p, 3, 0)
        self.onward(p, 1)

    def stage3(self, p):
        self.onward(p, 2)
        self.onward(p, 3)

    def stage4(self, p):
        for k in range(4):
            self.arrive(p, 6 + 4 * k, self.block(p, k, 3, 0))
            self.arrive(p, 7 + 4 * k, self.block(p, k, 3, 1))
            self.hand(p, k, 3)

    def stage5(self, p):
        for k in range(4):
            for m in range(4):
                chip = 2 * (self.sk[k] * self.sm + self.fk[m] * self.fm)
                ref = self.rows(p, (chip + 1 - self.core) * ROWS, None)
                self.arrive(p, 20 + 4 * k + m, ref)


class Across:
    def __init__(self, x, send, recv):
        self.x, self.send_sem, self.recv_sem = x, send, recv
        self.next, self.prev, self.far = (x + 1) % 4, (x + 3) % 4, (x + 2) % 4
        self.started = []

    def copy(self, phase, slot, src, dst, dev):
        return pltpu.make_async_remote_copy(
            src, dst, self.send_sem.at[phase, slot], self.recv_sem.at[phase, slot],
            device_id={"tp": dev}, device_id_type=MESH)

    def send(self, phase, slot, src, dst, dev):
        copy = self.copy(phase, slot, src, dst, dev)
        copy.start()
        self.started.append(copy)

    def arrive(self, phase, slot, ref):
        self.copy(phase, slot, ref, ref, self.next).wait_recv()

    def rows(self, x, half=None):
        if half is None:
            return pl.ds(pl.multiple_of(x * ROWS, ROWS), ROWS)
        return pl.ds(pl.multiple_of(x * ROWS + half * 32, 32), 32)

    def first(self, phase, part, relay, landed):
        self.send(phase, 0, part.at[0, self.rows(self.far)], relay.at[phase, 0], self.next)
        self.send(phase, 3, part.at[0, self.rows(self.prev)], landed.at[phase, 1, 0], self.prev)

    def second(self, phase, part, relay, landed):
        self.send(phase, 1, part.at[1, self.rows(self.far)], relay.at[phase, 1], self.prev)
        self.send(phase, 2, part.at[1, self.rows(self.next)], landed.at[phase, 0, 1], self.next)

    def pass_on(self, phase, part, relay, landed):
        for side, dev in ((0, self.next), (1, self.prev)):
            self.arrive(phase, side, relay.at[phase, side])
            total = relay[phase, side].astype(F32) + part[side, self.rows(dev)].astype(F32)
            relay[phase, side] = total.astype(BF16)
            self.send(phase, 4 + side, relay.at[phase, side], landed.at[phase, side, side], dev)

    def total(self, phase, part, landed):
        for slot, side, half in ((2, 0, 1), (3, 1, 0), (4, 0, 0), (5, 1, 1)):
            self.arrive(phase, slot, landed.at[phase, side, half])
        halves = [
            part[h, self.rows(self.x)].astype(F32)
            + landed[phase, 0, h].astype(F32)
            + landed[phase, 1, h].astype(F32)
            for h in range(2)
        ]
        return jnp.concatenate(halves, axis=1)

    def share(self, ref):
        own = ref.at[self.rows(self.x)]
        self.send(2, 0, own, own, self.next)
        self.send(2, 1, own, own, self.prev)

    def share_on(self, ref):
        self.arrive(2, 0, ref.at[self.rows(self.prev)])
        self.arrive(2, 1, ref.at[self.rows(self.next)])
        top = ref.at[self.rows(self.prev, 0)]
        bottom = ref.at[self.rows(self.next, 1)]
        self.send(2, 2, top, top, self.next)
        self.send(2, 3, bottom, bottom, self.prev)

    def shared(self, ref):
        self.arrive(2, 2, ref.at[self.rows(self.far, 0)])
        self.arrive(2, 3, ref.at[self.rows(self.far, 1)])


def layer_kernel(
    u_ref, a_ref, pr_ref, pi_ref, sl_ref, bre_ref, bim_ref, cre_ref, cim_ref,
    mix_gain_ref, pre_gain_ref, post_gain_ref, wo_hbm, res_hbm, gate_hbm, up_hbm, down_hbm,
    out_ref,
    e_ref, dr_ref, di_ref, act_ref, ra_ref, rb_ref, wo_ref, res_ref, gu_ref, dn_ref,
    part_ref, relay_ref, landed_ref, rows_ref, hid_ref,
    sa, qa, sb, qb, ws, wq, xs, xq, ls,
):
    sp = lax.axis_index("sp")
    tp = lax.axis_index("tp")
    q = sp % 8
    z = sp // 8
    peers_a = [z * 8 + (q + d) % 8 for d in range(1, 8)]
    peers_b = [((z + d) % 4) * 8 + q for d in range(1, 4)]
    weights = Gather((gu_ref, dn_ref), ws, wq, sp)
    across = Across(tp, xs, xq)
    own = pl.ds(pl.multiple_of(sp * ROWS, ROWS), ROWS)
    loads = []
    for j in range(TILES):
        for side, hbm in ((0, gate_hbm), (1, up_hbm)):
            loads.append(pltpu.make_async_copy(
                hbm.at[:, pl.ds(j * 128, 128)],
                gu_ref.at[own, pl.ds((2 * j + side) * 128, 128)], ls.at[2 * j + side]))
    loads.append(pltpu.make_async_copy(down_hbm, dn_ref.at[own], ls.at[2 * TILES]))
    loads.append(pltpu.make_async_copy(wo_hbm, wo_ref, ls.at[2 * TILES + 1]))
    loads.append(pltpu.make_async_copy(res_hbm, res_ref, ls.at[2 * TILES + 2]))
    for load in loads:
        load.start()
    barrier = pltpu.get_barrier_semaphore()
    for peer in peers_a + peers_b:
        pl.semaphore_signal(barrier, inc=1, device_id={"sp": peer}, device_id_type=MESH)
    for peer in (across.next, across.prev):
        pl.semaphore_signal(barrier, inc=1, device_id={"tp": peer}, device_id_type=MESH)
    for load in loads[: 2 * TILES]:
        load.wait()
    pl.semaphore_wait(barrier, 12)
    weights.stage0(0)

    base_r, base_i, ratio_r, ratio_i, groups = step_rows(pr_ref, pi_ref, sl_ref)
    perm = iota((T, T), 0) == (iota((T, T), 1) % SEGS) * STEPS + iota((T, T), 1) // SEGS
    e_small = dot(jnp.exp(a_ref[...]), one_hot(perm, F32), precision=EXACT)
    e_ref[...] = lax.dot_general(
        e_small, groups, (((0,), (0,)), ((), ())), precision=EXACT, preferred_element_type=F32)
    order = iota((T, T), 1) == (iota((T, T), 0) % SEGS) * STEPS + iota((T, T), 0) // SEGS
    u = dot(one_hot(order, BF16), u_ref[...]).astype(BF16)
    lay = one_hot(iota((N, 1024), 1) % N == iota((N, 1024), 0), BF16)
    inside = iota((256, 1024), 0) // C == iota((256, 1024), 1) // N

    def spread(v):
        return [jnp.where(inside, dot(piece, lay), 0.0).astype(BF16) for piece in split(v)]

    for h in range(2):
        gn = slice(h * 1024, (h + 1) * 1024)
        ch = slice(h * 256, (h + 1) * 256)
        raw = []
        for ref in (bre_ref, bim_ref):
            hi, lo = spread(ref[ch, :])
            raw.append(dot(u[:, ch], hi) + dot(u[:, ch], lo))
        rr, ri = ratio_r[:, gn], ratio_i[:, gn]
        dr_ref[:, gn] = rr * raw[0] - ri * raw[1]
        di_ref[:, gn] = rr * raw[1] + ri * raw[0]

    zero = jnp.zeros((SEGS, GN), F32)
    end_r, end_i, pe = scan_pass((base_r, base_i), e_ref, dr_ref, di_ref, (zero, zero), False)
    wr, wi = base_r, base_i
    for _ in range(5):
        wr, wi = cmul(wr, wi, wr, wi)
    seg_r, seg_i = wr * pe, wi * pe
    one_row = jnp.ones((1, GN), F32)
    no_row = jnp.zeros((1, GN), F32)
    total = (one_row, no_row, no_row, no_row)
    before = []
    for j in range(SEGS):
        before.append(total)
        total = link(total, (seg_r[j : j + 1], seg_i[j : j + 1], end_r[j : j + 1], end_i[j : j + 1]))
    for k in range(4):
        put_row(ra_ref, 0, k, total[k])

    copies = []
    for d in range(1, 8):
        copies.append(pltpu.make_async_remote_copy(
            ra_ref.at[0], ra_ref.at[d], sa.at[d], qa.at[d],
            device_id={"sp": peers_a[d - 1]}, device_id_type=MESH))
        copies[-1].start()
    for copy in copies:
        copy.wait()
    unit = jnp.ones((16, 128), F32)
    null = jnp.zeros((16, 128), F32)
    run = (unit, null, null, null)
    pre_a = run
    for k in range(8):
        pre_a = choose(q == k, run, pre_a)
        run = link(run, parts_of(ra_ref, (q - k + 8) % 8))
    for k in range(4):
        rb_ref[0, 16 * k : 16 * (k + 1), :] = run[k]
    copies = []
    for d in range(1, 4):
        copies.append(pltpu.make_async_remote_copy(
            rb_ref.at[0], rb_ref.at[d], sb.at[d], qb.at[d],
            device_id={"sp": peers_b[d - 1]}, device_id_type=MESH))
        copies[-1].start()
    weights.stage1(0)
    loads[2 * TILES].wait()
    weights.stage0(1)
    for copy in copies:
        copy.wait()
    run = (unit, null, null, null)
    pre_b = run
    for k in range(4):
        pre_b = choose(z == k, run, pre_b)
        run = link(run, parts_of(rb_ref, (z - k + 4) % 4))
    carry = link(pre_b, pre_a)
    cr, ci = to_row(carry[2]), to_row(carry[3])
    starts = []
    for k in range(SEGS):
        pr, pi, sr, si = before[k]
        tr, ti = cmul(pr, pi, cr, ci)
        starts.append((tr + sr, ti + si))
    init = [jnp.concatenate([s[k] for s in starts], axis=0) for k in range(2)]
    scan_pass((base_r, base_i), e_ref, dr_ref, di_ref, init, True)

    for h in range(2):
        gn = slice(h * 1024, (h + 1) * 1024)
        ch = slice(h * 256, (h + 1) * 256)
        y = None
        for s_ref, c_ref, sign in ((dr_ref, cre_ref, 1.0), (di_ref, cim_ref, -1.0)):
            s_hi, s_lo = split(s_ref[:, gn])
            c_hi, c_lo = spread(sign * c_ref[ch, :])
            term = dot_nt(s_hi, c_hi) + dot_nt(s_lo, c_hi) + dot_nt(s_hi, c_lo)
            y = term if y is None else y + term
        act_ref[:, ch] = jax.nn.gelu(y).astype(BF16)
    act = dot(one_hot(perm, BF16), act_ref[...]).astype(BF16)
    loads[2 * TILES + 1].wait()
    part_ref[0, 0] = dot(act, wo_ref[:, :HALF]).astype(BF16)
    across.first(0, part_ref.at[0], relay_ref, landed_ref)
    part_ref[0, 1] = dot(act, wo_ref[:, HALF:]).astype(BF16)
    across.second(0, part_ref.at[0], relay_ref, landed_ref)
    weights.stage2(0)
    across.pass_on(0, part_ref.at[0], relay_ref, landed_ref)
    weights.stage3(0)
    mixed = across.total(0, part_ref.at[0], landed_ref)
    loads[2 * TILES + 2].wait()
    middle = (res_ref[...].astype(F32) + rms_scale(mixed, mix_gain_ref[...])).astype(BF16)
    res_ref[...] = middle
    normed = rms_scale(middle.astype(F32), pre_gain_ref[...]).astype(BF16)
    rows_ref[across.rows(tp), :] = normed
    across.share(rows_ref)
    weights.stage1(1)
    weights.stage4(0)
    across.share_on(rows_ref)
    weights.stage2(1)
    weights.stage3(1)
    across.shared(rows_ref)
    weights.stage5(0)

    @pl.loop(0, TILES)
    def _(j):
        both = dot(rows_ref[...], gu_ref[:, pl.ds(pl.multiple_of(j * 256, 256), 256)])
        gate, up = both[:, :128], both[:, 128:]
        hidden = gate / (1.0 + jnp.exp(-gate)) * up
        hid_ref[pl.ds(pl.multiple_of(j * 128, 128), 128), :] = hidden.T.astype(BF16)

    weights.stage4(1)
    weights.stage5(1)
    for h in range(2):

        @pl.loop(0, 4)
        def _(j):
            block = dn_ref[pl.ds(pl.multiple_of(h * HALF + j * 256, 256), 256), :]
            part_ref[1, h, :, pl.ds(pl.multiple_of(j * 256, 256), 256)] = (
                dot(block, hid_ref[...]).T.astype(BF16))

        if h == 0:
            across.first(1, part_ref.at[1], relay_ref, landed_ref)
        else:
            across.second(1, part_ref.at[1], relay_ref, landed_ref)
    across.pass_on(1, part_ref.at[1], relay_ref, landed_ref)
    mixer = across.total(1, part_ref.at[1], landed_ref)
    merged = res_ref[...].astype(F32) + 0.5 * rms_scale(mixer, post_gain_ref[...])
    out_ref[...] = merged.astype(BF16)
    for copy in weights.started + across.started:
        copy.wait_send()


def layer(small, large):
    vmem = pl.BlockSpec(memory_space=pltpu.VMEM)
    hbm = pl.BlockSpec(memory_space=pl.ANY)
    dma = pltpu.SemaphoreType.DMA
    return pl.pallas_call(
        layer_kernel,
        out_shape=jax.ShapeDtypeStruct((ROWS, D), BF16),
        in_specs=[vmem] * len(small) + [hbm] * len(large),
        out_specs=vmem,
        scratch_shapes=[
            pltpu.VMEM((T, GN), F32),
            pltpu.VMEM((T, GN), F32),
            pltpu.VMEM((T, GN), F32),
            pltpu.VMEM((T, 512), BF16),
            pltpu.VMEM((8, 64, 128), F32),
            pltpu.VMEM((4, 64, 128), F32),
            pltpu.VMEM((512, D), BF16),
            pltpu.VMEM((ROWS, D), BF16),
            pltpu.VMEM((D, 2 * F), BF16),
            pltpu.VMEM((D, F), BF16),
            pltpu.VMEM((2, 2, T, HALF), BF16),
            pltpu.VMEM((2, 2, ROWS, HALF), BF16),
            pltpu.VMEM((2, 2, 2, ROWS, HALF), BF16),
            pltpu.VMEM((T, D), BF16),
            pltpu.VMEM((F, T), BF16),
            dma((8,)), dma((8,)), dma((4,)), dma((4,)),
            dma((2, 36)), dma((2, 36)), dma((3, 6)), dma((3, 6)), dma((2 * TILES + 3,)),
        ],
        compiler_params=pltpu.CompilerParams(
            collective_id=0, has_side_effects=True, vmem_limit_bytes=66000000
        ),
        name="layer",
    )(*small, *large)


def shards(
    residual, ssm_input, pole_real, pole_imaginary, step_log, input_real, entry_map_quadrature,
    output_real, output_imaginary, added_log_decay, out_weight, mix_gain, gate_weight, up_weight,
    down_weight, pre_gain, post_gain,
):
    small = (
        ssm_input, added_log_decay.T, pole_real, pole_imaginary, step_log.reshape(1, G),
        input_real.transpose(0, 2, 1).reshape(512, N),
        entry_map_quadrature.transpose(0, 2, 1).reshape(512, N),
        output_real.reshape(512, N), output_imaginary.reshape(512, N),
        mix_gain.reshape(1, D), pre_gain.reshape(1, D), post_gain.reshape(1, D),
    )
    return layer(small, (out_weight, residual, gate_weight, up_weight, down_weight))


def solution(mesh):
    return jax.shard_map(
        shards,
        mesh=mesh,
        in_specs=(
            P(("sp", "tp"), None), P("sp", "tp"), P("tp", None), P("tp", None), P("tp"),
            P("tp", None, None), P("tp", None, None), P("tp", None, None), P("tp", None, None),
            P("sp", "tp"), P("tp", None), P(), P("sp", "tp"), P("sp", "tp"), P("sp", "tp"),
            P(), P(),
        ),
        out_specs=P(("sp", "tp"), None),
        check_vma=False,
    )
```

```python
import functools

import jax
import jax.numpy as jnp
from jax import lax
from jax.experimental import pallas as pl
from jax.experimental.pallas import tpu as pltpu
from jax.sharding import PartitionSpec as P

EPSILON = 1e-06
EXACT = lax.Precision.HIGHEST
MESH = pl.DeviceIdType.MESH
F32 = jnp.float32
BF16 = jnp.bfloat16
T = 256
G = 32
N = 64
C = 16
GN = G * N
SEGS = 8
STEPS = T // SEGS
D = 2048
F = 1408
ROWS = 64
HALF = D // 2
TILES = F // 128


def dot(a, b, **kw):
    return jnp.dot(a, b, preferred_element_type=F32, **kw)


def dot_nt(a, b):
    return lax.dot_general(a, b, (((1,), (1,)), ((), ())), preferred_element_type=F32)


def iota(shape, dim):
    return lax.broadcasted_iota(jnp.int32, shape, dim)


def one_hot(mask, dtype):
    return jnp.where(mask, 1.0, 0.0).astype(dtype)


def cmul(ar, ai, br, bi):
    return ar * br - ai * bi, ar * bi + ai * br


def split(v):
    hi = v.astype(BF16)
    return hi, (v - hi.astype(F32)).astype(BF16)


def expm1(x):
    p = 1.0 / 40320.0
    for k in (5040.0, 720.0, 120.0, 24.0, 6.0, 2.0, 1.0):
        p = p * x + 1.0 / k
    return jnp.where(x > -0.5, p * x, jnp.exp(x) - 1.0)


def lanes_of(v, count):
    pair = jnp.concatenate([v, v], axis=1)
    return jnp.concatenate([pair] * (count // 128), axis=1)


def step_rows(pr, pi, sl):
    mine = iota((G, GN), 1) // N == iota((G, GN), 0)

    def row(v):
        return jnp.sum(jnp.where(mine, v, 0.0), axis=0, keepdims=True)

    same = iota((G, G), 0) == iota((G, G), 1)
    column = jnp.sum(jnp.where(same, jnp.broadcast_to(sl, (G, G)), 0.0), axis=1, keepdims=True)
    pr, pi, step = row(lanes_of(pr, GN)), row(lanes_of(pi, GN)), jnp.exp(row(column))
    log_size = pr * step
    angle = pi * step
    cosine, sine = jnp.cos(angle), jnp.sin(angle)
    size = jnp.exp(log_size)
    half = jnp.sin(0.5 * angle)
    lift_r = expm1(log_size) * cosine - 2.0 * half * half
    lift_i = size * sine
    inv = 1.0 / (pr * pr + pi * pi)
    ratio_r = (lift_r * pr + lift_i * pi) * inv
    ratio_i = (lift_i * pr - lift_r * pi) * inv
    return size * cosine, size * sine, ratio_r, ratio_i, mine, row


def thirds(v):
    hi = v.astype(BF16)
    rest = v - hi.astype(F32)
    mid = rest.astype(BF16)
    return jnp.concatenate([hi, mid, (rest - mid.astype(F32)).astype(BF16)], axis=0)


def scan_pass(base, e_ref, dr_ref, di_ref, init, store):
    ends = []
    width = GN // 4
    for lc in range(4):
        sl = slice(lc * width, (lc + 1) * width)
        br = jnp.broadcast_to(base[0][:, sl], (SEGS, width))
        bi = jnp.broadcast_to(base[1][:, sl], (SEGS, width))

        def body(i, st):
            sr, si, pe = st
            rows = pl.ds(pl.multiple_of(i * SEGS, SEGS), SEGS)
            e = e_ref[rows, sl]
            ar, ai = br * e, bi * e
            nr = ar * sr - ai * si + dr_ref[rows, sl]
            ni = ar * si + ai * sr + di_ref[rows, sl]
            if store:
                dr_ref[rows, sl] = nr
                di_ref[rows, sl] = ni
                return nr, ni, pe
            return nr, ni, pe * e

        st = (init[0][:, sl], init[1][:, sl], jnp.ones((SEGS, width), F32))
        ends.append(lax.fori_loop(0, STEPS, body, st, unroll=4))
    return [jnp.concatenate([p[k] for p in ends], axis=1) for k in range(3)]


def put_row(ref, slot, part, row):
    for k in range(16):
        ref[slot, part * 16 + k : part * 16 + k + 1, :] = row[:, k * 128 : (k + 1) * 128].astype(ref.dtype)


def to_block(row):
    return jnp.concatenate([row[:, k * 128 : (k + 1) * 128] for k in range(16)], axis=0)


def to_row(block):
    return jnp.concatenate([block[k : k + 1, :] for k in range(16)], axis=1)


def link(first, then):
    ar, ai, sr, si = first
    br, bi, tr, ti = then
    pr, pi = cmul(br, bi, ar, ai)
    ur, ui = cmul(br, bi, sr, si)
    return pr, pi, ur + tr, ui + ti


def choose(cond, a, b):
    return tuple(jnp.where(cond, x, y) for x, y in zip(a, b))


def rms_scale(values, gain):
    return values * lax.rsqrt(jnp.mean(values * values, axis=-1, keepdims=True) + EPSILON) * gain


class Gather:
    def __init__(self, refs, send, recv, sp):
        self.refs, self.send_sem, self.recv_sem = refs, send, recv
        core, y, z = sp % 2, (sp // 2) % 4, sp // 8
        self.core = core
        self.fm, self.sm = 1 + 3 * core, 4 - 3 * core
        f = y + core * (z - y)
        s = z + core * (y - z)
        self.fk = [f, (f + 3) % 4, (f + 1) % 4, (f + 2) % 4]
        self.sk = [s, (s + 3) % 4, (s + 1) % 4, (s + 2) % 4]
        self.f_next, self.f_prev = self.place(2, 0), self.place(1, 0)
        self.s_next, self.s_prev = self.place(0, 2), self.place(0, 1)
        self.partner = sp + 1 - 2 * core
        self.started = []

    def place(self, k, m):
        return 2 * (self.fk[k] * self.fm + self.sk[m] * self.sm) + self.core

    def block(self, p, k, m, half=None):
        start = self.place(k, m) * ROWS
        return self.rows(p, start, half)

    def rows(self, p, start, half):
        if half is None:
            return self.refs[p].at[pl.ds(pl.multiple_of(start, ROWS), ROWS)]
        return self.refs[p].at[pl.ds(pl.multiple_of(start + half * 32, 32), 32)]

    def copy(self, p, slot, ref, dev):
        return pltpu.make_async_remote_copy(
            ref, ref, self.send_sem.at[p, slot], self.recv_sem.at[p, slot],
            device_id={"sp": dev}, device_id_type=MESH)

    def send(self, p, slot, ref, dev):
        copy = self.copy(p, slot, ref, dev)
        copy.start()
        self.started.append(copy)

    def arrive(self, p, slot, ref):
        self.copy(p, slot, ref, self.partner).wait_recv()

    def hand(self, p, k, m):
        self.send(p, 20 + 4 * k + m, self.block(p, k, m), self.partner)

    def along_f(self, p):
        own = self.block(p, 0, 0)
        self.send(p, 0, own, self.f_next)
        self.send(p, 1, own, self.f_prev)

    def beyond_f(self, p):
        self.arrive(p, 0, self.block(p, 1, 0))
        self.arrive(p, 1, self.block(p, 2, 0))
        self.send(p, 2, self.block(p, 1, 0, 0), self.f_next)
        self.send(p, 3, self.block(p, 2, 0, 1), self.f_prev)

    def opposite_f(self, p):
        self.arrive(p, 2, self.block(p, 3, 0, 0))
        self.arrive(p, 3, self.block(p, 3, 0, 1))

    def along_s(self, p, k):
        ref = self.block(p, k, 0)
        self.send(p, 4 + 4 * k, ref, self.s_next)
        self.send(p, 5 + 4 * k, ref, self.s_prev)
        self.hand(p, k, 0)

    def beyond_s(self, p, k):
        self.arrive(p, 4 + 4 * k, self.block(p, k, 1))
        self.arrive(p, 5 + 4 * k, self.block(p, k, 2))
        self.send(p, 6 + 4 * k, self.block(p, k, 1, 0), self.s_next)
        self.send(p, 7 + 4 * k, self.block(p, k, 2, 1), self.s_prev)
        self.hand(p, k, 1)
        self.hand(p, k, 2)

    def opposite_s(self, p):
        for k in range(4):
            self.arrive(p, 6 + 4 * k, self.block(p, k, 3, 0))
            self.arrive(p, 7 + 4 * k, self.block(p, k, 3, 1))
            self.hand(p, k, 3)

    def handed(self, p, places):
        for k in range(4):
            for m in places:
                chip = 2 * (self.sk[k] * self.sm + self.fk[m] * self.fm)
                ref = self.rows(p, (chip + 1 - self.core) * ROWS, None)
                self.arrive(p, 20 + 4 * k + m, ref)

    def columns(self, k, m):
        return pl.multiple_of((self.fk[k] * self.fm + self.sk[m] * self.sm) * 128, 128)


class Across:
    def __init__(self, x, send, recv):
        self.x, self.send_sem, self.recv_sem = x, send, recv
        self.next, self.prev, self.far = (x + 1) % 4, (x + 3) % 4, (x + 2) % 4
        self.started = []

    def copy(self, phase, slot, src, dst, dev):
        return pltpu.make_async_remote_copy(
            src, dst, self.send_sem.at[phase, slot], self.recv_sem.at[phase, slot],
            device_id={"tp": dev}, device_id_type=MESH)

    def send(self, phase, slot, src, dst, dev):
        copy = self.copy(phase, slot, src, dst, dev)
        copy.start()
        self.started.append(copy)

    def arrive(self, phase, slot, ref):
        self.copy(phase, slot, ref, ref, self.next).wait_recv()

    def rows(self, x, half=None):
        if half is None:
            return pl.ds(pl.multiple_of(x * ROWS, ROWS), ROWS)
        return pl.ds(pl.multiple_of(x * ROWS + half * 32, 32), 32)

    def first(self, phase, part, relay, landed):
        self.send(phase, 0, part.at[0, self.rows(self.far)], relay.at[phase, 0], self.next)
        if phase == 1:
            self.send(phase, 3, part.at[0, self.rows(self.prev)], landed.at[phase, 1, 0], self.prev)

    def second(self, phase, part, relay, landed):
        self.send(phase, 1, part.at[1, self.rows(self.far)], relay.at[phase, 1], self.prev)
        if phase == 0:
            self.send(phase, 3, part.at[0, self.rows(self.prev)], landed.at[phase, 1, 0], self.prev)
        self.send(phase, 2, part.at[1, self.rows(self.next)], landed.at[phase, 0, 1], self.next)

    def pass_on(self, phase, side, part, relay, landed):
        dev = (self.next, self.prev)[side]
        self.arrive(phase, side, relay.at[phase, side])
        total = relay[phase, side].astype(F32) + part[side, self.rows(dev)].astype(F32)
        relay[phase, side] = total.astype(BF16)
        self.send(phase, 4 + side, relay.at[phase, side], landed.at[phase, side, side], dev)

    def total(self, phase, part, landed):
        for slot, side, half in ((2, 0, 1), (3, 1, 0), (4, 0, 0), (5, 1, 1)):
            self.arrive(phase, slot, landed.at[phase, side, half])
        halves = [
            part[h, self.rows(self.x)].astype(F32)
            + landed[phase, 0, h].astype(F32)
            + landed[phase, 1, h].astype(F32)
            for h in range(2)
        ]
        return jnp.concatenate(halves, axis=1)

    def share(self, ref):
        own = ref.at[self.rows(self.x)]
        self.send(2, 0, own, own, self.next)
        self.send(2, 1, own, own, self.prev)

    def share_on(self, ref):
        self.arrive(2, 0, ref.at[self.rows(self.prev)])
        self.arrive(2, 1, ref.at[self.rows(self.next)])
        top = ref.at[self.rows(self.prev, 0)]
        bottom = ref.at[self.rows(self.next, 1)]
        self.send(2, 2, top, top, self.next)
        self.send(2, 3, bottom, bottom, self.prev)

    def shared(self, ref):
        self.arrive(2, 2, ref.at[self.rows(self.far, 0)])
        self.arrive(2, 3, ref.at[self.rows(self.far, 1)])


EARLY = [(0, 0), (1, 0), (2, 0), (0, 1), (0, 2), (1, 1), (1, 2), (2, 1)]
LATE = [(2, 2), (3, 0), (3, 1), (3, 2), (0, 3), (1, 3), (2, 3), (3, 3)]


def layer_kernel(
    u_hbm, a_hbm, pr_hbm, pi_hbm, sl_hbm, bre_hbm, bim_hbm, cre_hbm, cim_hbm,
    mix_gain_hbm, pre_gain_hbm, post_gain_hbm, wo_hbm, res_hbm, gate_hbm, up_hbm, down_hbm,
    out_ref,
    u_ref, a_ref, pr_ref, pi_ref, sl_ref, bre_ref, bim_ref, cre_ref, cim_ref,
    mix_gain_ref, pre_gain_ref, post_gain_ref, wo_ref, res_ref,
    e_ref, dr_ref, di_ref, act_ref, cs_ref, ea_ref, eb_ref, ra_ref, rb_ref, gu_ref, dn_ref,
    part_ref, relay_ref, landed_ref, rows_ref, hid_ref, sum_ref,
    sa, qa, sb, qb, ws, wq, xs, xq, ls, gs,
):
    sp = lax.axis_index("sp")
    tp = lax.axis_index("tp")
    q = sp % 8
    z = sp // 8
    peers_a = [z * 8 + (q + d) % 8 for d in range(1, 8)]
    peers_b = [((z + d) % 4) * 8 + q for d in range(1, 4)]
    weights = Gather((gu_ref, dn_ref), ws, wq, sp)
    across = Across(tp, xs, xq)
    own = pl.ds(pl.multiple_of(sp * ROWS, ROWS), ROWS)
    barrier = pltpu.get_barrier_semaphore()
    for peer in peers_a + peers_b:
        pl.semaphore_signal(barrier, inc=1, device_id={"sp": peer}, device_id_type=MESH)
    for peer in (across.next, across.prev):
        pl.semaphore_signal(barrier, inc=1, device_id={"tp": peer}, device_id_type=MESH)
    pairs = (
        (pr_hbm, pr_ref), (pi_hbm, pi_ref), (sl_hbm, sl_ref), (a_hbm, a_ref), (u_hbm, u_ref),
        (bre_hbm, bre_ref), (bim_hbm, bim_ref), (cre_hbm, cre_ref), (cim_hbm, cim_ref),
        (wo_hbm, wo_ref), (res_hbm, res_ref), (mix_gain_hbm, mix_gain_ref),
        (pre_gain_hbm, pre_gain_ref), (post_gain_hbm, post_gain_ref), (down_hbm, dn_ref.at[own]),
    )
    loads = [pltpu.make_async_copy(src, dst, ls.at[k]) for k, (src, dst) in enumerate(pairs)]
    for load in loads[:4]:
        load.start()
    shard_loads = []
    for j in range(TILES):
        for side, hbm in ((0, gate_hbm), (1, up_hbm)):
            shard_loads.append(pltpu.make_async_copy(
                hbm.at[:, pl.ds(j * 128, 128)],
                gu_ref.at[own, pl.ds((2 * j + side) * 128, 128)], gs.at[2 * j + side]))
            shard_loads[-1].start()
    for load in loads[4:]:
        load.start()
    for load in loads[:4]:
        load.wait()

    base_r, base_i, ratio_r, ratio_i, mine, row = step_rows(pr_ref[...], pi_ref[...], sl_ref[...])
    ea_row = jnp.exp(row(jnp.sum(a_ref[...], axis=1, keepdims=True)))
    put_row(ea_ref, 0, 0, ea_row)
    for load in shard_loads:
        load.wait()
    pl.semaphore_wait(barrier, 12)
    early = []
    for d in range(1, 8):
        early.append(pltpu.make_async_remote_copy(
            ea_ref.at[0], ea_ref.at[d], sa.at[0, d], qa.at[0, d],
            device_id={"sp": peers_a[d - 1]}, device_id_type=MESH))
        early[-1].start()
    weights.along_f(0)

    perm = iota((T, T), 0) == (iota((T, T), 1) % SEGS) * STEPS + iota((T, T), 1) // SEGS
    order = iota((T, T), 1) == (iota((T, T), 0) % SEGS) * STEPS + iota((T, T), 0) // SEGS
    e_small = dot(thirds(jnp.exp(a_ref[...])), one_hot(perm, BF16)).astype(BF16)
    groups = one_hot(mine, BF16)
    e_ref[...] = lax.dot_general(
        e_small, jnp.concatenate([groups] * 3, axis=0), (((0,), (0,)), ((), ())),
        preferred_element_type=F32)
    for load in loads[4:9]:
        load.wait()
    u = dot(one_hot(order, BF16), u_ref[...]).astype(BF16)
    inside = iota((256, 1024), 0) // C == iota((256, 1024), 1) // N

    def spread(v):
        return jnp.where(inside, lanes_of(v, 1024), 0.0).astype(BF16)

    for h in range(2):
        gn = slice(h * 1024, (h + 1) * 1024)
        ch = slice(h * 256, (h + 1) * 256)
        raw_r = dot(u[:, ch], spread(bre_ref[ch, :]))
        raw_i = dot(u[:, ch], spread(bim_ref[ch, :]))
        rr, ri = ratio_r[:, gn], ratio_i[:, gn]
        dr_ref[:, gn] = rr * raw_r - ri * raw_i
        di_ref[:, gn] = rr * raw_i + ri * raw_r

    zero = jnp.zeros((SEGS, GN), F32)
    end_r, end_i, pe = scan_pass((base_r, base_i), e_ref, dr_ref, di_ref, (zero, zero), False)
    wr, wi = base_r, base_i
    for _ in range(5):
        wr, wi = cmul(wr, wi, wr, wi)
    seg_r, seg_i = wr * pe, wi * pe
    one_row = jnp.ones((1, GN), F32)
    no_row = jnp.zeros((1, GN), F32)
    total = (one_row, no_row, no_row, no_row)
    before = []
    for j in range(SEGS):
        before.append(total)
        total = link(total, (seg_r[j : j + 1], seg_i[j : j + 1], end_r[j : j + 1], end_i[j : j + 1]))
    put_row(ra_ref, 0, 0, total[2])
    put_row(ra_ref, 0, 1, total[3])

    sent_a = []
    for d in range(1, 8):
        sent_a.append(pltpu.make_async_remote_copy(
            ra_ref.at[0], ra_ref.at[d], sa.at[1, d], qa.at[1, d],
            device_id={"sp": peers_a[d - 1]}, device_id_type=MESH))
        sent_a[-1].start()
    loads[14].wait()
    weights.along_f(1)
    for h in range(2):
        ch = slice(h * 256, (h + 1) * 256)
        cs_ref[h, 0] = spread(cre_ref[ch, :])
        cs_ref[h, 1] = spread(-cim_ref[ch, :])
    w_r, w_i = to_block(wr), to_block(wi)
    for _ in range(3):
        w_r, w_i = cmul(w_r, w_i, w_r, w_i)
    v_r, v_i = w_r, w_i
    for _ in range(3):
        v_r, v_i = cmul(v_r, v_i, v_r, v_i)
    for copy in early:
        copy.wait()
    eb = ea_ref[0]
    for d in range(1, 8):
        eb = eb * ea_ref[d]
    eb_ref[0] = eb
    early_b = []
    for d in range(1, 4):
        early_b.append(pltpu.make_async_remote_copy(
            eb_ref.at[0], eb_ref.at[d], sb.at[0, d], qb.at[0, d],
            device_id={"sp": peers_b[d - 1]}, device_id_type=MESH))
        early_b[-1].start()
    for copy in sent_a:
        copy.wait()
    unit = jnp.ones((16, 128), F32)
    null = jnp.zeros((16, 128), F32)

    def stretch(e, pr, pi, ref, slot):
        block = ref[slot].astype(F32)
        decay = e[slot]
        return pr * decay, pi * decay, block[:16], block[16:]

    run = (unit, null, null, null)
    pre_a = run
    for k in range(8):
        pre_a = choose(q == k, run, pre_a)
        run = link(run, stretch(ea_ref, w_r, w_i, ra_ref, (q - k + 8) % 8))
    rb_ref[0, :16] = run[2].astype(BF16)
    rb_ref[0, 16:] = run[3].astype(BF16)
    sent_b = []
    for d in range(1, 4):
        sent_b.append(pltpu.make_async_remote_copy(
            rb_ref.at[0], rb_ref.at[d], sb.at[1, d], qb.at[1, d],
            device_id={"sp": peers_b[d - 1]}, device_id_type=MESH))
        sent_b[-1].start()
    weights.along_s(0, 0)
    weights.beyond_f(0)
    weights.along_s(0, 1)
    weights.along_s(0, 2)
    weights.beyond_f(1)
    for copy in early_b + sent_b:
        copy.wait()
    run = (unit, null, null, null)
    pre_b = run
    for k in range(4):
        pre_b = choose(z == k, run, pre_b)
        run = link(run, stretch(eb_ref, v_r, v_i, rb_ref, (z - k + 4) % 4))
    carry = link(pre_b, pre_a)
    cr, ci = to_row(carry[2]), to_row(carry[3])
    starts = []
    for k in range(SEGS):
        pr, pi, sr, si = before[k]
        tr, ti = cmul(pr, pi, cr, ci)
        starts.append((tr + sr, ti + si))
    init = [jnp.concatenate([s[k] for s in starts], axis=0) for k in range(2)]
    scan_pass((base_r, base_i), e_ref, dr_ref, di_ref, init, True)

    for h in range(2):
        gn = slice(h * 1024, (h + 1) * 1024)
        y = dot_nt(dr_ref[:, gn].astype(BF16), cs_ref[h, 0])
        y = y + dot_nt(di_ref[:, gn].astype(BF16), cs_ref[h, 1])
        act_ref[:, h * 256 : (h + 1) * 256] = jax.nn.gelu(y).astype(BF16)
    act = dot(one_hot(perm, BF16), act_ref[...]).astype(BF16)
    loads[9].wait()
    part_ref[0, 0] = dot(act, wo_ref[:, :HALF]).astype(BF16)
    across.first(0, part_ref.at[0], relay_ref, landed_ref)
    part_ref[0, 1] = dot(act, wo_ref[:, HALF:]).astype(BF16)
    across.second(0, part_ref.at[0], relay_ref, landed_ref)
    weights.opposite_f(0)
    weights.along_s(0, 3)
    weights.beyond_s(0, 0)
    across.pass_on(0, 0, part_ref.at[0], relay_ref, landed_ref)
    across.pass_on(0, 1, part_ref.at[0], relay_ref, landed_ref)
    weights.beyond_s(0, 1)
    mixed = across.total(0, part_ref.at[0], landed_ref)
    for load in loads[10:14]:
        load.wait()
    middle = (res_ref[...].astype(F32) + rms_scale(mixed, mix_gain_ref[...])).astype(BF16)
    res_ref[...] = middle
    normed = rms_scale(middle.astype(F32), pre_gain_ref[...]).astype(BF16)
    rows_ref[across.rows(tp), :] = normed
    across.share(rows_ref)
    weights.beyond_s(0, 2)
    weights.opposite_f(1)
    weights.along_s(1, 0)
    weights.along_s(1, 1)
    across.share_on(rows_ref)
    weights.beyond_s(0, 3)
    weights.along_s(1, 2)
    weights.along_s(1, 3)
    across.shared(rows_ref)
    weights.opposite_s(0)
    weights.handed(0, range(4))
    for j in range(TILES):
        both = dot(rows_ref[...], gu_ref[:, j * 256 : (j + 1) * 256])
        gate, up = both[:, :128], both[:, 128:]
        hidden = gate / (1.0 + jnp.exp(-gate)) * up
        hid_ref[j * 128 : (j + 1) * 128, :] = hidden.T.astype(BF16)
        if j == 5:
            weights.beyond_s(1, 0)
            weights.beyond_s(1, 1)

    weights.beyond_s(1, 2)
    weights.beyond_s(1, 3)
    weights.handed(1, range(3))
    for h, chips in enumerate((EARLY, LATE)):
        if h == 1:
            weights.opposite_s(1)
            weights.handed(1, (3,))
            across.pass_on(1, 0, part_ref.at[1], relay_ref, landed_ref)
        for j in (0, 4):
            block = jnp.concatenate(
                [dn_ref[pl.ds(weights.columns(k, m), 128), :] for k, m in chips[j : j + 4]], axis=0)
            out = dot(block, hid_ref[...])
            for i in range(4):
                part_ref[1, h, :, (j + i) * 128 : (j + i + 1) * 128] = (
                    out[i * 128 : (i + 1) * 128].T.astype(BF16))
        if h == 0:
            across.first(1, part_ref.at[1], relay_ref, landed_ref)
        else:
            across.second(1, part_ref.at[1], relay_ref, landed_ref)
    across.pass_on(1, 1, part_ref.at[1], relay_ref, landed_ref)
    mixer = across.total(1, part_ref.at[1], landed_ref)
    for j, (k, m) in enumerate(EARLY + LATE):
        sum_ref[:, pl.ds(weights.columns(k, m), 128)] = mixer[:, j * 128 : (j + 1) * 128]
    merged = res_ref[...].astype(F32) + 0.5 * rms_scale(sum_ref[...], post_gain_ref[...])
    out_ref[...] = merged.astype(BF16)
    for copy in weights.started + across.started:
        copy.wait_send()


def layer(arrays):
    hbm = pl.BlockSpec(memory_space=pl.ANY)
    dma = pltpu.SemaphoreType.DMA
    held = [pltpu.VMEM(v.shape, v.dtype) for v in arrays[:14]]
    return pl.pallas_call(
        layer_kernel,
        out_shape=jax.ShapeDtypeStruct((ROWS, D), BF16),
        in_specs=[hbm] * len(arrays),
        out_specs=pl.BlockSpec(memory_space=pltpu.VMEM),
        scratch_shapes=[
            *held,
            pltpu.VMEM((T, GN), F32),
            pltpu.VMEM((T, GN), F32),
            pltpu.VMEM((T, GN), F32),
            pltpu.VMEM((T, 512), BF16),
            pltpu.VMEM((2, 2, 256, 1024), BF16),
            pltpu.VMEM((8, 16, 128), F32),
            pltpu.VMEM((4, 16, 128), F32),
            pltpu.VMEM((8, 32, 128), BF16),
            pltpu.VMEM((4, 32, 128), BF16),
            pltpu.VMEM((D, 2 * F), BF16),
            pltpu.VMEM((D, F), BF16),
            pltpu.VMEM((2, 2, T, HALF), BF16),
            pltpu.VMEM((2, 2, ROWS, HALF), BF16),
            pltpu.VMEM((2, 2, 2, ROWS, HALF), BF16),
            pltpu.VMEM((T, D), BF16),
            pltpu.VMEM((F, T), BF16),
            pltpu.VMEM((ROWS, D), F32),
            dma((2, 8)), dma((2, 8)), dma((2, 4)), dma((2, 4)),
            dma((2, 36)), dma((2, 36)), dma((3, 6)), dma((3, 6)), dma((15,)), dma((2 * TILES,)),
        ],
        compiler_params=pltpu.CompilerParams(
            collective_id=0, has_side_effects=True, vmem_limit_bytes=66000000
        ),
        name="layer",
    )(*arrays)


def shards(
    residual, ssm_input, pole_real, pole_imaginary, step_log, input_real, entry_map_quadrature,
    output_real, output_imaginary, added_log_decay, out_weight, mix_gain, gate_weight, up_weight,
    down_weight, pre_gain, post_gain,
):
    small = (
        ssm_input, added_log_decay.T, pole_real, pole_imaginary, step_log.reshape(1, G),
        input_real.transpose(0, 2, 1).reshape(512, N),
        entry_map_quadrature.transpose(0, 2, 1).reshape(512, N),
        output_real.reshape(512, N), output_imaginary.reshape(512, N),
        mix_gain.reshape(1, D), pre_gain.reshape(1, D), post_gain.reshape(1, D),
    )
    return layer(small + (out_weight, residual, gate_weight, up_weight, down_weight))


def solution(mesh):
    return jax.shard_map(
        shards,
        mesh=mesh,
        in_specs=(
            P(("sp", "tp"), None), P("sp", "tp"), P("tp", None), P("tp", None), P("tp"),
            P("tp", None, None), P("tp", None, None), P("tp", None, None), P("tp", None, None),
            P("sp", "tp"), P("tp", None), P(), P("sp", "tp"), P("sp", "tp"), P("sp", "tp"),
            P(), P(),
        ),
        out_specs=P(("sp", "tp"), None),
        check_vma=False,
    )
```

```python
import functools

import jax
import jax.numpy as jnp
from jax import lax
from jax.experimental import pallas as pl
from jax.experimental.pallas import tpu as pltpu
from jax.sharding import PartitionSpec as P

EPSILON = 1e-06
EXACT = lax.Precision.HIGHEST
MESH = pl.DeviceIdType.MESH
F32 = jnp.float32
BF16 = jnp.bfloat16
T = 256
G = 32
N = 64
C = 16
GN = G * N
SEGS = 8
STEPS = T // SEGS
D = 2048
F = 1408
ROWS = 64
HALF = D // 2
TILES = F // 128


def dot(a, b, **kw):
    return jnp.dot(a, b, preferred_element_type=F32, **kw)


def dot_nt(a, b):
    return lax.dot_general(a, b, (((1,), (1,)), ((), ())), preferred_element_type=F32)


def iota(shape, dim):
    return lax.broadcasted_iota(jnp.int32, shape, dim)


def one_hot(mask, dtype):
    return jnp.where(mask, 1.0, 0.0).astype(dtype)


def cmul(ar, ai, br, bi):
    return ar * br - ai * bi, ar * bi + ai * br


def split(v):
    hi = v.astype(BF16)
    return hi, (v - hi.astype(F32)).astype(BF16)


def expm1(x):
    p = 1.0 / 40320.0
    for k in (5040.0, 720.0, 120.0, 24.0, 6.0, 2.0, 1.0):
        p = p * x + 1.0 / k
    return jnp.where(x > -0.5, p * x, jnp.exp(x) - 1.0)


def lanes_of(v, count):
    pair = jnp.concatenate([v, v], axis=1)
    return jnp.concatenate([pair] * (count // 128), axis=1)


def step_rows(pr, pi, sl):
    mine = iota((G, GN), 1) // N == iota((G, GN), 0)

    def row(v):
        return jnp.sum(jnp.where(mine, v, 0.0), axis=0, keepdims=True)

    same = iota((G, G), 0) == iota((G, G), 1)
    column = jnp.sum(jnp.where(same, jnp.broadcast_to(sl, (G, G)), 0.0), axis=1, keepdims=True)
    pr, pi, step = row(lanes_of(pr, GN)), row(lanes_of(pi, GN)), jnp.exp(row(column))
    log_size = pr * step
    angle = pi * step
    cosine, sine = jnp.cos(angle), jnp.sin(angle)
    size = jnp.exp(log_size)
    half = jnp.sin(0.5 * angle)
    lift_r = expm1(log_size) * cosine - 2.0 * half * half
    lift_i = size * sine
    inv = 1.0 / (pr * pr + pi * pi)
    ratio_r = (lift_r * pr + lift_i * pi) * inv
    ratio_i = (lift_i * pr - lift_r * pi) * inv
    return size * cosine, size * sine, ratio_r, ratio_i, mine, row


def thirds(v):
    hi = v.astype(BF16)
    rest = v - hi.astype(F32)
    mid = rest.astype(BF16)
    return jnp.concatenate([hi, mid, (rest - mid.astype(F32)).astype(BF16)], axis=0)


def scan_pass(base, e_ref, dr_ref, di_ref, init, store):
    ends = []
    width = GN // 4
    for lc in range(4):
        sl = slice(lc * width, (lc + 1) * width)
        br = jnp.broadcast_to(base[0][:, sl], (SEGS, width))
        bi = jnp.broadcast_to(base[1][:, sl], (SEGS, width))

        def body(i, st):
            sr, si, pe = st
            rows = pl.ds(pl.multiple_of(i * SEGS, SEGS), SEGS)
            e = e_ref[rows, sl]
            ar, ai = br * e, bi * e
            nr = ar * sr - ai * si + dr_ref[rows, sl]
            ni = ar * si + ai * sr + di_ref[rows, sl]
            if store:
                dr_ref[rows, sl] = nr
                di_ref[rows, sl] = ni
                return nr, ni, pe
            return nr, ni, pe * e

        st = (init[0][:, sl], init[1][:, sl], jnp.ones((SEGS, width), F32))
        ends.append(lax.fori_loop(0, STEPS, body, st, unroll=4))
    return [jnp.concatenate([p[k] for p in ends], axis=1) for k in range(3)]


def put_row(ref, slot, part, row):
    for k in range(16):
        ref[slot, part * 16 + k : part * 16 + k + 1, :] = row[:, k * 128 : (k + 1) * 128].astype(ref.dtype)


def to_block(row):
    return jnp.concatenate([row[:, k * 128 : (k + 1) * 128] for k in range(16)], axis=0)


def to_row(block):
    return jnp.concatenate([block[k : k + 1, :] for k in range(16)], axis=1)


def link(first, then):
    ar, ai, sr, si = first
    br, bi, tr, ti = then
    pr, pi = cmul(br, bi, ar, ai)
    ur, ui = cmul(br, bi, sr, si)
    return pr, pi, ur + tr, ui + ti


def choose(cond, a, b):
    return tuple(jnp.where(cond, x, y) for x, y in zip(a, b))


def rms_scale(values, gain):
    return values * lax.rsqrt(jnp.mean(values * values, axis=-1, keepdims=True) + EPSILON) * gain


class Gather:
    def __init__(self, refs, send, recv, sp):
        self.refs, self.send_sem, self.recv_sem = refs, send, recv
        core, y, z = sp % 2, (sp // 2) % 4, sp // 8
        self.core = core
        self.fm, self.sm = 1 + 3 * core, 4 - 3 * core
        f = y + core * (z - y)
        s = z + core * (y - z)
        self.fk = [f, (f + 3) % 4, (f + 1) % 4, (f + 2) % 4]
        self.sk = [s, (s + 3) % 4, (s + 1) % 4, (s + 2) % 4]
        self.f_next, self.f_prev = self.place(2, 0), self.place(1, 0)
        self.s_next, self.s_prev = self.place(0, 2), self.place(0, 1)
        self.partner = sp + 1 - 2 * core
        self.started = []

    def place(self, k, m):
        return 2 * (self.fk[k] * self.fm + self.sk[m] * self.sm) + self.core

    def block(self, p, k, m, half=None):
        start = self.place(k, m) * ROWS
        return self.rows(p, start, half)

    def rows(self, p, start, half):
        if half is None:
            return self.refs[p].at[pl.ds(pl.multiple_of(start, ROWS), ROWS)]
        return self.refs[p].at[pl.ds(pl.multiple_of(start + half * 32, 32), 32)]

    def copy(self, p, slot, ref, dev):
        return pltpu.make_async_remote_copy(
            ref, ref, self.send_sem.at[p, slot], self.recv_sem.at[p, slot],
            device_id={"sp": dev}, device_id_type=MESH)

    def send(self, p, slot, ref, dev):
        copy = self.copy(p, slot, ref, dev)
        copy.start()
        self.started.append(copy)

    def arrive(self, p, slot, ref):
        self.copy(p, slot, ref, self.partner).wait_recv()

    def hand(self, p, k, m):
        self.send(p, 20 + 4 * k + m, self.block(p, k, m), self.partner)

    def own_along(self, p, turn, half):
        own = self.block(p, 0, 0, half)
        nexts, prevs = (self.f_next, self.s_next), (self.f_prev, self.s_prev)
        for side, (f_dev, s_dev) in enumerate((nexts, prevs)):
            f_slot, s_slot = side, 4 + side
            if half:
                f_slot, s_slot = 36 + side, 38 + side
            self.send(p, f_slot + turn * (s_slot - f_slot), own, f_dev + turn * (s_dev - f_dev))

    def beyond_f(self, p):
        self.arrive(p, 0, self.block(p, 1, 0))
        self.arrive(p, 1, self.block(p, 2, 0))
        self.send(p, 2, self.block(p, 1, 0, 0), self.f_next)
        self.send(p, 3, self.block(p, 2, 0, 1), self.f_prev)

    def beyond_f_next(self):
        self.arrive(0, 0, self.block(0, 1, 0, 0))
        self.send(0, 2, self.block(0, 1, 0, 0), self.f_next)

    def beyond_f_prev(self):
        self.arrive(0, 37, self.block(0, 2, 0, 1))
        self.send(0, 3, self.block(0, 2, 0, 1), self.f_prev)
        self.arrive(0, 36, self.block(0, 1, 0, 1))
        self.arrive(0, 1, self.block(0, 2, 0, 0))

    def beyond_s_own(self):
        self.arrive(0, 4, self.block(0, 0, 1, 0))
        self.arrive(0, 39, self.block(0, 0, 2, 1))
        self.send(0, 6, self.block(0, 0, 1, 0), self.s_next)
        self.send(0, 7, self.block(0, 0, 2, 1), self.s_prev)
        self.arrive(0, 38, self.block(0, 0, 1, 1))
        self.arrive(0, 5, self.block(0, 0, 2, 0))
        self.hand(0, 0, 1)
        self.hand(0, 0, 2)

    def opposite_f(self, p):
        self.arrive(p, 2, self.block(p, 3, 0, 0))
        self.arrive(p, 3, self.block(p, 3, 0, 1))

    def along_s(self, p, k):
        ref = self.block(p, k, 0)
        self.send(p, 4 + 4 * k, ref, self.s_next)
        self.send(p, 5 + 4 * k, ref, self.s_prev)
        self.hand(p, k, 0)

    def beyond_s(self, p, k):
        self.arrive(p, 4 + 4 * k, self.block(p, k, 1))
        self.arrive(p, 5 + 4 * k, self.block(p, k, 2))
        self.send(p, 6 + 4 * k, self.block(p, k, 1, 0), self.s_next)
        self.send(p, 7 + 4 * k, self.block(p, k, 2, 1), self.s_prev)
        self.hand(p, k, 1)
        self.hand(p, k, 2)

    def opposite_s(self, p):
        for k in range(4):
            self.arrive(p, 6 + 4 * k, self.block(p, k, 3, 0))
            self.arrive(p, 7 + 4 * k, self.block(p, k, 3, 1))
            self.hand(p, k, 3)

    def handed(self, p, places):
        for k, m in places:
            chip = 2 * (self.sk[k] * self.sm + self.fk[m] * self.fm)
            ref = self.rows(p, (chip + 1 - self.core) * ROWS, None)
            self.arrive(p, 20 + 4 * k + m, ref)

    def columns(self, k, m):
        return pl.multiple_of((self.fk[k] * self.fm + self.sk[m] * self.sm) * 128, 128)


class Across:
    def __init__(self, x, send, recv):
        self.x, self.send_sem, self.recv_sem = x, send, recv
        self.next, self.prev, self.far = (x + 1) % 4, (x + 3) % 4, (x + 2) % 4
        self.started = []

    def copy(self, phase, slot, src, dst, dev):
        return pltpu.make_async_remote_copy(
            src, dst, self.send_sem.at[phase, slot], self.recv_sem.at[phase, slot],
            device_id={"tp": dev}, device_id_type=MESH)

    def send(self, phase, slot, src, dst, dev):
        copy = self.copy(phase, slot, src, dst, dev)
        copy.start()
        self.started.append(copy)

    def arrive(self, phase, slot, ref):
        self.copy(phase, slot, ref, ref, self.next).wait_recv()

    def rows(self, x, half=None):
        if half is None:
            return pl.ds(pl.multiple_of(x * ROWS, ROWS), ROWS)
        return pl.ds(pl.multiple_of(x * ROWS + half * 32, 32), 32)

    def start_sum(self, phase, g, part, relay, landed):
        self.send(phase, 6 * g, part.at[g, 0, self.rows(self.far)], relay.at[phase, g, 0], self.next)
        self.send(phase, 6 * g + 1, part.at[g, 1, self.rows(self.far)], relay.at[phase, g, 1], self.prev)
        self.send(
            phase, 6 * g + 2, part.at[g, 1, self.rows(self.next)], landed.at[phase, g, 0, 1], self.next)
        self.send(
            phase, 6 * g + 3, part.at[g, 0, self.rows(self.prev)], landed.at[phase, g, 1, 0], self.prev)

    def pass_on(self, phase, g, part, relay, landed):
        for side, dev in ((0, self.next), (1, self.prev)):
            self.arrive(phase, 6 * g + side, relay.at[phase, g, side])
            total = relay[phase, g, side].astype(F32) + part[g, side, self.rows(dev)].astype(F32)
            relay[phase, g, side] = total.astype(BF16)
            self.send(
                phase, 6 * g + 4 + side, relay.at[phase, g, side], landed.at[phase, g, side, side], dev)

    def total(self, phase, g, part, landed):
        for slot, side, sub in ((2, 0, 1), (3, 1, 0), (4, 0, 0), (5, 1, 1)):
            self.arrive(phase, 6 * g + slot, landed.at[phase, g, side, sub])
        return [
            part[g, sub, self.rows(self.x)].astype(F32)
            + landed[phase, g, 0, sub].astype(F32)
            + landed[phase, g, 1, sub].astype(F32)
            for sub in range(2)
        ]

    def share(self, ref):
        top, bottom = (ref.at[self.rows(self.x, half)] for half in range(2))
        self.send(2, 0, top, top, self.next)
        self.send(2, 1, bottom, bottom, self.prev)
        self.send(2, 6, bottom, bottom, self.next)
        self.send(2, 7, top, top, self.prev)

    def share_on(self, ref):
        top, bottom = ref.at[self.rows(self.prev, 0)], ref.at[self.rows(self.next, 1)]
        self.arrive(2, 0, top)
        self.send(2, 2, top, top, self.next)
        self.arrive(2, 1, bottom)
        self.send(2, 3, bottom, bottom, self.prev)

    def shared(self, ref):
        self.arrive(2, 6, ref.at[self.rows(self.prev, 1)])
        self.arrive(2, 7, ref.at[self.rows(self.next, 0)])
        self.arrive(2, 2, ref.at[self.rows(self.far, 0)])
        self.arrive(2, 3, ref.at[self.rows(self.far, 1)])


QUARTER = D // 4
EARLY = [(0, 0), (1, 0), (2, 0), (0, 1), (0, 2), (1, 1), (1, 2), (2, 1)]
LATE = [(2, 2), (3, 0), (3, 1), (3, 2), (0, 3), (1, 3), (2, 3), (3, 3)]


def layer_kernel(
    u_hbm, a_hbm, pr_hbm, pi_hbm, sl_hbm, bre_hbm, bim_hbm, cre_hbm, cim_hbm,
    mix_gain_hbm, pre_gain_hbm, post_gain_hbm, wo_hbm, res_hbm, gate_hbm, up_hbm, down_hbm,
    out_ref,
    u_ref, a_ref, pr_ref, pi_ref, sl_ref, bre_ref, bim_ref, cre_ref, cim_ref,
    mix_gain_ref, pre_gain_ref, post_gain_ref, wo_ref, res_ref,
    e_ref, dr_ref, di_ref, act_ref, cs_ref, ea_ref, eb_ref, ra_ref, rb_ref, gu_ref, dn_ref,
    part_ref, relay_ref, landed_ref, rows_ref, hid_ref, sum_ref,
    sa, qa, sb, qb, ws, wq, xs, xq, ls, gs,
):
    sp = lax.axis_index("sp")
    tp = lax.axis_index("tp")
    q = sp % 8
    z = sp // 8
    peers_a = [z * 8 + (q + d) % 8 for d in range(1, 8)]
    peers_b = [((z + d) % 4) * 8 + q for d in range(1, 4)]
    weights = Gather((gu_ref, dn_ref), ws, wq, sp)
    across = Across(tp, xs, xq)
    own = pl.ds(pl.multiple_of(sp * ROWS, ROWS), ROWS)
    shard_loads = [
        pltpu.make_async_copy(hbm, gu_ref.at[own, pl.ds(side * F, F)], gs.at[side])
        for side, hbm in enumerate((gate_hbm, up_hbm))
    ]
    for load in shard_loads:
        load.start()
    barrier = pltpu.get_barrier_semaphore()
    for peer in peers_a + peers_b:
        pl.semaphore_signal(barrier, inc=1, device_id={"sp": peer}, device_id_type=MESH)
    for peer in (across.next, across.prev):
        pl.semaphore_signal(barrier, inc=1, device_id={"tp": peer}, device_id_type=MESH)
    pairs = (
        (pr_hbm, pr_ref), (pi_hbm, pi_ref), (sl_hbm, sl_ref), (a_hbm, a_ref), (u_hbm, u_ref),
        (bre_hbm, bre_ref), (bim_hbm, bim_ref), (cre_hbm, cre_ref), (cim_hbm, cim_ref),
        (wo_hbm, wo_ref), (res_hbm, res_ref), (mix_gain_hbm, mix_gain_ref),
        (pre_gain_hbm, pre_gain_ref), (post_gain_hbm, post_gain_ref), (down_hbm, dn_ref.at[own]),
    )
    loads = [pltpu.make_async_copy(src, dst, ls.at[k]) for k, (src, dst) in enumerate(pairs)]
    for load in loads[:4]:
        load.start()
    for load in loads[4:]:
        load.start()
    for load in shard_loads:
        load.wait()
    pl.semaphore_wait(barrier, 12)
    weights.own_along(0, weights.core, 0)
    weights.own_along(0, 1 - weights.core, 0)
    weights.own_along(0, 1 - weights.core, 1)
    weights.hand(0, 0, 0)
    for load in loads[:4]:
        load.wait()

    base_r, base_i, ratio_r, ratio_i, mine, row = step_rows(pr_ref[...], pi_ref[...], sl_ref[...])
    ea_row = jnp.exp(row(jnp.sum(a_ref[...], axis=1, keepdims=True)))
    put_row(ea_ref, 0, 0, ea_row)
    early = []
    for d in range(1, 8):
        early.append(pltpu.make_async_remote_copy(
            ea_ref.at[0], ea_ref.at[d], sa.at[0, d], qa.at[0, d],
            device_id={"sp": peers_a[d - 1]}, device_id_type=MESH))
        early[-1].start()

    perm = iota((T, T), 0) == (iota((T, T), 1) % SEGS) * STEPS + iota((T, T), 1) // SEGS
    order = iota((T, T), 1) == (iota((T, T), 0) % SEGS) * STEPS + iota((T, T), 0) // SEGS
    e_small = dot(thirds(jnp.exp(a_ref[...])), one_hot(perm, BF16)).astype(BF16)
    groups = one_hot(mine, BF16)
    e_ref[...] = lax.dot_general(
        e_small, jnp.concatenate([groups] * 3, axis=0), (((0,), (0,)), ((), ())),
        preferred_element_type=F32)
    for load in loads[4:9]:
        load.wait()
    u = dot(one_hot(order, BF16), u_ref[...]).astype(BF16)
    inside = iota((256, 1024), 0) // C == iota((256, 1024), 1) // N

    def spread(v):
        return jnp.where(inside, lanes_of(v, 1024), 0.0).astype(BF16)

    for h in range(2):
        gn = slice(h * 1024, (h + 1) * 1024)
        ch = slice(h * 256, (h + 1) * 256)
        raw_r = dot(u[:, ch], spread(bre_ref[ch, :]))
        raw_i = dot(u[:, ch], spread(bim_ref[ch, :]))
        rr, ri = ratio_r[:, gn], ratio_i[:, gn]
        dr_ref[:, gn] = rr * raw_r - ri * raw_i
        di_ref[:, gn] = rr * raw_i + ri * raw_r

    zero = jnp.zeros((SEGS, GN), F32)
    end_r, end_i, pe = scan_pass((base_r, base_i), e_ref, dr_ref, di_ref, (zero, zero), False)
    wr, wi = base_r, base_i
    for _ in range(5):
        wr, wi = cmul(wr, wi, wr, wi)
    seg_r, seg_i = wr * pe, wi * pe
    one_row = jnp.ones((1, GN), F32)
    no_row = jnp.zeros((1, GN), F32)
    total = (one_row, no_row, no_row, no_row)
    before = []
    for j in range(SEGS):
        before.append(total)
        total = link(total, (seg_r[j : j + 1], seg_i[j : j + 1], end_r[j : j + 1], end_i[j : j + 1]))
    put_row(ra_ref, 0, 0, total[2])
    put_row(ra_ref, 0, 1, total[3])

    sent_a = []
    for d in range(1, 8):
        sent_a.append(pltpu.make_async_remote_copy(
            ra_ref.at[0], ra_ref.at[d], sa.at[1, d], qa.at[1, d],
            device_id={"sp": peers_a[d - 1]}, device_id_type=MESH))
        sent_a[-1].start()
    weights.own_along(0, weights.core, 1)
    loads[14].wait()
    weights.own_along(1, weights.core, None)
    weights.hand(1, 0, 0)
    for h in range(2):
        ch = slice(h * 256, (h + 1) * 256)
        cs_ref[h, 0] = spread(cre_ref[ch, :])
        cs_ref[h, 1] = spread(-cim_ref[ch, :])
    w_r, w_i = to_block(wr), to_block(wi)
    for _ in range(3):
        w_r, w_i = cmul(w_r, w_i, w_r, w_i)
    v_r, v_i = w_r, w_i
    for _ in range(3):
        v_r, v_i = cmul(v_r, v_i, v_r, v_i)
    for copy in early:
        copy.wait()
    eb = ea_ref[0]
    for d in range(1, 8):
        eb = eb * ea_ref[d]
    eb_ref[0] = eb
    early_b = []
    for d in range(1, 4):
        early_b.append(pltpu.make_async_remote_copy(
            eb_ref.at[0], eb_ref.at[d], sb.at[0, d], qb.at[0, d],
            device_id={"sp": peers_b[d - 1]}, device_id_type=MESH))
        early_b[-1].start()
    for copy in sent_a:
        copy.wait()
    unit = jnp.ones((16, 128), F32)
    null = jnp.zeros((16, 128), F32)

    def stretch(e, pr, pi, ref, slot):
        block = ref[slot].astype(F32)
        decay = e[slot]
        return pr * decay, pi * decay, block[:16], block[16:]

    run = (unit, null, null, null)
    pre_a = run
    for k in range(8):
        pre_a = choose(q == k, run, pre_a)
        run = link(run, stretch(ea_ref, w_r, w_i, ra_ref, (q - k + 8) % 8))
    rb_ref[0, :16] = run[2].astype(BF16)
    rb_ref[0, 16:] = run[3].astype(BF16)
    sent_b = []
    for d in range(1, 4):
        sent_b.append(pltpu.make_async_remote_copy(
            rb_ref.at[0], rb_ref.at[d], sb.at[1, d], qb.at[1, d],
            device_id={"sp": peers_b[d - 1]}, device_id_type=MESH))
        sent_b[-1].start()
    weights.own_along(1, 1 - weights.core, None)
    weights.beyond_f_next()
    weights.beyond_f_prev()
    weights.along_s(0, 1)
    weights.along_s(0, 2)
    for copy in early_b + sent_b:
        copy.wait()
    run = (unit, null, null, null)
    pre_b = run
    for k in range(4):
        pre_b = choose(z == k, run, pre_b)
        run = link(run, stretch(eb_ref, v_r, v_i, rb_ref, (z - k + 4) % 4))
    carry = link(pre_b, pre_a)
    cr, ci = to_row(carry[2]), to_row(carry[3])
    starts = []
    for k in range(SEGS):
        pr, pi, sr, si = before[k]
        tr, ti = cmul(pr, pi, cr, ci)
        starts.append((tr + sr, ti + si))
    init = [jnp.concatenate([s[k] for s in starts], axis=0) for k in range(2)]
    scan_pass((base_r, base_i), e_ref, dr_ref, di_ref, init, True)

    for h in range(2):
        gn = slice(h * 1024, (h + 1) * 1024)
        y = dot_nt(dr_ref[:, gn].astype(BF16), cs_ref[h, 0])
        y = y + dot_nt(di_ref[:, gn].astype(BF16), cs_ref[h, 1])
        act_ref[:, h * 256 : (h + 1) * 256] = jax.nn.gelu(y).astype(BF16)
    act = dot(one_hot(perm, BF16), act_ref[...]).astype(BF16)
    loads[9].wait()
    for g in range(2):
        out = dot(act, wo_ref[:, g * HALF : (g + 1) * HALF]).astype(BF16)
        part_ref[0, g, 0] = out[:, :QUARTER]
        part_ref[0, g, 1] = out[:, QUARTER:]
        across.start_sum(0, g, part_ref.at[0], relay_ref, landed_ref)
    weights.beyond_s_own()
    across.pass_on(0, 0, part_ref.at[0], relay_ref, landed_ref)
    weights.opposite_f(0)
    weights.along_s(0, 3)
    across.pass_on(0, 1, part_ref.at[0], relay_ref, landed_ref)
    weights.beyond_s(0, 1)
    weights.beyond_f(1)
    mixed = jnp.concatenate(
        across.total(0, 0, part_ref.at[0], landed_ref)
        + across.total(0, 1, part_ref.at[0], landed_ref), axis=1)
    for load in loads[10:14]:
        load.wait()
    middle = (res_ref[...].astype(F32) + rms_scale(mixed, mix_gain_ref[...])).astype(BF16)
    res_ref[...] = middle
    normed = rms_scale(middle.astype(F32), pre_gain_ref[...]).astype(BF16)
    rows_ref[across.rows(tp), :] = normed
    across.share(rows_ref)
    weights.beyond_s(0, 2)
    across.share_on(rows_ref)
    weights.beyond_s(0, 3)
    weights.along_s(1, 1)
    weights.along_s(1, 2)
    weights.opposite_f(1)
    weights.along_s(1, 3)
    weights.beyond_s(1, 0)
    across.shared(rows_ref)
    weights.opposite_s(0)
    weights.handed(0, [(k, m) for k in range(4) for m in range(4)])
    def hidden_tile(gate, up, first):
        hidden = gate / (1.0 + jnp.exp(-gate)) * up
        hid_ref[first : first + gate.shape[1], :] = hidden.T.astype(BF16)

    for first in range(0, F - 128, 256):
        tile = [gu_ref[:, side * F + first : side * F + first + 256] for side in range(2)]
        hidden_tile(dot(rows_ref[...], tile[0]), dot(rows_ref[...], tile[1]), first)
        if first == 512:
            weights.beyond_s(1, 1)
    both = dot(rows_ref[...], jnp.concatenate([gu_ref[:, F - 128 : F], gu_ref[:, 2 * F - 128 :]], axis=1))
    hidden_tile(both[:, :128], both[:, 128:], F - 128)

    weights.beyond_s(1, 2)
    weights.beyond_s(1, 3)
    weights.handed(1, [(k, m) for k in range(3) for m in range(3)])
    for g, chips in enumerate((EARLY, LATE)):
        if g == 1:
            weights.opposite_s(1)
            weights.handed(1, [(k, m) for k in range(4) for m in range(4) if k == 3 or m == 3])
            across.pass_on(1, 0, part_ref.at[1], relay_ref, landed_ref)
        for sub in range(2):
            block = jnp.concatenate(
                [dn_ref[pl.ds(weights.columns(k, m), 128), :] for k, m in chips[4 * sub : 4 * sub + 4]],
                axis=0)
            out = dot(block, hid_ref[...])
            for i in range(4):
                part_ref[1, g, sub, :, i * 128 : (i + 1) * 128] = (
                    out[i * 128 : (i + 1) * 128].T.astype(BF16))
        across.start_sum(1, g, part_ref.at[1], relay_ref, landed_ref)
    across.pass_on(1, 1, part_ref.at[1], relay_ref, landed_ref)
    for g, chips in enumerate((EARLY, LATE)):
        sums = across.total(1, g, part_ref.at[1], landed_ref)
        for j, (k, m) in enumerate(chips):
            piece = sums[j // 4][:, (j % 4) * 128 : (j % 4 + 1) * 128]
            sum_ref[:, pl.ds(weights.columns(k, m), 128)] = piece
    merged = res_ref[...].astype(F32) + 0.5 * rms_scale(sum_ref[...], post_gain_ref[...])
    out_ref[...] = merged
    for copy in weights.started + across.started:
        copy.wait_send()


def layer(arrays):
    hbm = pl.BlockSpec(memory_space=pl.ANY)
    dma = pltpu.SemaphoreType.DMA
    held = [pltpu.VMEM(v.shape, v.dtype) for v in arrays[:14]]
    return pl.pallas_call(
        layer_kernel,
        out_shape=jax.ShapeDtypeStruct((ROWS, D), F32),
        in_specs=[hbm] * len(arrays),
        out_specs=pl.BlockSpec(memory_space=pltpu.VMEM),
        scratch_shapes=[
            *held,
            pltpu.VMEM((T, GN), F32),
            pltpu.VMEM((T, GN), F32),
            pltpu.VMEM((T, GN), F32),
            pltpu.VMEM((T, 512), BF16),
            pltpu.VMEM((2, 2, 256, 1024), BF16),
            pltpu.VMEM((8, 16, 128), F32),
            pltpu.VMEM((4, 16, 128), F32),
            pltpu.VMEM((8, 32, 128), BF16),
            pltpu.VMEM((4, 32, 128), BF16),
            pltpu.VMEM((D, 2 * F), BF16),
            pltpu.VMEM((D, F), BF16),
            pltpu.VMEM((2, 2, 2, T, QUARTER), BF16),
            pltpu.VMEM((2, 2, 2, ROWS, QUARTER), BF16),
            pltpu.VMEM((2, 2, 2, 2, ROWS, QUARTER), BF16),
            pltpu.VMEM((T, D), BF16),
            pltpu.VMEM((F, T), BF16),
            pltpu.VMEM((ROWS, D), F32),
            dma((2, 8)), dma((2, 8)), dma((2, 4)), dma((2, 4)),
            dma((2, 40)), dma((2, 40)), dma((3, 12)), dma((3, 12)), dma((15,)), dma((2,)),
        ],
        compiler_params=pltpu.CompilerParams(
            collective_id=0, has_side_effects=True, vmem_limit_bytes=66000000
        ),
        name="layer",
    )(*arrays)


def shards(
    residual, ssm_input, pole_real, pole_imaginary, step_log, input_real, entry_map_quadrature,
    output_real, output_imaginary, added_log_decay, out_weight, mix_gain, gate_weight, up_weight,
    down_weight, pre_gain, post_gain,
):
    small = (
        ssm_input, added_log_decay.T, pole_real, pole_imaginary, step_log.reshape(1, G),
        input_real.transpose(0, 2, 1).reshape(512, N),
        entry_map_quadrature.transpose(0, 2, 1).reshape(512, N),
        output_real.reshape(512, N), output_imaginary.reshape(512, N),
        mix_gain.reshape(1, D), pre_gain.reshape(1, D), post_gain.reshape(1, D),
    )
    return layer(small + (out_weight, residual, gate_weight, up_weight, down_weight)).astype(BF16)


def solution(mesh):
    return jax.shard_map(
        shards,
        mesh=mesh,
        in_specs=(
            P(("sp", "tp"), None), P("sp", "tp"), P("tp", None), P("tp", None), P("tp"),
            P("tp", None, None), P("tp", None, None), P("tp", None, None), P("tp", None, None),
            P("sp", "tp"), P("tp", None), P(), P("sp", "tp"), P("sp", "tp"), P("sp", "tp"),
            P(), P(),
        ),
        out_specs=P(("sp", "tp"), None),
        check_vma=False,
    )
```

```python
import functools

import jax
import jax.numpy as jnp
from jax import lax
from jax.experimental import pallas as pl
from jax.experimental.pallas import tpu as pltpu
from jax.sharding import PartitionSpec as P

EPSILON = 1e-06
EXACT = lax.Precision.HIGHEST
MESH = pl.DeviceIdType.MESH
F32 = jnp.float32
BF16 = jnp.bfloat16
T = 256
G = 32
N = 64
C = 16
GN = G * N
SEGS = 8
STEPS = T // SEGS
D = 2048
F = 1408
ROWS = 64
HALF = D // 2
TILES = F // 128


def dot(a, b, **kw):
    return jnp.dot(a, b, preferred_element_type=F32, **kw)


def dot_nt(a, b):
    return lax.dot_general(a, b, (((1,), (1,)), ((), ())), preferred_element_type=F32)


def iota(shape, dim):
    return lax.broadcasted_iota(jnp.int32, shape, dim)


def one_hot(mask, dtype):
    return jnp.where(mask, 1.0, 0.0).astype(dtype)


def cmul(ar, ai, br, bi):
    return ar * br - ai * bi, ar * bi + ai * br


def split(v):
    hi = v.astype(BF16)
    return hi, (v - hi.astype(F32)).astype(BF16)


def expm1(x):
    p = 1.0 / 40320.0
    for k in (5040.0, 720.0, 120.0, 24.0, 6.0, 2.0, 1.0):
        p = p * x + 1.0 / k
    return jnp.where(x > -0.5, p * x, jnp.exp(x) - 1.0)


def lanes_of(v, count):
    pair = jnp.concatenate([v, v], axis=1)
    return jnp.concatenate([pair] * (count // 128), axis=1)


def step_rows(pr, pi, sl, row):
    same = iota((G, G), 0) == iota((G, G), 1)
    column = jnp.sum(jnp.where(same, jnp.broadcast_to(sl, (G, G)), 0.0), axis=1, keepdims=True)
    pr, pi, step = row(lanes_of(pr, GN)), row(lanes_of(pi, GN)), jnp.exp(row(column))
    log_size = pr * step
    angle = pi * step
    cosine, sine = jnp.cos(angle), jnp.sin(angle)
    size = jnp.exp(log_size)
    half = jnp.sin(0.5 * angle)
    lift_r = expm1(log_size) * cosine - 2.0 * half * half
    lift_i = size * sine
    inv = 1.0 / (pr * pr + pi * pi)
    ratio_r = (lift_r * pr + lift_i * pi) * inv
    ratio_i = (lift_i * pr - lift_r * pi) * inv
    return size * cosine, size * sine, ratio_r, ratio_i


def thirds(v):
    hi = v.astype(BF16)
    rest = v - hi.astype(F32)
    mid = rest.astype(BF16)
    return jnp.concatenate([hi, mid, (rest - mid.astype(F32)).astype(BF16)], axis=0)


def scan_pass(base, e_ref, dr_ref, di_ref, init, store):
    ends = []
    width = GN // 4
    for lc in range(4):
        sl = slice(lc * width, (lc + 1) * width)
        br = jnp.broadcast_to(base[0][:, sl], (SEGS, width))
        bi = jnp.broadcast_to(base[1][:, sl], (SEGS, width))

        def body(i, st):
            sr, si, pe = st
            rows = pl.ds(pl.multiple_of(i * SEGS, SEGS), SEGS)
            e = e_ref[rows, sl]
            ar, ai = br * e, bi * e
            nr = ar * sr - ai * si + dr_ref[rows, sl]
            ni = ar * si + ai * sr + di_ref[rows, sl]
            if store:
                dr_ref[rows, sl] = nr
                di_ref[rows, sl] = ni
                return nr, ni, pe
            return nr, ni, pe * e

        st = (init[0][:, sl], init[1][:, sl], jnp.ones((SEGS, width), F32))
        ends.append(lax.fori_loop(0, STEPS, body, st, unroll=4))
    return [jnp.concatenate([p[k] for p in ends], axis=1) for k in range(3)]


def put_row(ref, slot, part, row):
    for k in range(16):
        ref[slot, part * 16 + k : part * 16 + k + 1, :] = row[:, k * 128 : (k + 1) * 128].astype(ref.dtype)


def to_block(row):
    return jnp.concatenate([row[:, k * 128 : (k + 1) * 128] for k in range(16)], axis=0)


def to_row(block):
    return jnp.concatenate([block[k : k + 1, :] for k in range(16)], axis=1)


def link(first, then):
    ar, ai, sr, si = first
    br, bi, tr, ti = then
    pr, pi = cmul(br, bi, ar, ai)
    ur, ui = cmul(br, bi, sr, si)
    return pr, pi, ur + tr, ui + ti


def choose(cond, a, b):
    return tuple(jnp.where(cond, x, y) for x, y in zip(a, b))


def rms_scale(values, gain):
    return values * lax.rsqrt(jnp.mean(values * values, axis=-1, keepdims=True) + EPSILON) * gain


class Gather:
    def __init__(self, refs, send, recv, sp):
        self.refs, self.send_sem, self.recv_sem = refs, send, recv
        core, y, z = sp % 2, (sp // 2) % 4, sp // 8
        self.core = core
        self.fm, self.sm = 1 + 3 * core, 4 - 3 * core
        f = y + core * (z - y)
        s = z + core * (y - z)
        self.fk = [f, (f + 3) % 4, (f + 1) % 4, (f + 2) % 4]
        self.sk = [s, (s + 3) % 4, (s + 1) % 4, (s + 2) % 4]
        self.f_next, self.f_prev = self.place(2, 0), self.place(1, 0)
        self.s_next, self.s_prev = self.place(0, 2), self.place(0, 1)
        self.partner = sp + 1 - 2 * core

    def place(self, k, m):
        return 2 * (self.fk[k] * self.fm + self.sk[m] * self.sm) + self.core

    def block(self, p, k, m, half=None):
        start = self.place(k, m) * ROWS
        return self.rows(p, start, half)

    def rows(self, p, start, half):
        if half is None:
            return self.refs[p].at[pl.ds(pl.multiple_of(start, ROWS), ROWS)]
        return self.refs[p].at[pl.ds(pl.multiple_of(start + half * 32, 32), 32)]

    def copy(self, p, sem, ref, dev):
        return pltpu.make_async_remote_copy(
            ref, ref, self.send_sem.at[p], self.recv_sem.at[p, sem],
            device_id={"sp": dev}, device_id_type=MESH)

    def send(self, p, sem, ref, dev):
        self.copy(p, sem, ref, dev).start()

    def arrive(self, p, sem, rows):
        self.copy(p, sem, self.refs[p].at[pl.ds(0, rows)], self.partner).wait_recv()

    def drain(self):
        for p in range(2):
            self.copy(p, 0, self.refs[p].at[pl.ds(0, 1984)], self.partner).wait_send()

    def hand(self, p, k, m):
        late = p == 1 and (k == 3 or m == 3)
        self.send(p, 1 if late else 11, self.block(p, k, m), self.partner)

    def handed(self, p, sem, count):
        self.arrive(p, sem, count * ROWS)

    def own_along(self, p, turn, half):
        own = self.block(p, 0, 0, half)
        nexts, prevs = (self.f_next, self.s_next), (self.f_prev, self.s_prev)
        for side, (f_dev, s_dev) in enumerate((nexts, prevs)):
            f_sem = 0 if p == 1 or (half == 0 and side == 0) else 1
            self.send(p, f_sem + turn * (3 - f_sem), own, f_dev + turn * (s_dev - f_dev))

    def beyond_f(self, p):
        self.arrive(p, 0, 128)
        self.send(p, 2, self.block(p, 1, 0, 0), self.f_next)
        self.send(p, 2, self.block(p, 2, 0, 1), self.f_prev)

    def beyond_f_next(self):
        self.arrive(0, 0, 32)
        self.send(0, 2, self.block(0, 1, 0, 0), self.f_next)

    def beyond_f_prev(self):
        self.arrive(0, 1, 96)
        self.send(0, 2, self.block(0, 2, 0, 1), self.f_prev)

    def opposite_f(self, p):
        self.arrive(p, 2, 64)

    def beyond_s_own(self):
        self.beyond_s(0, 0)

    def along_s(self, p, k):
        ref = self.block(p, k, 0)
        self.send(p, 3 + k, ref, self.s_next)
        self.send(p, 3 + k, ref, self.s_prev)
        self.hand(p, k, 0)

    def beyond_s(self, p, k):
        self.arrive(p, 3 + k, 128)
        self.send(p, 7 + k, self.block(p, k, 1, 0), self.s_next)
        self.send(p, 7 + k, self.block(p, k, 2, 1), self.s_prev)
        self.hand(p, k, 1)
        self.hand(p, k, 2)

    def opposite_s(self, p, k):
        self.arrive(p, 7 + k, 64)
        self.hand(p, k, 3)

    def columns(self, k, m):
        return pl.multiple_of((self.fk[k] * self.fm + self.sk[m] * self.sm) * 128, 128)


class Across:
    def __init__(self, x, send, recv):
        self.x, self.send_sem, self.recv_sem = x, send, recv
        self.next, self.prev, self.far = (x + 1) % 4, (x + 3) % 4, (x + 2) % 4

    def copy(self, phase, sem, src, dst, dev):
        return pltpu.make_async_remote_copy(
            src, dst, self.send_sem.at[phase], self.recv_sem.at[phase, sem],
            device_id={"tp": dev}, device_id_type=MESH)

    def send(self, phase, sem, src, dst, dev):
        self.copy(phase, sem, src, dst, dev).start()

    def arrive(self, phase, sem, ref):
        self.copy(phase, sem, ref, ref, self.next).wait_recv()

    def drain(self, phase, ref):
        self.copy(phase, 0, ref, ref, self.next).wait_send()

    def rows(self, x, half=None):
        if half is None:
            return pl.ds(pl.multiple_of(x * ROWS, ROWS), ROWS)
        return pl.ds(pl.multiple_of(x * ROWS + half * 32, 32), 32)

    def start_relay(self, phase, g, part, relay):
        self.send(phase, g, part.at[g, 0, self.rows(self.far)], relay.at[phase, g, 0], self.next)
        self.send(phase, g, part.at[g, 1, self.rows(self.far)], relay.at[phase, g, 1], self.prev)

    def start_own(self, phase, g, part, landed):
        self.send(
            phase, 2 + g, part.at[g, 1, self.rows(self.next)], landed.at[phase, g, 0, 1], self.next)
        self.send(
            phase, 2 + g, part.at[g, 0, self.rows(self.prev)], landed.at[phase, g, 1, 0], self.prev)

    def pass_on(self, phase, g, part, relay, landed):
        self.arrive(phase, g, relay.at[phase, g])
        for side, dev in ((0, self.next), (1, self.prev)):
            total = relay[phase, g, side].astype(F32) + part[g, side, self.rows(dev)].astype(F32)
            relay[phase, g, side] = total.astype(BF16)
            self.send(phase, 2 + g, relay.at[phase, g, side], landed.at[phase, g, side, side], dev)

    def total(self, phase, g, part, landed):
        self.arrive(phase, 2 + g, landed.at[phase, g])
        return [
            part[g, sub, self.rows(self.x)].astype(F32)
            + landed[phase, g, 0, sub].astype(F32)
            + landed[phase, g, 1, sub].astype(F32)
            for sub in range(2)
        ]

    def share(self, ref):
        top, bottom = (ref.at[self.rows(self.x, half)] for half in range(2))
        self.send(2, 0, top, top, self.next)
        self.send(2, 1, bottom, bottom, self.prev)
        self.send(2, 2, bottom, bottom, self.next)
        self.send(2, 2, top, top, self.prev)

    def share_on(self, ref):
        top, bottom = ref.at[self.rows(self.prev, 0)], ref.at[self.rows(self.next, 1)]
        self.arrive(2, 0, top)
        self.send(2, 2, top, top, self.next)
        self.arrive(2, 1, bottom)
        self.send(2, 2, bottom, bottom, self.prev)

    def shared(self, ref):
        self.arrive(2, 2, ref.at[pl.ds(0, 128)])


QUARTER = D // 4
EARLY = [(0, 0), (1, 0), (2, 0), (0, 1), (0, 2), (1, 1), (1, 2), (2, 1)]
LATE = [(2, 2), (3, 0), (3, 1), (3, 2), (0, 3), (1, 3), (2, 3), (3, 3)]


def layer_kernel(
    u_hbm, a_hbm, pr_hbm, pi_hbm, sl_hbm, bre_hbm, bim_hbm, cre_hbm, cim_hbm,
    mix_gain_hbm, pre_gain_hbm, post_gain_hbm, wo_hbm, res_hbm, gate_hbm, up_hbm, down_hbm,
    out_ref,
    u_ref, a_ref, poles_ref, sl_ref, maps_ref, gains_ref, wo_ref, res_ref,
    e_ref, dr_ref, di_ref, act_ref, read_ref, ea_ref, eb_ref, ra_ref, rb_ref, gu_ref, dn_ref,
    part_ref, relay_ref, landed_ref, rows_ref, hid_ref, sum_ref,
    cs, cq, ws, wq, xs, xq, ls,
):
    sp = lax.axis_index("sp")
    tp = lax.axis_index("tp")
    q = sp % 8
    z = sp // 8
    peers_a = [z * 8 + (q + d) % 8 for d in range(1, 8)]
    peers_b = [((z + d) % 4) * 8 + q for d in range(1, 4)]
    weights = Gather((gu_ref, dn_ref), ws, wq, sp)
    across = Across(tp, xs, xq)
    own = pl.ds(pl.multiple_of(sp * ROWS, ROWS), ROWS)
    for side, hbm in enumerate((gate_hbm, up_hbm)):
        pltpu.make_async_copy(hbm, gu_ref.at[own, pl.ds(side * F, F)], ls.at[0]).start()
    barrier = pltpu.get_barrier_semaphore()
    for peer in peers_a + peers_b:
        pl.semaphore_signal(barrier, inc=1, device_id={"sp": peer}, device_id_type=MESH)
    for peer in (across.next, across.prev):
        pl.semaphore_signal(barrier, inc=1, device_id={"tp": peer}, device_id_type=MESH)
    pairs = (
        (a_hbm, a_ref, 1), (pr_hbm, poles_ref.at[0], 2), (pi_hbm, poles_ref.at[1], 2),
        (sl_hbm, sl_ref, 3), (u_hbm, u_ref, 4),
        (bre_hbm, maps_ref.at[0], 5), (bim_hbm, maps_ref.at[1], 5),
        (cre_hbm, maps_ref.at[2], 5), (cim_hbm, maps_ref.at[3], 5),
        (wo_hbm, wo_ref, 6), (res_hbm, res_ref, 7), (mix_gain_hbm, gains_ref.at[0], 8),
        (pre_gain_hbm, gains_ref.at[1], 8), (post_gain_hbm, gains_ref.at[2], 8),
        (down_hbm, dn_ref.at[own], 9),
    )
    for src, dst, sem in pairs:
        pltpu.make_async_copy(src, dst, ls.at[sem]).start()

    def loaded(ref, sem):
        pltpu.make_async_copy(ref, ref, ls.at[sem]).wait()

    mine = iota((G, GN), 1) // N == iota((G, GN), 0)

    def row(v):
        return jnp.sum(jnp.where(mine, v, 0.0), axis=0, keepdims=True)

    loaded(a_ref, 1)
    put_row(ea_ref, 0, 0, jnp.exp(row(jnp.sum(a_ref[...], axis=1, keepdims=True))))
    loaded(gu_ref.at[own], 0)
    pl.semaphore_wait(barrier, 12)

    def to_all(ref, peers, sem):
        for d, peer in enumerate(peers, 1):
            pltpu.make_async_remote_copy(
                ref.at[0], ref.at[d], cs.at[sem], cq.at[sem],
                device_id={"sp": peer}, device_id_type=MESH).start()

    def from_all(ref, peers, sem):
        others = ref.at[pl.ds(1, len(peers))]
        pltpu.make_async_remote_copy(
            others, others, cs.at[sem], cq.at[sem],
            device_id={"sp": peers[0]}, device_id_type=MESH).wait()

    to_all(ea_ref, peers_a, 0)
    weights.own_along(0, weights.core, 0)
    weights.own_along(0, 1 - weights.core, 0)
    weights.own_along(0, 1 - weights.core, 1)
    weights.hand(0, 0, 0)
    loaded(poles_ref, 2)
    loaded(sl_ref, 3)

    base_r, base_i, ratio_r, ratio_i = step_rows(poles_ref[0], poles_ref[1], sl_ref[...], row)

    perm = iota((T, T), 0) == (iota((T, T), 1) % SEGS) * STEPS + iota((T, T), 1) // SEGS
    order = iota((T, T), 1) == (iota((T, T), 0) % SEGS) * STEPS + iota((T, T), 0) // SEGS
    e_small = dot(thirds(jnp.exp(a_ref[...])), one_hot(perm, BF16)).astype(BF16)
    groups = one_hot(mine, BF16)
    e_ref[...] = lax.dot_general(
        e_small, jnp.concatenate([groups] * 3, axis=0), (((0,), (0,)), ((), ())),
        preferred_element_type=F32)
    loaded(u_ref, 4)
    loaded(maps_ref, 5)
    u = dot(one_hot(order, BF16), u_ref[...]).astype(BF16)
    inside = iota((256, 1024), 0) // C == iota((256, 1024), 1) // N

    def spread(v):
        return jnp.where(inside, lanes_of(v, 1024), 0.0).astype(BF16)

    for h in range(2):
        gn = slice(h * 1024, (h + 1) * 1024)
        ch = slice(h * 256, (h + 1) * 256)
        raw_r = dot(u[:, ch], spread(maps_ref[0, ch, :]))
        raw_i = dot(u[:, ch], spread(maps_ref[1, ch, :]))
        rr, ri = ratio_r[:, gn], ratio_i[:, gn]
        dr_ref[:, gn] = rr * raw_r - ri * raw_i
        di_ref[:, gn] = rr * raw_i + ri * raw_r

    zero = jnp.zeros((SEGS, GN), F32)
    end_r, end_i, pe = scan_pass((base_r, base_i), e_ref, dr_ref, di_ref, (zero, zero), False)
    wr, wi = base_r, base_i
    for _ in range(5):
        wr, wi = cmul(wr, wi, wr, wi)
    seg_r, seg_i = wr * pe, wi * pe
    one_row = jnp.ones((1, GN), F32)
    no_row = jnp.zeros((1, GN), F32)
    total = (one_row, no_row, no_row, no_row)
    before = []
    for j in range(SEGS):
        before.append(total)
        total = link(total, (seg_r[j : j + 1], seg_i[j : j + 1], end_r[j : j + 1], end_i[j : j + 1]))
    put_row(ra_ref, 0, 0, total[2])
    put_row(ra_ref, 0, 1, total[3])

    to_all(ra_ref, peers_a, 1)
    weights.own_along(0, weights.core, 1)
    loaded(dn_ref.at[own], 9)
    weights.own_along(1, weights.core, None)
    weights.hand(1, 0, 0)
    for h in range(2):
        ch = slice(h * 256, (h + 1) * 256)
        read_ref[h, 0] = spread(maps_ref[2, ch, :])
        read_ref[h, 1] = spread(-maps_ref[3, ch, :])
    w_r, w_i = to_block(wr), to_block(wi)
    for _ in range(3):
        w_r, w_i = cmul(w_r, w_i, w_r, w_i)
    v_r, v_i = w_r, w_i
    for _ in range(3):
        v_r, v_i = cmul(v_r, v_i, v_r, v_i)
    from_all(ea_ref, peers_a, 0)
    eb = ea_ref[0]
    for d in range(1, 8):
        eb = eb * ea_ref[d]
    eb_ref[0] = eb
    to_all(eb_ref, peers_b, 2)
    from_all(ra_ref, peers_a, 1)
    unit = jnp.ones((16, 128), F32)
    null = jnp.zeros((16, 128), F32)

    def stretch(e, pr, pi, ref, slot):
        block = ref[slot].astype(F32)
        decay = e[slot]
        return pr * decay, pi * decay, block[:16], block[16:]

    run = (unit, null, null, null)
    pre_a = run
    for k in range(8):
        pre_a = choose(q == k, run, pre_a)
        run = link(run, stretch(ea_ref, w_r, w_i, ra_ref, (q - k + 8) % 8))
    rb_ref[0, :16] = run[2].astype(BF16)
    rb_ref[0, 16:] = run[3].astype(BF16)
    to_all(rb_ref, peers_b, 3)
    weights.own_along(1, 1 - weights.core, None)
    weights.beyond_f_next()
    weights.beyond_f_prev()
    weights.along_s(0, 1)
    weights.along_s(0, 2)
    from_all(eb_ref, peers_b, 2)
    from_all(rb_ref, peers_b, 3)
    run = (unit, null, null, null)
    pre_b = run
    for k in range(4):
        pre_b = choose(z == k, run, pre_b)
        run = link(run, stretch(eb_ref, v_r, v_i, rb_ref, (z - k + 4) % 4))
    carry = link(pre_b, pre_a)
    cr, ci = to_row(carry[2]), to_row(carry[3])
    starts = []
    for k in range(SEGS):
        pr, pi, sr, si = before[k]
        tr, ti = cmul(pr, pi, cr, ci)
        starts.append((tr + sr, ti + si))
    init = [jnp.concatenate([s[k] for s in starts], axis=0) for k in range(2)]
    scan_pass((base_r, base_i), e_ref, dr_ref, di_ref, init, True)

    for h in range(2):
        gn = slice(h * 1024, (h + 1) * 1024)
        y = dot_nt(dr_ref[:, gn].astype(BF16), read_ref[h, 0])
        y = y + dot_nt(di_ref[:, gn].astype(BF16), read_ref[h, 1])
        act_ref[:, h * 256 : (h + 1) * 256] = jax.nn.gelu(y).astype(BF16)
    act = dot(one_hot(perm, BF16), act_ref[...]).astype(BF16)
    loaded(wo_ref, 6)
    for g in range(2):
        out = dot(act, wo_ref[:, g * HALF : (g + 1) * HALF]).astype(BF16)
        part_ref[0, g, 0] = out[:, :QUARTER]
        part_ref[0, g, 1] = out[:, QUARTER:]
        across.start_relay(0, g, part_ref.at[0], relay_ref)
        across.start_own(0, g, part_ref.at[0], landed_ref)
    weights.beyond_s_own()
    across.pass_on(0, 0, part_ref.at[0], relay_ref, landed_ref)
    weights.opposite_f(0)
    weights.along_s(0, 3)
    across.pass_on(0, 1, part_ref.at[0], relay_ref, landed_ref)
    weights.beyond_s(0, 1)
    weights.beyond_f(1)
    mixed = jnp.concatenate(
        across.total(0, 0, part_ref.at[0], landed_ref)
        + across.total(0, 1, part_ref.at[0], landed_ref), axis=1)
    loaded(res_ref, 7)
    loaded(gains_ref, 8)
    middle = (res_ref[...].astype(F32) + rms_scale(mixed, gains_ref[0])).astype(BF16)
    res_ref[...] = middle
    normed = rms_scale(middle.astype(F32), gains_ref[1]).astype(BF16)
    rows_ref[across.rows(tp), :] = normed
    across.share(rows_ref)
    weights.beyond_s(0, 2)
    across.share_on(rows_ref)
    weights.beyond_s(0, 3)
    weights.along_s(1, 1)
    weights.along_s(1, 2)
    weights.opposite_f(1)
    weights.along_s(1, 3)
    weights.beyond_s(1, 0)
    across.shared(rows_ref)
    for k in range(4):
        weights.opposite_s(0, k)
    weights.handed(0, 11, 16)
    def hidden_tile(gate, up, first):
        hidden = gate / (1.0 + jnp.exp(-gate)) * up
        hid_ref[first : first + gate.shape[1], :] = hidden.T.astype(BF16)

    for first in range(0, F - 128, 256):
        tile = [gu_ref[:, side * F + first : side * F + first + 256] for side in range(2)]
        hidden_tile(dot(rows_ref[...], tile[0]), dot(rows_ref[...], tile[1]), first)
        if first in (256, 1024):
            weights.beyond_s(1, 1 if first == 256 else 2)
    both = dot(rows_ref[...], jnp.concatenate([gu_ref[:, F - 128 : F], gu_ref[:, 2 * F - 128 :]], axis=1))
    hidden_tile(both[:, :128], both[:, 128:], F - 128)

    weights.beyond_s(1, 3)
    weights.handed(1, 11, 9)
    for g, chips in enumerate((EARLY, LATE)):
        if g == 1:
            for i in range(4):
                weights.opposite_s(1, i)
            weights.handed(1, 1, 7)
        for sub in range(2):
            block = jnp.concatenate(
                [dn_ref[pl.ds(weights.columns(k, m), 128), :] for k, m in chips[4 * sub : 4 * sub + 4]],
                axis=0)
            out = dot(block, hid_ref[...])
            for i in range(4):
                part_ref[1, g, sub, :, i * 128 : (i + 1) * 128] = (
                    out[i * 128 : (i + 1) * 128].T.astype(BF16))
        across.start_relay(1, g, part_ref.at[1], relay_ref)
        if g == 1:
            across.pass_on(1, 0, part_ref.at[1], relay_ref, landed_ref)
        across.start_own(1, g, part_ref.at[1], landed_ref)
    across.pass_on(1, 1, part_ref.at[1], relay_ref, landed_ref)
    for g, chips in enumerate((EARLY, LATE)):
        sums = across.total(1, g, part_ref.at[1], landed_ref)
        for j, (k, m) in enumerate(chips):
            piece = sums[j // 4][:, (j % 4) * 128 : (j % 4 + 1) * 128]
            sum_ref[:, pl.ds(weights.columns(k, m), 128)] = piece
    merged = res_ref[...].astype(F32) + 0.5 * rms_scale(sum_ref[...], gains_ref[2])
    out_ref[...] = merged.astype(BF16)
    weights.drain()
    across.drain(0, part_ref.at[0, :, :, pl.ds(0, 192)])
    across.drain(1, part_ref.at[1, :, :, pl.ds(0, 192)])
    across.drain(2, rows_ref.at[pl.ds(0, 192)])


def layer(arrays):
    hbm = pl.BlockSpec(memory_space=pl.ANY)
    dma = pltpu.SemaphoreType.DMA
    return pl.pallas_call(
        layer_kernel,
        out_shape=jax.ShapeDtypeStruct((ROWS, D), BF16),
        in_specs=[hbm] * len(arrays),
        out_specs=pl.BlockSpec(memory_space=pltpu.VMEM),
        scratch_shapes=[
            pltpu.VMEM((T, 512), BF16),
            pltpu.VMEM((G, T), F32),
            pltpu.VMEM((2, G, N), F32),
            pltpu.VMEM((1, G), F32),
            pltpu.VMEM((4, 512, N), F32),
            pltpu.VMEM((3, 1, D), F32),
            pltpu.VMEM((512, D), BF16),
            pltpu.VMEM((ROWS, D), BF16),
            pltpu.VMEM((T, GN), F32),
            pltpu.VMEM((T, GN), F32),
            pltpu.VMEM((T, GN), F32),
            pltpu.VMEM((T, 512), BF16),
            pltpu.VMEM((2, 2, 256, 1024), BF16),
            pltpu.VMEM((8, 16, 128), F32),
            pltpu.VMEM((4, 16, 128), F32),
            pltpu.VMEM((8, 32, 128), BF16),
            pltpu.VMEM((4, 32, 128), BF16),
            pltpu.VMEM((D, 2 * F), BF16),
            pltpu.VMEM((D, F), BF16),
            pltpu.VMEM((2, 2, 2, T, QUARTER), BF16),
            pltpu.VMEM((2, 2, 2, ROWS, QUARTER), BF16),
            pltpu.VMEM((2, 2, 2, 2, ROWS, QUARTER), BF16),
            pltpu.VMEM((T, D), BF16),
            pltpu.VMEM((F, T), BF16),
            pltpu.VMEM((ROWS, D), F32),
            dma((4,)), dma((4,)), dma((2,)), dma((2, 12)), dma((3,)), dma((3, 4)), dma((10,)),
        ],
        compiler_params=pltpu.CompilerParams(
            collective_id=0, has_side_effects=True, vmem_limit_bytes=66000000
        ),
        name="layer",
    )(*arrays)


def shards(
    residual, ssm_input, pole_real, pole_imaginary, step_log, input_real, entry_map_quadrature,
    output_real, output_imaginary, added_log_decay, out_weight, mix_gain, gate_weight, up_weight,
    down_weight, pre_gain, post_gain,
):
    small = (
        ssm_input, added_log_decay.T, pole_real, pole_imaginary, step_log.reshape(1, G),
        input_real.transpose(0, 2, 1).reshape(512, N),
        entry_map_quadrature.transpose(0, 2, 1).reshape(512, N),
        output_real.reshape(512, N), output_imaginary.reshape(512, N),
        mix_gain.reshape(1, D), pre_gain.reshape(1, D), post_gain.reshape(1, D),
    )
    return layer(small + (out_weight, residual, gate_weight, up_weight, down_weight))


def solution(mesh):
    return jax.shard_map(
        shards,
        mesh=mesh,
        in_specs=(
            P(("sp", "tp"), None), P("sp", "tp"), P("tp", None), P("tp", None), P("tp"),
            P("tp", None, None), P("tp", None, None), P("tp", None, None), P("tp", None, None),
            P("sp", "tp"), P("tp", None), P(), P("sp", "tp"), P("sp", "tp"), P("sp", "tp"),
            P(), P(),
        ),
        out_specs=P(("sp", "tp"), None),
        check_vma=False,
    )
```

```python
import functools

import jax
import jax.numpy as jnp
from jax import lax
from jax.experimental import pallas as pl
from jax.experimental.pallas import tpu as pltpu
from jax.sharding import PartitionSpec as P

EPSILON = 1e-06
EXACT = lax.Precision.HIGHEST
MESH = pl.DeviceIdType.MESH
F32 = jnp.float32
BF16 = jnp.bfloat16
T = 256
G = 32
N = 64
C = 16
GN = G * N
SEGS = 8
STEPS = T // SEGS
D = 2048
F = 1408
ROWS = 64
HALF = D // 2
TILES = F // 128


def dot(a, b, **kw):
    return jnp.dot(a, b, preferred_element_type=F32, **kw)


def dot_nt(a, b):
    return lax.dot_general(a, b, (((1,), (1,)), ((), ())), preferred_element_type=F32)


def iota(shape, dim):
    return lax.broadcasted_iota(jnp.int32, shape, dim)


def one_hot(mask, dtype):
    return jnp.where(mask, 1.0, 0.0).astype(dtype)


def cmul(ar, ai, br, bi):
    return ar * br - ai * bi, ar * bi + ai * br


def split(v):
    hi = v.astype(BF16)
    return hi, (v - hi.astype(F32)).astype(BF16)


def expm1(x):
    p = 1.0 / 40320.0
    for k in (5040.0, 720.0, 120.0, 24.0, 6.0, 2.0, 1.0):
        p = p * x + 1.0 / k
    return jnp.where(x > -0.5, p * x, jnp.exp(x) - 1.0)


def lanes_of(v, count):
    pair = jnp.concatenate([v, v], axis=1)
    return jnp.concatenate([pair] * (count // 128), axis=1)


def step_rows(pr, pi, sl, row):
    same = iota((G, G), 0) == iota((G, G), 1)
    column = jnp.sum(jnp.where(same, jnp.broadcast_to(sl, (G, G)), 0.0), axis=1, keepdims=True)
    pr, pi, step = row(lanes_of(pr, GN)), row(lanes_of(pi, GN)), jnp.exp(row(column))
    log_size = pr * step
    angle = pi * step
    cosine, sine = jnp.cos(angle), jnp.sin(angle)
    size = jnp.exp(log_size)
    half = jnp.sin(0.5 * angle)
    lift_r = expm1(log_size) * cosine - 2.0 * half * half
    lift_i = size * sine
    inv = 1.0 / (pr * pr + pi * pi)
    ratio_r = (lift_r * pr + lift_i * pi) * inv
    ratio_i = (lift_i * pr - lift_r * pi) * inv
    return size * cosine, size * sine, ratio_r, ratio_i


def thirds(v):
    hi = v.astype(BF16)
    rest = v - hi.astype(F32)
    mid = rest.astype(BF16)
    return jnp.concatenate([hi, mid, (rest - mid.astype(F32)).astype(BF16)], axis=0)


def scan_pass(base, e_ref, dr_ref, di_ref, init, store):
    ends = []
    width = GN // 4
    for lc in range(4):
        sl = slice(lc * width, (lc + 1) * width)
        br = jnp.broadcast_to(base[0][:, sl], (SEGS, width))
        bi = jnp.broadcast_to(base[1][:, sl], (SEGS, width))

        def body(i, st):
            sr, si, pe = st
            rows = pl.ds(pl.multiple_of(i * SEGS, SEGS), SEGS)
            e = e_ref[rows, sl]
            ar, ai = br * e, bi * e
            nr = ar * sr - ai * si + dr_ref[rows, sl]
            ni = ar * si + ai * sr + di_ref[rows, sl]
            if store:
                dr_ref[rows, sl] = nr
                di_ref[rows, sl] = ni
                return nr, ni, pe
            return nr, ni, pe * e

        st = (init[0][:, sl], init[1][:, sl], jnp.ones((SEGS, width), F32))
        ends.append(lax.fori_loop(0, STEPS, body, st, unroll=4))
    return [jnp.concatenate([p[k] for p in ends], axis=1) for k in range(3)]


def put_row(ref, slot, part, row):
    for k in range(16):
        ref[slot, part * 16 + k : part * 16 + k + 1, :] = row[:, k * 128 : (k + 1) * 128].astype(ref.dtype)


def to_block(row):
    return jnp.concatenate([row[:, k * 128 : (k + 1) * 128] for k in range(16)], axis=0)


def to_row(block):
    return jnp.concatenate([block[k : k + 1, :] for k in range(16)], axis=1)


def link(first, then):
    ar, ai, sr, si = first
    br, bi, tr, ti = then
    pr, pi = cmul(br, bi, ar, ai)
    ur, ui = cmul(br, bi, sr, si)
    return pr, pi, ur + tr, ui + ti


def choose(cond, a, b):
    return tuple(jnp.where(cond, x, y) for x, y in zip(a, b))


def rms_scale(values, gain):
    return values * lax.rsqrt(jnp.mean(values * values, axis=-1, keepdims=True) + EPSILON) * gain


CHIPS = (
    ((0, 0), (0, 1), (1, 0), (0, 2)),
    ((2, 0), (1, 1), (1, 2), (2, 1)),
    ((2, 2), (3, 0), (0, 3), (1, 3)),
    ((3, 1), (2, 3), (3, 2), (3, 3)),
)
GROUP_SEMS = (11, 1, 12, 13)


class Gather:
    def __init__(self, refs, send, recv, sp):
        self.refs, self.send_sem, self.recv_sem = refs, send, recv
        core, y, z = sp % 2, (sp // 2) % 4, sp // 8
        self.core = core
        self.fm, self.sm = 1 + 3 * core, 4 - 3 * core
        f = y + core * (z - y)
        s = z + core * (y - z)
        self.fk = [f, (f + 3) % 4, (f + 1) % 4, (f + 2) % 4]
        self.sk = [s, (s + 3) % 4, (s + 1) % 4, (s + 2) % 4]
        self.f_next, self.f_prev = self.place(2, 0), self.place(1, 0)
        self.s_next, self.s_prev = self.place(0, 2), self.place(0, 1)
        self.partner = sp + 1 - 2 * core

    def place(self, k, m):
        return 2 * (self.fk[k] * self.fm + self.sk[m] * self.sm) + self.core

    def block(self, p, k, m, half=None):
        start = self.place(k, m) * ROWS
        return self.rows(p, start, half)

    def rows(self, p, start, half):
        if half is None:
            return self.refs[p].at[pl.ds(pl.multiple_of(start, ROWS), ROWS)]
        return self.refs[p].at[pl.ds(pl.multiple_of(start + half * 32, 32), 32)]

    def copy(self, p, sem, ref, dev):
        return pltpu.make_async_remote_copy(
            ref, ref, self.send_sem.at[p], self.recv_sem.at[p, sem],
            device_id={"sp": dev}, device_id_type=MESH)

    def send(self, p, sem, ref, dev):
        self.copy(p, sem, ref, dev).start()

    def arrive(self, p, sem, rows):
        self.copy(p, sem, self.refs[p].at[pl.ds(0, rows)], self.partner).wait_recv()

    def drain(self):
        for p in range(2):
            self.copy(p, 0, self.refs[p].at[pl.ds(0, 1984)], self.partner).wait_send()

    def hand(self, p, k, m):
        group = next(g for g in range(4) if (m, k) in CHIPS[g])
        self.send(p, GROUP_SEMS[group] if p == 1 else 11, self.block(p, k, m), self.partner)

    def handed_group(self, g):
        self.arrive(1, GROUP_SEMS[g], 4 * ROWS)

    def handed(self, p, sem, count):
        self.arrive(p, sem, count * ROWS)

    def own_along(self, p, turn, half):
        own = self.block(p, 0, 0, half)
        nexts, prevs = (self.f_next, self.s_next), (self.f_prev, self.s_prev)
        for side, (f_dev, s_dev) in enumerate((nexts, prevs)):
            f_sem = 0 if p == 1 or (half == 0 and side == 0) else 1
            self.send(p, f_sem + turn * (3 - f_sem), own, f_dev + turn * (s_dev - f_dev))

    def beyond_f(self, p):
        self.arrive(p, 0, 128)
        self.send(p, 2, self.block(p, 1, 0, 0), self.f_next)
        self.send(p, 2, self.block(p, 2, 0, 1), self.f_prev)

    def beyond_f_next(self):
        self.arrive(0, 0, 32)
        self.send(0, 2, self.block(0, 1, 0, 0), self.f_next)

    def beyond_f_prev(self):
        self.arrive(0, 1, 96)
        self.send(0, 2, self.block(0, 2, 0, 1), self.f_prev)

    def opposite_f(self, p):
        self.arrive(p, 2, 64)

    def beyond_s_own(self):
        self.beyond_s(0, 0)

    def along_s(self, p, k):
        ref = self.block(p, k, 0)
        self.send(p, 3 + k, ref, self.s_next)
        self.send(p, 3 + k, ref, self.s_prev)
        self.hand(p, k, 0)

    def beyond_s(self, p, k):
        self.arrive(p, 3 + k, 128)
        self.send(p, 7 + k, self.block(p, k, 1, 0), self.s_next)
        self.send(p, 7 + k, self.block(p, k, 2, 1), self.s_prev)
        self.hand(p, k, 1)
        self.hand(p, k, 2)

    def opposite_s(self, p, k):
        self.arrive(p, 7 + k, 64)
        self.hand(p, k, 3)

    def columns(self, k, m):
        return pl.multiple_of((self.fk[k] * self.fm + self.sk[m] * self.sm) * 128, 128)


class Across:
    def __init__(self, x, send, recv):
        self.x, self.send_sem, self.recv_sem = x, send, recv
        self.next, self.prev, self.far = (x + 1) % 4, (x + 3) % 4, (x + 2) % 4

    def copy(self, phase, sem, src, dst, dev):
        return pltpu.make_async_remote_copy(
            src, dst, self.send_sem.at[phase], self.recv_sem.at[(0, 4, 12)[phase] + sem],
            device_id={"tp": dev}, device_id_type=MESH)

    def send(self, phase, sem, src, dst, dev):
        self.copy(phase, sem, src, dst, dev).start()

    def arrive(self, phase, sem, ref):
        self.copy(phase, sem, ref, ref, self.next).wait_recv()

    def drain(self, phase, ref):
        self.copy(phase, 0, ref, ref, self.next).wait_send()

    def rows(self, x, half=None):
        if half is None:
            return pl.ds(pl.multiple_of(x * ROWS, ROWS), ROWS)
        return pl.ds(pl.multiple_of(x * ROWS + half * 32, 32), 32)

    def start_relay(self, phase, g, part, relay):
        self.send(phase, g, part.at[g, 0, self.rows(self.far)], relay.at[g, 0], self.next)
        self.send(phase, g, part.at[g, 1, self.rows(self.far)], relay.at[g, 1], self.prev)

    def start_own(self, phase, g, part, landed):
        self.send(
            phase, part.shape[0] + g, part.at[g, 1, self.rows(self.next)], landed.at[g, 0, 1], self.next)
        self.send(
            phase, part.shape[0] + g, part.at[g, 0, self.rows(self.prev)], landed.at[g, 1, 0], self.prev)

    def pass_on(self, phase, g, part, relay, landed):
        self.arrive(phase, g, relay.at[g])
        for side, dev in ((0, self.next), (1, self.prev)):
            total = relay[g, side].astype(F32) + part[g, side, self.rows(dev)].astype(F32)
            relay[g, side] = total.astype(BF16)
            self.send(phase, part.shape[0] + g, relay.at[g, side], landed.at[g, side, side], dev)

    def total(self, phase, g, part, landed):
        self.arrive(phase, part.shape[0] + g, landed.at[g])
        return [
            part[g, sub, self.rows(self.x)].astype(F32)
            + landed[g, 0, sub].astype(F32)
            + landed[g, 1, sub].astype(F32)
            for sub in range(2)
        ]

    def share(self, ref):
        top, bottom = (ref.at[self.rows(self.x, half)] for half in range(2))
        self.send(2, 0, top, top, self.next)
        self.send(2, 1, bottom, bottom, self.prev)
        self.send(2, 2, bottom, bottom, self.next)
        self.send(2, 2, top, top, self.prev)

    def share_on(self, ref):
        top, bottom = ref.at[self.rows(self.prev, 0)], ref.at[self.rows(self.next, 1)]
        self.arrive(2, 0, top)
        self.send(2, 2, top, top, self.next)
        self.arrive(2, 1, bottom)
        self.send(2, 2, bottom, bottom, self.prev)

    def shared(self, ref):
        self.arrive(2, 2, ref.at[pl.ds(0, 128)])


QUARTER = D // 4
def layer_kernel(
    u_hbm, a_hbm, pr_hbm, pi_hbm, sl_hbm, bre_hbm, bim_hbm, cre_hbm, cim_hbm,
    mix_gain_hbm, pre_gain_hbm, post_gain_hbm, wo_hbm, res_hbm, gate_hbm, up_hbm, down_hbm,
    out_ref,
    u_ref, a_ref, poles_ref, sl_ref, maps_ref, gains_ref, wo_ref, res_ref,
    e_ref, dr_ref, di_ref, act_ref, read_ref, ea_ref, eb_ref, ra_ref, rb_ref, gu_ref, dn_ref,
    mix_part, out_part, mix_relay, out_relay, mix_landed, out_landed, rows_ref, hid_ref, sum_ref,
    cs, cq, ws, wq, xs, xq, ls,
):
    sp = lax.axis_index("sp")
    tp = lax.axis_index("tp")
    q = sp % 8
    z = sp // 8
    peers_a = [z * 8 + (q + d) % 8 for d in range(1, 8)]
    peers_b = [((z + d) % 4) * 8 + q for d in range(1, 4)]
    weights = Gather((gu_ref, dn_ref), ws, wq, sp)
    across = Across(tp, xs, xq)
    own = pl.ds(pl.multiple_of(sp * ROWS, ROWS), ROWS)
    for side, hbm in enumerate((gate_hbm, up_hbm)):
        pltpu.make_async_copy(hbm, gu_ref.at[own, pl.ds(side * F, F)], ls.at[0]).start()
    barrier = pltpu.get_barrier_semaphore()
    for peer in peers_a + peers_b:
        pl.semaphore_signal(barrier, inc=1, device_id={"sp": peer}, device_id_type=MESH)
    for peer in (across.next, across.prev):
        pl.semaphore_signal(barrier, inc=1, device_id={"tp": peer}, device_id_type=MESH)
    pairs = (
        (a_hbm, a_ref, 1), (pr_hbm, poles_ref.at[0], 2), (pi_hbm, poles_ref.at[1], 2),
        (sl_hbm, sl_ref, 3), (u_hbm, u_ref, 4),
        (bre_hbm, maps_ref.at[0], 5), (bim_hbm, maps_ref.at[1], 5),
        (cre_hbm, maps_ref.at[2], 5), (cim_hbm, maps_ref.at[3], 5),
        (wo_hbm, wo_ref, 6), (res_hbm, res_ref, 7), (mix_gain_hbm, gains_ref.at[0], 8),
        (pre_gain_hbm, gains_ref.at[1], 8), (post_gain_hbm, gains_ref.at[2], 8),
        (down_hbm, dn_ref.at[own], 9),
    )
    for src, dst, sem in pairs:
        pltpu.make_async_copy(src, dst, ls.at[sem]).start()

    def loaded(ref, sem):
        pltpu.make_async_copy(ref, ref, ls.at[sem]).wait()

    mine = iota((G, GN), 1) // N == iota((G, GN), 0)

    def row(v):
        return jnp.sum(jnp.where(mine, v, 0.0), axis=0, keepdims=True)

    loaded(a_ref, 1)
    put_row(ea_ref, 0, 0, jnp.exp(row(jnp.sum(a_ref[...], axis=1, keepdims=True))))
    loaded(gu_ref.at[own], 0)
    pl.semaphore_wait(barrier, 12)

    def to_all(ref, peers, sem):
        for d, peer in enumerate(peers, 1):
            pltpu.make_async_remote_copy(
                ref.at[0], ref.at[d], cs.at[sem], cq.at[sem],
                device_id={"sp": peer}, device_id_type=MESH).start()

    def from_all(ref, peers, sem):
        others = ref.at[pl.ds(1, len(peers))]
        pltpu.make_async_remote_copy(
            others, others, cs.at[sem], cq.at[sem],
            device_id={"sp": peers[0]}, device_id_type=MESH).wait()

    to_all(ea_ref, peers_a, 0)
    weights.own_along(0, weights.core, 0)
    weights.own_along(0, 1 - weights.core, 0)
    weights.own_along(0, 1 - weights.core, 1)
    weights.hand(0, 0, 0)
    loaded(poles_ref, 2)
    loaded(sl_ref, 3)

    base_r, base_i, ratio_r, ratio_i = step_rows(poles_ref[0], poles_ref[1], sl_ref[...], row)

    perm = iota((T, T), 0) == (iota((T, T), 1) % SEGS) * STEPS + iota((T, T), 1) // SEGS
    order = iota((T, T), 1) == (iota((T, T), 0) % SEGS) * STEPS + iota((T, T), 0) // SEGS
    e_small = dot(thirds(jnp.exp(a_ref[...])), one_hot(perm, BF16)).astype(BF16)
    groups = one_hot(mine, BF16)
    e_ref[...] = lax.dot_general(
        e_small, jnp.concatenate([groups] * 3, axis=0), (((0,), (0,)), ((), ())),
        preferred_element_type=F32)
    loaded(u_ref, 4)
    loaded(maps_ref, 5)
    u = dot(one_hot(order, BF16), u_ref[...]).astype(BF16)
    inside = iota((256, 1024), 0) // C == iota((256, 1024), 1) // N

    def spread(v):
        return jnp.where(inside, lanes_of(v, 1024), 0.0).astype(BF16)

    for h in range(2):
        gn = slice(h * 1024, (h + 1) * 1024)
        ch = slice(h * 256, (h + 1) * 256)
        raw_r = dot(u[:, ch], spread(maps_ref[0, ch, :]))
        raw_i = dot(u[:, ch], spread(maps_ref[1, ch, :]))
        rr, ri = ratio_r[:, gn], ratio_i[:, gn]
        dr_ref[:, gn] = rr * raw_r - ri * raw_i
        di_ref[:, gn] = rr * raw_i + ri * raw_r

    zero = jnp.zeros((SEGS, GN), F32)
    end_r, end_i, pe = scan_pass((base_r, base_i), e_ref, dr_ref, di_ref, (zero, zero), False)
    wr, wi = base_r, base_i
    for _ in range(5):
        wr, wi = cmul(wr, wi, wr, wi)
    seg_r, seg_i = wr * pe, wi * pe
    one_row = jnp.ones((1, GN), F32)
    no_row = jnp.zeros((1, GN), F32)
    total = (one_row, no_row, no_row, no_row)
    before = []
    for j in range(SEGS):
        before.append(total)
        total = link(total, (seg_r[j : j + 1], seg_i[j : j + 1], end_r[j : j + 1], end_i[j : j + 1]))
    put_row(ra_ref, 0, 0, total[2])
    put_row(ra_ref, 0, 1, total[3])

    to_all(ra_ref, peers_a, 1)
    weights.own_along(0, weights.core, 1)
    loaded(dn_ref.at[own], 9)
    weights.own_along(1, weights.core, None)
    weights.hand(1, 0, 0)
    for h in range(2):
        ch = slice(h * 256, (h + 1) * 256)
        read_ref[h, 0] = spread(maps_ref[2, ch, :])
        read_ref[h, 1] = spread(-maps_ref[3, ch, :])
    w_r, w_i = to_block(wr), to_block(wi)
    for _ in range(3):
        w_r, w_i = cmul(w_r, w_i, w_r, w_i)
    v_r, v_i = w_r, w_i
    for _ in range(3):
        v_r, v_i = cmul(v_r, v_i, v_r, v_i)
    from_all(ea_ref, peers_a, 0)
    eb = ea_ref[0]
    for d in range(1, 8):
        eb = eb * ea_ref[d]
    eb_ref[0] = eb
    to_all(eb_ref, peers_b, 2)
    from_all(ra_ref, peers_a, 1)
    unit = jnp.ones((16, 128), F32)
    null = jnp.zeros((16, 128), F32)

    def stretch(e, pr, pi, ref, slot):
        block = ref[slot].astype(F32)
        decay = e[slot]
        return pr * decay, pi * decay, block[:16], block[16:]

    run = (unit, null, null, null)
    pre_a = run
    for k in range(8):
        pre_a = choose(q == k, run, pre_a)
        run = link(run, stretch(ea_ref, w_r, w_i, ra_ref, (q - k + 8) % 8))
    rb_ref[0, :16] = run[2].astype(BF16)
    rb_ref[0, 16:] = run[3].astype(BF16)
    to_all(rb_ref, peers_b, 3)
    weights.own_along(1, 1 - weights.core, None)
    weights.beyond_f_next()
    weights.beyond_f_prev()
    weights.along_s(0, 1)
    weights.along_s(0, 2)
    from_all(eb_ref, peers_b, 2)
    from_all(rb_ref, peers_b, 3)
    run = (unit, null, null, null)
    pre_b = run
    for k in range(4):
        pre_b = choose(z == k, run, pre_b)
        run = link(run, stretch(eb_ref, v_r, v_i, rb_ref, (z - k + 4) % 4))
    carry = link(pre_b, pre_a)
    cr, ci = to_row(carry[2]), to_row(carry[3])
    starts = []
    for k in range(SEGS):
        pr, pi, sr, si = before[k]
        tr, ti = cmul(pr, pi, cr, ci)
        starts.append((tr + sr, ti + si))
    init = [jnp.concatenate([s[k] for s in starts], axis=0) for k in range(2)]
    scan_pass((base_r, base_i), e_ref, dr_ref, di_ref, init, True)

    for h in range(2):
        gn = slice(h * 1024, (h + 1) * 1024)
        y = dot_nt(dr_ref[:, gn].astype(BF16), read_ref[h, 0])
        y = y + dot_nt(di_ref[:, gn].astype(BF16), read_ref[h, 1])
        act_ref[:, h * 256 : (h + 1) * 256] = jax.nn.gelu(y).astype(BF16)
    act = dot(one_hot(perm, BF16), act_ref[...]).astype(BF16)
    loaded(wo_ref, 6)
    for g in range(2):
        out = dot(act, wo_ref[:, g * HALF : (g + 1) * HALF]).astype(BF16)
        mix_part[g, 0] = out[:, :QUARTER]
        mix_part[g, 1] = out[:, QUARTER:]
        across.start_relay(0, g, mix_part, mix_relay)
        across.start_own(0, g, mix_part, mix_landed)
    weights.beyond_s_own()
    across.pass_on(0, 0, mix_part, mix_relay, mix_landed)
    weights.opposite_f(0)
    weights.along_s(0, 3)
    across.pass_on(0, 1, mix_part, mix_relay, mix_landed)
    weights.beyond_s(0, 1)
    weights.beyond_f(1)
    mixed = jnp.concatenate(
        across.total(0, 0, mix_part, mix_landed)
        + across.total(0, 1, mix_part, mix_landed), axis=1)
    loaded(res_ref, 7)
    loaded(gains_ref, 8)
    middle = (res_ref[...].astype(F32) + rms_scale(mixed, gains_ref[0])).astype(BF16)
    res_ref[...] = middle
    normed = rms_scale(middle.astype(F32), gains_ref[1]).astype(BF16)
    rows_ref[across.rows(tp), :] = normed
    across.share(rows_ref)
    weights.beyond_s(0, 2)
    across.share_on(rows_ref)
    weights.beyond_s(0, 3)
    weights.along_s(1, 1)
    weights.along_s(1, 2)
    weights.opposite_f(1)
    weights.along_s(1, 3)
    weights.beyond_s(1, 0)
    across.shared(rows_ref)
    for k in range(4):
        weights.opposite_s(0, k)
    weights.handed(0, 11, 16)
    def hidden_tile(gate, up, first):
        hidden = gate / (1.0 + jnp.exp(-gate)) * up
        hid_ref[first : first + gate.shape[1], :] = hidden.T.astype(BF16)

    for first in range(0, F - 128, 256):
        tile = [gu_ref[:, side * F + first : side * F + first + 256] for side in range(2)]
        hidden_tile(dot(rows_ref[...], tile[0]), dot(rows_ref[...], tile[1]), first)
        if first in (256, 1024):
            weights.beyond_s(1, 1 if first == 256 else 2)
    both = dot(rows_ref[...], jnp.concatenate([gu_ref[:, F - 128 : F], gu_ref[:, 2 * F - 128 :]], axis=1))
    hidden_tile(both[:, :128], both[:, 128:], F - 128)

    def down(g):
        weights.handed_group(g)
        block = jnp.concatenate(
            [dn_ref[pl.ds(weights.columns(k, m), 128), :] for k, m in CHIPS[g]], axis=0)
        out = dot(block, hid_ref[...])
        for i in range(4):
            out_part[g, i // 2, :, (i % 2) * 128 : (i % 2 + 1) * 128] = (
                out[i * 128 : (i + 1) * 128].T.astype(BF16))
        across.start_relay(1, g, out_part, out_relay)
        across.start_own(1, g, out_part, out_landed)

    down(0)
    weights.beyond_s(1, 3)
    down(1)
    weights.opposite_s(1, 0)
    weights.opposite_s(1, 1)
    down(2)
    weights.opposite_s(1, 2)
    weights.opposite_s(1, 3)
    across.pass_on(1, 0, out_part, out_relay, out_landed)
    down(3)
    across.pass_on(1, 1, out_part, out_relay, out_landed)
    across.pass_on(1, 2, out_part, out_relay, out_landed)
    across.pass_on(1, 3, out_part, out_relay, out_landed)
    for g, chips in enumerate(CHIPS):
        sums = across.total(1, g, out_part, out_landed)
        for j, (k, m) in enumerate(chips):
            piece = sums[j // 2][:, (j % 2) * 128 : (j % 2 + 1) * 128]
            sum_ref[:, pl.ds(weights.columns(k, m), 128)] = piece
    merged = res_ref[...].astype(F32) + 0.5 * rms_scale(sum_ref[...], gains_ref[2])
    out_ref[...] = merged.astype(BF16)
    weights.drain()
    across.drain(0, mix_part.at[:, :, pl.ds(0, 192)])
    across.drain(1, out_part.at[:, :, pl.ds(0, 192)])
    across.drain(2, rows_ref.at[pl.ds(0, 192)])


def layer(arrays):
    hbm = pl.BlockSpec(memory_space=pl.ANY)
    dma = pltpu.SemaphoreType.DMA
    return pl.pallas_call(
        layer_kernel,
        out_shape=jax.ShapeDtypeStruct((ROWS, D), BF16),
        in_specs=[hbm] * len(arrays),
        out_specs=pl.BlockSpec(memory_space=pltpu.VMEM),
        scratch_shapes=[
            pltpu.VMEM((T, 512), BF16),
            pltpu.VMEM((G, T), F32),
            pltpu.VMEM((2, G, N), F32),
            pltpu.VMEM((1, G), F32),
            pltpu.VMEM((4, 512, N), F32),
            pltpu.VMEM((3, 1, D), F32),
            pltpu.VMEM((512, D), BF16),
            pltpu.VMEM((ROWS, D), BF16),
            pltpu.VMEM((T, GN), F32),
            pltpu.VMEM((T, GN), F32),
            pltpu.VMEM((T, GN), F32),
            pltpu.VMEM((T, 512), BF16),
            pltpu.VMEM((2, 2, 256, 1024), BF16),
            pltpu.VMEM((8, 16, 128), F32),
            pltpu.VMEM((4, 16, 128), F32),
            pltpu.VMEM((8, 32, 128), BF16),
            pltpu.VMEM((4, 32, 128), BF16),
            pltpu.VMEM((D, 2 * F), BF16),
            pltpu.VMEM((D, F), BF16),
            pltpu.VMEM((2, 2, T, QUARTER), BF16),
            pltpu.VMEM((4, 2, T, QUARTER // 2), BF16),
            pltpu.VMEM((2, 2, ROWS, QUARTER), BF16),
            pltpu.VMEM((4, 2, ROWS, QUARTER // 2), BF16),
            pltpu.VMEM((2, 2, 2, ROWS, QUARTER), BF16),
            pltpu.VMEM((4, 2, 2, ROWS, QUARTER // 2), BF16),
            pltpu.VMEM((T, D), BF16),
            pltpu.VMEM((F, T), BF16),
            pltpu.VMEM((ROWS, D), F32),
            dma((4,)), dma((4,)), dma((2,)), dma((2, 14)), dma((3,)), dma((15,)), dma((10,)),
        ],
        compiler_params=pltpu.CompilerParams(
            collective_id=0, has_side_effects=True, vmem_limit_bytes=66000000
        ),
        name="layer",
    )(*arrays)


def shards(
    residual, ssm_input, pole_real, pole_imaginary, step_log, input_real, entry_map_quadrature,
    output_real, output_imaginary, added_log_decay, out_weight, mix_gain, gate_weight, up_weight,
    down_weight, pre_gain, post_gain,
):
    small = (
        ssm_input, added_log_decay.T, pole_real, pole_imaginary, step_log.reshape(1, G),
        input_real.transpose(0, 2, 1).reshape(512, N),
        entry_map_quadrature.transpose(0, 2, 1).reshape(512, N),
        output_real.reshape(512, N), output_imaginary.reshape(512, N),
        mix_gain.reshape(1, D), pre_gain.reshape(1, D), post_gain.reshape(1, D),
    )
    return layer(small + (out_weight, residual, gate_weight, up_weight, down_weight))


def solution(mesh):
    return jax.shard_map(
        shards,
        mesh=mesh,
        in_specs=(
            P(("sp", "tp"), None), P("sp", "tp"), P("tp", None), P("tp", None), P("tp"),
            P("tp", None, None), P("tp", None, None), P("tp", None, None), P("tp", None, None),
            P("sp", "tp"), P("tp", None), P(), P("sp", "tp"), P("sp", "tp"), P("sp", "tp"),
            P(), P(),
        ),
        out_specs=P(("sp", "tp"), None),
        check_vma=False,
    )
```

```python
import functools

import jax
import jax.numpy as jnp
from jax import lax
from jax.experimental import pallas as pl
from jax.experimental.pallas import tpu as pltpu
from jax.sharding import PartitionSpec as P

EPSILON = 1e-06
EXACT = lax.Precision.HIGHEST
MESH = pl.DeviceIdType.MESH
F32 = jnp.float32
BF16 = jnp.bfloat16
T = 256
G = 32
N = 64
C = 16
GN = G * N
SEGS = 8
STEPS = T // SEGS
D = 2048
F = 1408
ROWS = 64
HALF = D // 2
TILES = F // 128


def dot(a, b, **kw):
    return jnp.dot(a, b, preferred_element_type=F32, **kw)


def dot_nt(a, b):
    return lax.dot_general(a, b, (((1,), (1,)), ((), ())), preferred_element_type=F32)


def iota(shape, dim):
    return lax.broadcasted_iota(jnp.int32, shape, dim)


def one_hot(mask, dtype):
    return jnp.where(mask, 1.0, 0.0).astype(dtype)


def cmul(ar, ai, br, bi):
    return ar * br - ai * bi, ar * bi + ai * br


def split(v):
    hi = v.astype(BF16)
    return hi, (v - hi.astype(F32)).astype(BF16)


def expm1(x):
    p = 1.0 / 40320.0
    for k in (5040.0, 720.0, 120.0, 24.0, 6.0, 2.0, 1.0):
        p = p * x + 1.0 / k
    return jnp.where(x > -0.5, p * x, jnp.exp(x) - 1.0)


def lanes_of(v, count):
    pair = jnp.concatenate([v, v], axis=1)
    return jnp.concatenate([pair] * (count // 128), axis=1)


def step_rows(pr, pi, sl, row):
    same = iota((G, G), 0) == iota((G, G), 1)
    column = jnp.sum(jnp.where(same, jnp.broadcast_to(sl, (G, G)), 0.0), axis=1, keepdims=True)
    pr, pi, step = row(lanes_of(pr, GN)), row(lanes_of(pi, GN)), jnp.exp(row(column))
    log_size = pr * step
    angle = pi * step
    cosine, sine = jnp.cos(angle), jnp.sin(angle)
    size = jnp.exp(log_size)
    half = jnp.sin(0.5 * angle)
    lift_r = expm1(log_size) * cosine - 2.0 * half * half
    lift_i = size * sine
    inv = 1.0 / (pr * pr + pi * pi)
    ratio_r = (lift_r * pr + lift_i * pi) * inv
    ratio_i = (lift_i * pr - lift_r * pi) * inv
    return size * cosine, size * sine, ratio_r, ratio_i


def thirds(v):
    hi = v.astype(BF16)
    rest = v - hi.astype(F32)
    mid = rest.astype(BF16)
    return jnp.concatenate([hi, mid, (rest - mid.astype(F32)).astype(BF16)], axis=0)


def scan_pass(base, e_ref, dr_ref, di_ref, init, store):
    ends = []
    width = GN // 4
    for lc in range(4):
        sl = slice(lc * width, (lc + 1) * width)
        br = jnp.broadcast_to(base[0][:, sl], (SEGS, width))
        bi = jnp.broadcast_to(base[1][:, sl], (SEGS, width))

        def body(i, st):
            sr, si, pe = st
            rows = pl.ds(pl.multiple_of(i * SEGS, SEGS), SEGS)
            e = e_ref[rows, sl]
            ar, ai = br * e, bi * e
            nr = ar * sr - ai * si + dr_ref[rows, sl]
            ni = ar * si + ai * sr + di_ref[rows, sl]
            if store:
                dr_ref[rows, sl] = nr
                di_ref[rows, sl] = ni
                return nr, ni, pe
            return nr, ni, pe * e

        st = (init[0][:, sl], init[1][:, sl], jnp.ones((SEGS, width), F32))
        ends.append(lax.fori_loop(0, STEPS, body, st, unroll=4))
    return [jnp.concatenate([p[k] for p in ends], axis=1) for k in range(3)]


def put_row(ref, slot, part, row):
    for k in range(16):
        ref[slot, part * 16 + k : part * 16 + k + 1, :] = row[:, k * 128 : (k + 1) * 128].astype(ref.dtype)


def to_block(row):
    return jnp.concatenate([row[:, k * 128 : (k + 1) * 128] for k in range(16)], axis=0)


def to_row(block):
    return jnp.concatenate([block[k : k + 1, :] for k in range(16)], axis=1)


def link(first, then):
    ar, ai, sr, si = first
    br, bi, tr, ti = then
    pr, pi = cmul(br, bi, ar, ai)
    ur, ui = cmul(br, bi, sr, si)
    return pr, pi, ur + tr, ui + ti


def choose(cond, a, b):
    return tuple(jnp.where(cond, x, y) for x, y in zip(a, b))


def rms_scale(values, gain):
    return values * lax.rsqrt(jnp.mean(values * values, axis=-1, keepdims=True) + EPSILON) * gain


CHIPS = (
    ((0, 0), (0, 1), (1, 0), (0, 2)),
    ((2, 0), (1, 1), (1, 2), (2, 1)),
    ((2, 2), (3, 0), (0, 3), (1, 3)),
    ((3, 1), (2, 3), (3, 2), (3, 3)),
)
GROUP_SEMS = (11, 1, 12, 13)


class Gather:
    def __init__(self, refs, send, recv, sp):
        self.refs, self.send_sem, self.recv_sem = refs, send, recv
        core, y, z = sp % 2, (sp // 2) % 4, sp // 8
        self.core = core
        self.fm, self.sm = 1 + 3 * core, 4 - 3 * core
        f = y + core * (z - y)
        s = z + core * (y - z)
        self.fk = [f, (f + 3) % 4, (f + 1) % 4, (f + 2) % 4]
        self.sk = [s, (s + 3) % 4, (s + 1) % 4, (s + 2) % 4]
        self.f_next, self.f_prev = self.place(2, 0), self.place(1, 0)
        self.s_next, self.s_prev = self.place(0, 2), self.place(0, 1)
        self.partner = sp + 1 - 2 * core

    def place(self, k, m):
        return 2 * (self.fk[k] * self.fm + self.sk[m] * self.sm) + self.core

    def block(self, p, k, m, half=None):
        start = self.place(k, m) * ROWS
        return self.rows(p, start, half)

    def rows(self, p, start, half):
        if half is None:
            return self.refs[p].at[pl.ds(pl.multiple_of(start, ROWS), ROWS)]
        return self.refs[p].at[pl.ds(pl.multiple_of(start + half * 32, 32), 32)]

    def copy(self, p, sem, ref, dev):
        return pltpu.make_async_remote_copy(
            ref, ref, self.send_sem.at[p], self.recv_sem.at[p, sem],
            device_id={"sp": dev}, device_id_type=MESH)

    def send(self, p, sem, ref, dev):
        self.copy(p, sem, ref, dev).start()

    def arrive(self, p, sem, rows):
        self.copy(p, sem, self.refs[p].at[pl.ds(0, rows)], self.partner).wait_recv()

    def drain(self):
        for p in range(2):
            self.copy(p, 0, self.refs[p].at[pl.ds(0, 1984)], self.partner).wait_send()

    def hand(self, p, k, m):
        group = next(g for g in range(4) if (m, k) in CHIPS[g])
        self.send(p, GROUP_SEMS[group] if p == 1 else 11, self.block(p, k, m), self.partner)

    def handed_group(self, g):
        self.arrive(1, GROUP_SEMS[g], 4 * ROWS)

    def handed(self, p, sem, count):
        self.arrive(p, sem, count * ROWS)

    def own_along(self, p, turn, half):
        own = self.block(p, 0, 0, half)
        nexts, prevs = (self.f_next, self.s_next), (self.f_prev, self.s_prev)
        for side, (f_dev, s_dev) in enumerate((nexts, prevs)):
            f_sem = 0 if p == 1 or (half == 0 and side == 0) else 1
            self.send(p, f_sem + turn * (3 - f_sem), own, f_dev + turn * (s_dev - f_dev))

    def beyond_f(self, p):
        self.arrive(p, 0, 128)
        self.send(p, 2, self.block(p, 1, 0, 0), self.f_next)
        self.send(p, 2, self.block(p, 2, 0, 1), self.f_prev)

    def beyond_f_next(self):
        self.arrive(0, 0, 32)
        self.send(0, 2, self.block(0, 1, 0, 0), self.f_next)

    def beyond_f_prev(self):
        self.arrive(0, 1, 96)
        self.send(0, 2, self.block(0, 2, 0, 1), self.f_prev)

    def opposite_f(self, p):
        self.arrive(p, 2, 64)

    def beyond_s_own(self):
        self.beyond_s(0, 0)

    def along_s(self, p, k):
        ref = self.block(p, k, 0)
        self.send(p, 3 + k, ref, self.s_next)
        self.send(p, 3 + k, ref, self.s_prev)
        self.hand(p, k, 0)

    def beyond_s(self, p, k):
        self.arrive(p, 3 + k, 128)
        self.send(p, 7 + k, self.block(p, k, 1, 0), self.s_next)
        self.send(p, 7 + k, self.block(p, k, 2, 1), self.s_prev)
        self.hand(p, k, 1)
        self.hand(p, k, 2)

    def opposite_s(self, p, k):
        self.arrive(p, 7 + k, 64)
        self.hand(p, k, 3)

    def columns(self, k, m):
        return pl.multiple_of((self.fk[k] * self.fm + self.sk[m] * self.sm) * 128, 128)


class Across:
    def __init__(self, x, send, recv):
        self.x, self.send_sem, self.recv_sem = x, send, recv
        self.next, self.prev, self.far = (x + 1) % 4, (x + 3) % 4, (x + 2) % 4

    def copy(self, phase, sem, src, dst, dev):
        return pltpu.make_async_remote_copy(
            src, dst, self.send_sem.at[phase], self.recv_sem.at[(0, 4, 12)[phase] + sem],
            device_id={"tp": dev}, device_id_type=MESH)

    def send(self, phase, sem, src, dst, dev):
        self.copy(phase, sem, src, dst, dev).start()

    def arrive(self, phase, sem, ref):
        self.copy(phase, sem, ref, ref, self.next).wait_recv()

    def drain(self, phase, ref):
        self.copy(phase, 0, ref, ref, self.next).wait_send()

    def rows(self, x, half=None):
        if half is None:
            return pl.ds(pl.multiple_of(x * ROWS, ROWS), ROWS)
        return pl.ds(pl.multiple_of(x * ROWS + half * 32, 32), 32)

    def start_relay(self, phase, g, part, relay):
        self.send(phase, g, part.at[g, 0, self.rows(self.far)], relay.at[g, 0], self.next)
        self.send(phase, g, part.at[g, 1, self.rows(self.far)], relay.at[g, 1], self.prev)

    def start_own(self, phase, g, part, landed):
        self.send(
            phase, part.shape[0] + g, part.at[g, 1, self.rows(self.next)], landed.at[g, 0, 1], self.next)
        self.send(
            phase, part.shape[0] + g, part.at[g, 0, self.rows(self.prev)], landed.at[g, 1, 0], self.prev)

    def pass_on(self, phase, g, part, relay, landed):
        self.arrive(phase, g, relay.at[g])
        for side, dev in ((0, self.next), (1, self.prev)):
            total = relay[g, side].astype(F32) + part[g, side, self.rows(dev)].astype(F32)
            relay[g, side] = total.astype(BF16)
            self.send(phase, part.shape[0] + g, relay.at[g, side], landed.at[g, side, side], dev)

    def total(self, phase, g, part, landed):
        self.arrive(phase, part.shape[0] + g, landed.at[g])
        return [
            part[g, sub, self.rows(self.x)].astype(F32)
            + landed[g, 0, sub].astype(F32)
            + landed[g, 1, sub].astype(F32)
            for sub in range(2)
        ]

    def share(self, ref):
        top, bottom = (ref.at[self.rows(self.x, half)] for half in range(2))
        self.send(2, 0, top, top, self.next)
        self.send(2, 1, bottom, bottom, self.prev)
        self.send(2, 2, bottom, bottom, self.next)
        self.send(2, 2, top, top, self.prev)

    def share_on(self, ref):
        top, bottom = ref.at[self.rows(self.prev, 0)], ref.at[self.rows(self.next, 1)]
        self.arrive(2, 0, top)
        self.send(2, 2, top, top, self.next)
        self.arrive(2, 1, bottom)
        self.send(2, 2, bottom, bottom, self.prev)

    def shared(self, ref):
        self.arrive(2, 2, ref.at[pl.ds(0, 128)])


QUARTER = D // 4
def layer_kernel(
    u_hbm, a_hbm, pr_hbm, pi_hbm, sl_hbm, bre_hbm, bim_hbm, cre_hbm, cim_hbm,
    mix_gain_hbm, pre_gain_hbm, post_gain_hbm, wo_hbm, res_hbm, gate_hbm, up_hbm, down_hbm,
    out_ref,
    u_ref, a_ref, poles_ref, sl_ref, maps_ref, gains_ref, wo_ref, res_ref,
    e_ref, dr_ref, di_ref, act_ref, read_ref, ea_ref, eb_ref, ra_ref, rb_ref, gu_ref, dn_ref,
    mix_part, out_part, mix_relay, out_relay, mix_landed, out_landed, rows_ref, hid_ref, sum_ref,
    cs, cq, ws, wq, xs, xq, ls,
):
    sp = lax.axis_index("sp")
    tp = lax.axis_index("tp")
    q = sp % 8
    z = sp // 8
    peers_a = [z * 8 + (q + d) % 8 for d in range(1, 8)]
    peers_b = [((z + d) % 4) * 8 + q for d in range(1, 4)]
    weights = Gather((gu_ref, dn_ref), ws, wq, sp)
    across = Across(tp, xs, xq)
    own = pl.ds(pl.multiple_of(sp * ROWS, ROWS), ROWS)
    for side, hbm in enumerate((gate_hbm, up_hbm)):
        pltpu.make_async_copy(hbm, gu_ref.at[own, pl.ds(side * F, F)], ls.at[0]).start()
    barrier = pltpu.get_barrier_semaphore()
    for peer in peers_a + peers_b:
        pl.semaphore_signal(barrier, inc=1, device_id={"sp": peer}, device_id_type=MESH)
    for peer in (across.next, across.prev):
        pl.semaphore_signal(barrier, inc=1, device_id={"tp": peer}, device_id_type=MESH)
    pairs = (
        (a_hbm, a_ref, 1), (pr_hbm, poles_ref.at[0], 2), (pi_hbm, poles_ref.at[1], 2),
        (sl_hbm, sl_ref, 3), (u_hbm, u_ref, 4),
        (bre_hbm, maps_ref.at[0], 5), (bim_hbm, maps_ref.at[1], 5),
        (cre_hbm, maps_ref.at[2], 5), (cim_hbm, maps_ref.at[3], 5),
        (wo_hbm, wo_ref, 6), (res_hbm, res_ref, 7), (mix_gain_hbm, gains_ref.at[0], 8),
        (pre_gain_hbm, gains_ref.at[1], 8), (post_gain_hbm, gains_ref.at[2], 8),
        (down_hbm, dn_ref.at[own], 9),
    )
    for src, dst, sem in pairs:
        pltpu.make_async_copy(src, dst, ls.at[sem]).start()

    def loaded(ref, sem):
        pltpu.make_async_copy(ref, ref, ls.at[sem]).wait()

    mine = iota((G, GN), 1) // N == iota((G, GN), 0)

    def row(v):
        return jnp.sum(jnp.where(mine, v, 0.0), axis=0, keepdims=True)

    loaded(a_ref, 1)
    put_row(ea_ref, 0, 0, jnp.exp(row(jnp.sum(a_ref[...], axis=1, keepdims=True))))
    loaded(gu_ref.at[own], 0)
    pl.semaphore_wait(barrier, 12)

    def to_all(ref, peers, sem):
        for d, peer in enumerate(peers, 1):
            pltpu.make_async_remote_copy(
                ref.at[0], ref.at[d], cs.at[sem], cq.at[sem],
                device_id={"sp": peer}, device_id_type=MESH).start()

    def from_all(ref, peers, sem):
        others = ref.at[pl.ds(1, len(peers))]
        pltpu.make_async_remote_copy(
            others, others, cs.at[sem], cq.at[sem],
            device_id={"sp": peers[0]}, device_id_type=MESH).wait()

    to_all(ea_ref, peers_a, 0)
    weights.own_along(0, weights.core, 0)
    weights.own_along(0, 1 - weights.core, 0)
    weights.own_along(0, 1 - weights.core, 1)
    weights.hand(0, 0, 0)
    loaded(poles_ref, 2)
    loaded(sl_ref, 3)

    base_r, base_i, ratio_r, ratio_i = step_rows(poles_ref[0], poles_ref[1], sl_ref[...], row)

    perm = iota((T, T), 0) == (iota((T, T), 1) % SEGS) * STEPS + iota((T, T), 1) // SEGS
    order = iota((T, T), 1) == (iota((T, T), 0) % SEGS) * STEPS + iota((T, T), 0) // SEGS
    e_small = dot(thirds(jnp.exp(a_ref[...])), one_hot(perm, BF16)).astype(BF16)
    groups = one_hot(mine, BF16)
    e_ref[...] = lax.dot_general(
        e_small, jnp.concatenate([groups] * 3, axis=0), (((0,), (0,)), ((), ())),
        preferred_element_type=F32)
    loaded(u_ref, 4)
    loaded(maps_ref, 5)
    u = dot(one_hot(order, BF16), u_ref[...]).astype(BF16)
    inside = iota((256, 1024), 0) // C == iota((256, 1024), 1) // N

    def spread(v):
        return jnp.where(inside, lanes_of(v, 1024), 0.0).astype(BF16)

    for h in range(2):
        gn = slice(h * 1024, (h + 1) * 1024)
        ch = slice(h * 256, (h + 1) * 256)
        raw_r = dot(u[:, ch], spread(maps_ref[0, ch, :]))
        raw_i = dot(u[:, ch], spread(maps_ref[1, ch, :]))
        rr, ri = ratio_r[:, gn], ratio_i[:, gn]
        dr_ref[:, gn] = rr * raw_r - ri * raw_i
        di_ref[:, gn] = rr * raw_i + ri * raw_r

    zero = jnp.zeros((SEGS, GN), F32)
    end_r, end_i, pe = scan_pass((base_r, base_i), e_ref, dr_ref, di_ref, (zero, zero), False)
    wr, wi = base_r, base_i
    for _ in range(5):
        wr, wi = cmul(wr, wi, wr, wi)
    seg_r, seg_i = wr * pe, wi * pe
    one_row = jnp.ones((1, GN), F32)
    no_row = jnp.zeros((1, GN), F32)
    total = (one_row, no_row, no_row, no_row)
    before = []
    for j in range(SEGS):
        before.append(total)
        total = link(total, (seg_r[j : j + 1], seg_i[j : j + 1], end_r[j : j + 1], end_i[j : j + 1]))
    put_row(ra_ref, 0, 0, total[2])
    put_row(ra_ref, 0, 1, total[3])

    to_all(ra_ref, peers_a, 1)
    weights.own_along(0, weights.core, 1)
    loaded(dn_ref.at[own], 9)
    weights.own_along(1, weights.core, None)
    weights.hand(1, 0, 0)
    for h in range(2):
        ch = slice(h * 256, (h + 1) * 256)
        read_ref[h, 0] = spread(maps_ref[2, ch, :])
        read_ref[h, 1] = spread(-maps_ref[3, ch, :])
    w_r, w_i = to_block(wr), to_block(wi)
    for _ in range(3):
        w_r, w_i = cmul(w_r, w_i, w_r, w_i)
    v_r, v_i = w_r, w_i
    for _ in range(3):
        v_r, v_i = cmul(v_r, v_i, v_r, v_i)
    from_all(ea_ref, peers_a, 0)
    eb = ea_ref[0]
    for d in range(1, 8):
        eb = eb * ea_ref[d]
    eb_ref[0] = eb
    to_all(eb_ref, peers_b, 2)
    from_all(ra_ref, peers_a, 1)
    unit = jnp.ones((16, 128), F32)
    null = jnp.zeros((16, 128), F32)

    def stretch(e, pr, pi, ref, slot):
        block = ref[slot].astype(F32)
        decay = e[slot]
        return pr * decay, pi * decay, block[:16], block[16:]

    run = (unit, null, null, null)
    pre_a = run
    for k in range(8):
        pre_a = choose(q == k, run, pre_a)
        run = link(run, stretch(ea_ref, w_r, w_i, ra_ref, (q - k + 8) % 8))
    rb_ref[0, :16] = run[2].astype(BF16)
    rb_ref[0, 16:] = run[3].astype(BF16)
    to_all(rb_ref, peers_b, 3)
    weights.own_along(1, 1 - weights.core, None)
    weights.beyond_f_next()
    weights.beyond_f_prev()
    weights.along_s(0, 1)
    weights.along_s(0, 2)
    from_all(eb_ref, peers_b, 2)
    from_all(rb_ref, peers_b, 3)
    run = (unit, null, null, null)
    pre_b = run
    for k in range(4):
        pre_b = choose(z == k, run, pre_b)
        run = link(run, stretch(eb_ref, v_r, v_i, rb_ref, (z - k + 4) % 4))
    carry = link(pre_b, pre_a)
    cr, ci = to_row(carry[2]), to_row(carry[3])
    starts = []
    for k in range(SEGS):
        pr, pi, sr, si = before[k]
        tr, ti = cmul(pr, pi, cr, ci)
        starts.append((tr + sr, ti + si))
    init = [jnp.concatenate([s[k] for s in starts], axis=0) for k in range(2)]
    scan_pass((base_r, base_i), e_ref, dr_ref, di_ref, init, True)

    for h in range(2):
        gn = slice(h * 1024, (h + 1) * 1024)
        y = dot_nt(dr_ref[:, gn].astype(BF16), read_ref[h, 0])
        y = y + dot_nt(di_ref[:, gn].astype(BF16), read_ref[h, 1])
        act_ref[:, h * 256 : (h + 1) * 256] = jax.nn.gelu(y).astype(BF16)
    act = dot(one_hot(perm, BF16), act_ref[...]).astype(BF16)
    loaded(wo_ref, 6)
    for g in range(2):
        out = dot(act, wo_ref[:, g * HALF : (g + 1) * HALF]).astype(BF16)
        mix_part[g, 0] = out[:, :QUARTER]
        mix_part[g, 1] = out[:, QUARTER:]
        across.start_relay(0, g, mix_part, mix_relay)
        across.start_own(0, g, mix_part, mix_landed)
    weights.beyond_s_own()
    across.pass_on(0, 0, mix_part, mix_relay, mix_landed)
    weights.opposite_f(0)
    weights.along_s(0, 3)
    across.pass_on(0, 1, mix_part, mix_relay, mix_landed)
    weights.beyond_s(0, 1)
    weights.beyond_f(1)
    mixed = jnp.concatenate(
        across.total(0, 0, mix_part, mix_landed)
        + across.total(0, 1, mix_part, mix_landed), axis=1)
    loaded(res_ref, 7)
    loaded(gains_ref, 8)
    middle = (res_ref[...].astype(F32) + rms_scale(mixed, gains_ref[0])).astype(BF16)
    res_ref[...] = middle
    normed = rms_scale(middle.astype(F32), gains_ref[1]).astype(BF16)
    rows_ref[across.rows(tp), :] = normed
    across.share(rows_ref)
    weights.beyond_s(0, 2)
    across.share_on(rows_ref)
    weights.beyond_s(0, 3)
    weights.along_s(1, 1)
    weights.along_s(1, 2)
    weights.opposite_f(1)
    weights.along_s(1, 3)
    weights.beyond_s(1, 0)
    across.shared(rows_ref)
    for k in range(4):
        weights.opposite_s(0, k)
    weights.handed(0, 11, 16)
    def hidden_tile(gate, up, first):
        hidden = gate / (1.0 + jnp.exp(-gate)) * up
        hid_ref[first : first + gate.shape[1], :] = hidden.T.astype(BF16)

    for first in range(0, F - 128, 256):
        tile = [gu_ref[:, side * F + first : side * F + first + 256] for side in range(2)]
        hidden_tile(dot(rows_ref[...], tile[0]), dot(rows_ref[...], tile[1]), first)
        if first in (256, 1024):
            weights.beyond_s(1, 1 if first == 256 else 2)
    both = dot(rows_ref[...], jnp.concatenate([gu_ref[:, F - 128 : F], gu_ref[:, 2 * F - 128 :]], axis=1))
    hidden_tile(both[:, :128], both[:, 128:], F - 128)

    def down(g):
        weights.handed_group(g)
        block = jnp.concatenate(
            [dn_ref[pl.ds(weights.columns(k, m), 128), :] for k, m in CHIPS[g]], axis=0)
        out = dot(block, hid_ref[...])
        for i in range(4):
            out_part[g, i // 2, :, (i % 2) * 128 : (i % 2 + 1) * 128] = (
                out[i * 128 : (i + 1) * 128].T.astype(BF16))
        across.start_relay(1, g, out_part, out_relay)
        across.start_own(1, g, out_part, out_landed)

    down(0)
    weights.beyond_s(1, 3)
    down(1)
    weights.opposite_s(1, 0)
    weights.opposite_s(1, 1)
    down(2)
    weights.opposite_s(1, 2)
    weights.opposite_s(1, 3)
    across.pass_on(1, 0, out_part, out_relay, out_landed)
    down(3)
    across.pass_on(1, 1, out_part, out_relay, out_landed)
    across.pass_on(1, 2, out_part, out_relay, out_landed)
    across.pass_on(1, 3, out_part, out_relay, out_landed)
    for g, chips in enumerate(CHIPS):
        sums = across.total(1, g, out_part, out_landed)
        for j, (k, m) in enumerate(chips):
            piece = sums[j // 2][:, (j % 2) * 128 : (j % 2 + 1) * 128]
            sum_ref[:, pl.ds(weights.columns(k, m), 128)] = piece
    merged = res_ref[...].astype(F32) + 0.5 * rms_scale(sum_ref[...], gains_ref[2])
    out_ref[...] = merged.astype(BF16)
    weights.drain()
    across.drain(0, mix_part.at[:, :, pl.ds(0, 192)])
    across.drain(1, out_part.at[:, :, pl.ds(0, 192)])
    across.drain(2, rows_ref.at[pl.ds(0, 192)])


def layer(arrays):
    hbm = pl.BlockSpec(memory_space=pl.ANY)
    dma = pltpu.SemaphoreType.DMA
    return pl.pallas_call(
        layer_kernel,
        out_shape=pltpu.VMEM((ROWS, D), BF16),
        in_specs=[hbm] * len(arrays),
        out_specs=pl.BlockSpec(memory_space=pltpu.VMEM),
        scratch_shapes=[
            pltpu.VMEM((T, 512), BF16),
            pltpu.VMEM((G, T), F32),
            pltpu.VMEM((2, G, N), F32),
            pltpu.VMEM((1, G), F32),
            pltpu.VMEM((4, 512, N), F32),
            pltpu.VMEM((3, 1, D), F32),
            pltpu.VMEM((512, D), BF16),
            pltpu.VMEM((ROWS, D), BF16),
            pltpu.VMEM((T, GN), F32),
            pltpu.VMEM((T, GN), F32),
            pltpu.VMEM((T, GN), F32),
            pltpu.VMEM((T, 512), BF16),
            pltpu.VMEM((2, 2, 256, 1024), BF16),
            pltpu.VMEM((8, 16, 128), F32),
            pltpu.VMEM((4, 16, 128), F32),
            pltpu.VMEM((8, 32, 128), BF16),
            pltpu.VMEM((4, 32, 128), BF16),
            pltpu.VMEM((D, 2 * F), BF16),
            pltpu.VMEM((D, F), BF16),
            pltpu.VMEM((2, 2, T, QUARTER), BF16),
            pltpu.VMEM((4, 2, T, QUARTER // 2), BF16),
            pltpu.VMEM((2, 2, ROWS, QUARTER), BF16),
            pltpu.VMEM((4, 2, ROWS, QUARTER // 2), BF16),
            pltpu.VMEM((2, 2, 2, ROWS, QUARTER), BF16),
            pltpu.VMEM((4, 2, 2, ROWS, QUARTER // 2), BF16),
            pltpu.VMEM((T, D), BF16),
            pltpu.VMEM((F, T), BF16),
            pltpu.VMEM((ROWS, D), F32),
            dma((4,)), dma((4,)), dma((2,)), dma((2, 14)), dma((3,)), dma((15,)), dma((10,)),
        ],
        compiler_params=pltpu.CompilerParams(
            collective_id=0, has_side_effects=True, vmem_limit_bytes=60000000
        ),
        name="layer",
    )(*arrays)


def shards(
    residual, ssm_input, pole_real, pole_imaginary, step_log, input_real, entry_map_quadrature,
    output_real, output_imaginary, added_log_decay, out_weight, mix_gain, gate_weight, up_weight,
    down_weight, pre_gain, post_gain,
):
    small = (
        ssm_input, added_log_decay.T, pole_real, pole_imaginary, step_log.reshape(1, G),
        input_real.transpose(0, 2, 1).reshape(512, N),
        entry_map_quadrature.transpose(0, 2, 1).reshape(512, N),
        output_real.reshape(512, N), output_imaginary.reshape(512, N),
        mix_gain.reshape(1, D), pre_gain.reshape(1, D), post_gain.reshape(1, D),
    )
    return layer(small + (out_weight, residual, gate_weight, up_weight, down_weight))


def solution(mesh):
    return jax.shard_map(
        shards,
        mesh=mesh,
        in_specs=(
            P(("sp", "tp"), None), P("sp", "tp"), P("tp", None), P("tp", None), P("tp"),
            P("tp", None, None), P("tp", None, None), P("tp", None, None), P("tp", None, None),
            P("sp", "tp"), P("tp", None), P(), P("sp", "tp"), P("sp", "tp"), P("sp", "tp"),
            P(), P(),
        ),
        out_specs=P(("sp", "tp"), None),
        check_vma=False,
    )
```

```python
import functools

import jax
import jax.numpy as jnp
from jax import lax
from jax.experimental import pallas as pl
from jax.experimental.pallas import tpu as pltpu
from jax.sharding import PartitionSpec as P

EPSILON = 1e-06
EXACT = lax.Precision.HIGHEST
MESH = pl.DeviceIdType.MESH
F32 = jnp.float32
BF16 = jnp.bfloat16
T = 256
G = 32
N = 64
C = 16
GN = G * N
SEGS = 8
STEPS = T // SEGS
D = 2048
F = 1408
ROWS = 64
HALF = D // 2
TILES = F // 128


def dot(a, b, **kw):
    return jnp.dot(a, b, preferred_element_type=F32, **kw)


def dot_nt(a, b):
    return lax.dot_general(a, b, (((1,), (1,)), ((), ())), preferred_element_type=F32)


def iota(shape, dim):
    return lax.broadcasted_iota(jnp.int32, shape, dim)


def one_hot(mask, dtype):
    return jnp.where(mask, 1.0, 0.0).astype(dtype)


def cmul(ar, ai, br, bi):
    return ar * br - ai * bi, ar * bi + ai * br


def split(v):
    hi = v.astype(BF16)
    return hi, (v - hi.astype(F32)).astype(BF16)


def expm1(x):
    p = 1.0 / 40320.0
    for k in (5040.0, 720.0, 120.0, 24.0, 6.0, 2.0, 1.0):
        p = p * x + 1.0 / k
    return jnp.where(x > -0.5, p * x, jnp.exp(x) - 1.0)


def lanes_of(v, count):
    pair = jnp.concatenate([v, v], axis=1)
    return jnp.concatenate([pair] * (count // 128), axis=1)


def step_rows(pr, pi, sl, row):
    same = iota((G, G), 0) == iota((G, G), 1)
    column = jnp.sum(jnp.where(same, jnp.broadcast_to(sl, (G, G)), 0.0), axis=1, keepdims=True)
    pr, pi, step = row(lanes_of(pr, GN)), row(lanes_of(pi, GN)), jnp.exp(row(column))
    log_size = pr * step
    angle = pi * step
    cosine, sine = jnp.cos(angle), jnp.sin(angle)
    size = jnp.exp(log_size)
    half = jnp.sin(0.5 * angle)
    lift_r = expm1(log_size) * cosine - 2.0 * half * half
    lift_i = size * sine
    inv = 1.0 / (pr * pr + pi * pi)
    ratio_r = (lift_r * pr + lift_i * pi) * inv
    ratio_i = (lift_i * pr - lift_r * pi) * inv
    return size * cosine, size * sine, ratio_r, ratio_i


def thirds(v):
    hi = v.astype(BF16)
    rest = v - hi.astype(F32)
    mid = rest.astype(BF16)
    return jnp.concatenate([hi, mid, (rest - mid.astype(F32)).astype(BF16)], axis=0)


def scan_pass(base, e_ref, dr_ref, di_ref, init, store):
    ends = []
    width = GN // 4
    for lc in range(4):
        sl = slice(lc * width, (lc + 1) * width)
        br = jnp.broadcast_to(base[0][:, sl], (SEGS, width))
        bi = jnp.broadcast_to(base[1][:, sl], (SEGS, width))

        def body(i, st):
            sr, si, pe = st
            rows = pl.ds(pl.multiple_of(i * SEGS, SEGS), SEGS)
            e = e_ref[rows, sl]
            ar, ai = br * e, bi * e
            nr = ar * sr - ai * si + dr_ref[rows, sl]
            ni = ar * si + ai * sr + di_ref[rows, sl]
            if store:
                dr_ref[rows, sl] = nr
                di_ref[rows, sl] = ni
                return nr, ni, pe
            return nr, ni, pe * e

        st = (init[0][:, sl], init[1][:, sl], jnp.ones((SEGS, width), F32))
        ends.append(lax.fori_loop(0, STEPS, body, st, unroll=4))
    return [jnp.concatenate([p[k] for p in ends], axis=1) for k in range(3)]


def put_row(ref, slot, part, row):
    for k in range(16):
        ref[slot, part * 16 + k : part * 16 + k + 1, :] = row[:, k * 128 : (k + 1) * 128].astype(ref.dtype)


def to_block(row):
    return jnp.concatenate([row[:, k * 128 : (k + 1) * 128] for k in range(16)], axis=0)


def to_row(block):
    return jnp.concatenate([block[k : k + 1, :] for k in range(16)], axis=1)


def link(first, then):
    ar, ai, sr, si = first
    br, bi, tr, ti = then
    pr, pi = cmul(br, bi, ar, ai)
    ur, ui = cmul(br, bi, sr, si)
    return pr, pi, ur + tr, ui + ti


def choose(cond, a, b):
    return tuple(jnp.where(cond, x, y) for x, y in zip(a, b))


def rms_scale(values, gain):
    return values * lax.rsqrt(jnp.mean(values * values, axis=-1, keepdims=True) + EPSILON) * gain


CHIPS = (
    ((0, 0), (0, 1), (1, 0), (0, 2)),
    ((2, 0), (1, 1), (1, 2), (2, 1)),
    ((2, 2), (3, 0), (0, 3), (1, 3)),
    ((3, 1), (2, 3), (3, 2), (3, 3)),
)
GROUP_SEMS = (11, 1, 12, 13)


class Gather:
    def __init__(self, refs, send, recv, sp):
        self.refs, self.send_sem, self.recv_sem = refs, send, recv
        core, y, z = sp % 2, (sp // 2) % 4, sp // 8
        self.core = core
        self.fm, self.sm = 1 + 3 * core, 4 - 3 * core
        f = y + core * (z - y)
        s = z + core * (y - z)
        self.fk = [f, (f + 3) % 4, (f + 1) % 4, (f + 2) % 4]
        self.sk = [s, (s + 3) % 4, (s + 1) % 4, (s + 2) % 4]
        self.f_next, self.f_prev = self.place(2, 0), self.place(1, 0)
        self.s_next, self.s_prev = self.place(0, 2), self.place(0, 1)
        self.partner = sp + 1 - 2 * core

    def place(self, k, m):
        return 2 * (self.fk[k] * self.fm + self.sk[m] * self.sm) + self.core

    def block(self, p, k, m, half=None):
        start = self.place(k, m) * ROWS
        return self.rows(p, start, half)

    def rows(self, p, start, half):
        if half is None:
            return self.refs[p].at[pl.ds(pl.multiple_of(start, ROWS), ROWS)]
        return self.refs[p].at[pl.ds(pl.multiple_of(start + half * 32, 32), 32)]

    def copy(self, p, sem, ref, dev):
        return pltpu.make_async_remote_copy(
            ref, ref, self.send_sem.at[p], self.recv_sem.at[p, sem],
            device_id={"sp": dev}, device_id_type=MESH)

    def send(self, p, sem, ref, dev):
        self.copy(p, sem, ref, dev).start()

    def arrive(self, p, sem, rows):
        self.copy(p, sem, self.refs[p].at[pl.ds(0, rows)], self.partner).wait_recv()

    def drain(self):
        for p in range(2):
            self.copy(p, 0, self.refs[p].at[pl.ds(0, 1984)], self.partner).wait_send()

    def hand(self, p, k, m):
        group = next(g for g in range(4) if (m, k) in CHIPS[g])
        self.send(p, GROUP_SEMS[group] if p == 1 else 11, self.block(p, k, m), self.partner)

    def handed_group(self, g):
        self.arrive(1, GROUP_SEMS[g], 4 * ROWS)

    def handed(self, p, sem, count):
        self.arrive(p, sem, count * ROWS)

    def own_along(self, p, turn, half):
        own = self.block(p, 0, 0, half)
        nexts, prevs = (self.f_next, self.s_next), (self.f_prev, self.s_prev)
        for side, (f_dev, s_dev) in enumerate((nexts, prevs)):
            f_sem = 0 if p == 1 or (half == 0 and side == 0) else 1
            self.send(p, f_sem + turn * (3 - f_sem), own, f_dev + turn * (s_dev - f_dev))

    def beyond_f(self, p):
        self.arrive(p, 0, 128)
        self.send(p, 2, self.block(p, 1, 0, 0), self.f_next)
        self.send(p, 2, self.block(p, 2, 0, 1), self.f_prev)

    def beyond_f_next(self):
        self.arrive(0, 0, 32)
        self.send(0, 2, self.block(0, 1, 0, 0), self.f_next)

    def beyond_f_prev(self):
        self.arrive(0, 1, 96)
        self.send(0, 2, self.block(0, 2, 0, 1), self.f_prev)

    def opposite_f(self, p):
        self.arrive(p, 2, 64)

    def beyond_s_own(self):
        self.beyond_s(0, 0)

    def along_s(self, p, k):
        if (p, k) == (1, 3):
            top, bottom = self.block(p, k, 0, 0), self.block(p, k, 0, 1)
            self.send(p, 6, top, self.s_next)
            self.send(p, 6, bottom, self.s_prev)
            self.send(p, 14, bottom, self.s_next)
            self.send(p, 14, top, self.s_prev)
        else:
            ref = self.block(p, k, 0)
            self.send(p, 3 + k, ref, self.s_next)
            self.send(p, 3 + k, ref, self.s_prev)
        self.hand(p, k, 0)

    def beyond_s(self, p, k):
        self.arrive(p, 3 + k, 64 if (p, k) == (1, 3) else 128)
        self.send(p, 7 + k, self.block(p, k, 1, 0), self.s_next)
        self.send(p, 7 + k, self.block(p, k, 2, 1), self.s_prev)
        if (p, k) == (1, 3):
            self.arrive(p, 14, 64)
        self.hand(p, k, 1)
        self.hand(p, k, 2)

    def opposite_s(self, p, k):
        self.arrive(p, 7 + k, 64)
        self.hand(p, k, 3)

    def columns(self, k, m):
        return pl.multiple_of((self.fk[k] * self.fm + self.sk[m] * self.sm) * 128, 128)


class Across:
    def __init__(self, x, send, recv):
        self.x, self.send_sem, self.recv_sem = x, send, recv
        self.next, self.prev, self.far = (x + 1) % 4, (x + 3) % 4, (x + 2) % 4

    def copy(self, phase, sem, src, dst, dev):
        return pltpu.make_async_remote_copy(
            src, dst, self.send_sem.at[phase], self.recv_sem.at[(0, 4, 12)[phase] + sem],
            device_id={"tp": dev}, device_id_type=MESH)

    def send(self, phase, sem, src, dst, dev):
        self.copy(phase, sem, src, dst, dev).start()

    def arrive(self, phase, sem, ref):
        self.copy(phase, sem, ref, ref, self.next).wait_recv()

    def drain(self, phase, ref):
        self.copy(phase, 0, ref, ref, self.next).wait_send()

    def rows(self, x, half=None):
        if half is None:
            return pl.ds(pl.multiple_of(x * ROWS, ROWS), ROWS)
        return pl.ds(pl.multiple_of(x * ROWS + half * 32, 32), 32)

    def start_relay(self, phase, g, part, relay):
        self.send(phase, g, part.at[g, 0, self.rows(self.far)], relay.at[g, 0], self.next)
        self.send(phase, g, part.at[g, 1, self.rows(self.far)], relay.at[g, 1], self.prev)

    def start_own(self, phase, g, part, landed):
        self.send(
            phase, part.shape[0] + g, part.at[g, 1, self.rows(self.next)], landed.at[g, 0, 1], self.next)
        self.send(
            phase, part.shape[0] + g, part.at[g, 0, self.rows(self.prev)], landed.at[g, 1, 0], self.prev)

    def pass_on(self, phase, g, part, relay, landed):
        self.arrive(phase, g, relay.at[g])
        for side, dev in ((0, self.next), (1, self.prev)):
            total = relay[g, side].astype(F32) + part[g, side, self.rows(dev)].astype(F32)
            relay[g, side] = total.astype(BF16)
            self.send(phase, part.shape[0] + g, relay.at[g, side], landed.at[g, side, side], dev)

    def total(self, phase, g, part, landed):
        self.arrive(phase, part.shape[0] + g, landed.at[g])
        return [
            part[g, sub, self.rows(self.x)].astype(F32)
            + landed[g, 0, sub].astype(F32)
            + landed[g, 1, sub].astype(F32)
            for sub in range(2)
        ]

    def share(self, ref):
        top, bottom = (ref.at[self.rows(self.x, half)] for half in range(2))
        self.send(2, 0, top, top, self.next)
        self.send(2, 1, bottom, bottom, self.prev)
        self.send(2, 2, bottom, bottom, self.next)
        self.send(2, 2, top, top, self.prev)

    def share_on(self, ref):
        top, bottom = ref.at[self.rows(self.prev, 0)], ref.at[self.rows(self.next, 1)]
        self.arrive(2, 0, top)
        self.send(2, 2, top, top, self.next)
        self.arrive(2, 1, bottom)
        self.send(2, 2, bottom, bottom, self.prev)

    def shared(self, ref):
        self.arrive(2, 2, ref.at[pl.ds(0, 128)])


QUARTER = D // 4
def layer_kernel(
    u_hbm, a_hbm, pr_hbm, pi_hbm, sl_hbm, bre_hbm, bim_hbm, cre_hbm, cim_hbm,
    mix_gain_hbm, pre_gain_hbm, post_gain_hbm, wo_hbm, res_hbm, gate_hbm, up_hbm, down_hbm,
    out_ref,
    u_ref, a_ref, poles_ref, sl_ref, maps_ref, gains_ref, wo_ref, res_ref,
    e_ref, dr_ref, di_ref, act_ref, read_ref, ea_ref, eb_ref, ra_ref, rb_ref, gu_ref, dn_ref,
    mix_part, out_part, mix_relay, out_relay, mix_landed, out_landed, rows_ref, hid_ref, sum_ref,
    cs, cq, ws, wq, xs, xq, ls,
):
    sp = lax.axis_index("sp")
    tp = lax.axis_index("tp")
    q = sp % 8
    z = sp // 8
    peers_a = [z * 8 + (q + d) % 8 for d in range(1, 8)]
    peers_b = [((z + d) % 4) * 8 + q for d in range(1, 4)]
    weights = Gather((gu_ref, dn_ref), ws, wq, sp)
    across = Across(tp, xs, xq)
    own = pl.ds(pl.multiple_of(sp * ROWS, ROWS), ROWS)
    for side, hbm in enumerate((gate_hbm, up_hbm)):
        pltpu.make_async_copy(hbm, gu_ref.at[own, pl.ds(side * F, F)], ls.at[0]).start()
    barrier = pltpu.get_barrier_semaphore()
    for peer in peers_a + peers_b:
        pl.semaphore_signal(barrier, inc=1, device_id={"sp": peer}, device_id_type=MESH)
    for peer in (across.next, across.prev):
        pl.semaphore_signal(barrier, inc=1, device_id={"tp": peer}, device_id_type=MESH)
    pairs = (
        (a_hbm, a_ref, 1), (pr_hbm, poles_ref.at[0], 2), (pi_hbm, poles_ref.at[1], 2),
        (sl_hbm, sl_ref, 3), (u_hbm, u_ref, 4),
        (bre_hbm, maps_ref.at[0], 5), (bim_hbm, maps_ref.at[1], 5),
        (cre_hbm, maps_ref.at[2], 5), (cim_hbm, maps_ref.at[3], 5),
        (wo_hbm, wo_ref, 6), (res_hbm, res_ref, 7), (mix_gain_hbm, gains_ref.at[0], 8),
        (pre_gain_hbm, gains_ref.at[1], 8), (post_gain_hbm, gains_ref.at[2], 8),
        (down_hbm, dn_ref.at[own], 9),
    )
    for src, dst, sem in pairs:
        pltpu.make_async_copy(src, dst, ls.at[sem]).start()

    def loaded(ref, sem):
        pltpu.make_async_copy(ref, ref, ls.at[sem]).wait()

    mine = iota((G, GN), 1) // N == iota((G, GN), 0)

    def row(v):
        return jnp.sum(jnp.where(mine, v, 0.0), axis=0, keepdims=True)

    loaded(a_ref, 1)
    put_row(ea_ref, 0, 0, jnp.exp(row(jnp.sum(a_ref[...], axis=1, keepdims=True))))
    loaded(gu_ref.at[own], 0)
    pl.semaphore_wait(barrier, 12)

    def to_all(ref, peers, sem):
        for d, peer in enumerate(peers, 1):
            pltpu.make_async_remote_copy(
                ref.at[0], ref.at[d], cs.at[sem], cq.at[sem],
                device_id={"sp": peer}, device_id_type=MESH).start()

    def from_all(ref, peers, sem):
        others = ref.at[pl.ds(1, len(peers))]
        pltpu.make_async_remote_copy(
            others, others, cs.at[sem], cq.at[sem],
            device_id={"sp": peers[0]}, device_id_type=MESH).wait()

    to_all(ea_ref, peers_a, 0)
    weights.own_along(0, weights.core, 0)
    weights.own_along(0, 1 - weights.core, 0)
    weights.own_along(0, 1 - weights.core, 1)
    weights.hand(0, 0, 0)
    loaded(poles_ref, 2)
    loaded(sl_ref, 3)

    base_r, base_i, ratio_r, ratio_i = step_rows(poles_ref[0], poles_ref[1], sl_ref[...], row)

    perm = iota((T, T), 0) == (iota((T, T), 1) % SEGS) * STEPS + iota((T, T), 1) // SEGS
    order = iota((T, T), 1) == (iota((T, T), 0) % SEGS) * STEPS + iota((T, T), 0) // SEGS
    e_small = dot(thirds(jnp.exp(a_ref[...])), one_hot(perm, BF16)).astype(BF16)
    groups = one_hot(mine, BF16)
    e_ref[...] = lax.dot_general(
        e_small, jnp.concatenate([groups] * 3, axis=0), (((0,), (0,)), ((), ())),
        preferred_element_type=F32)
    loaded(u_ref, 4)
    loaded(maps_ref, 5)
    u = dot(one_hot(order, BF16), u_ref[...]).astype(BF16)
    inside = iota((256, 1024), 0) // C == iota((256, 1024), 1) // N

    def spread(v):
        return jnp.where(inside, lanes_of(v, 1024), 0.0).astype(BF16)

    for h in range(2):
        gn = slice(h * 1024, (h + 1) * 1024)
        ch = slice(h * 256, (h + 1) * 256)
        raw_r = dot(u[:, ch], spread(maps_ref[0, ch, :]))
        raw_i = dot(u[:, ch], spread(maps_ref[1, ch, :]))
        rr, ri = ratio_r[:, gn], ratio_i[:, gn]
        dr_ref[:, gn] = rr * raw_r - ri * raw_i
        di_ref[:, gn] = rr * raw_i + ri * raw_r

    zero = jnp.zeros((SEGS, GN), F32)
    end_r, end_i, pe = scan_pass((base_r, base_i), e_ref, dr_ref, di_ref, (zero, zero), False)
    wr, wi = base_r, base_i
    for _ in range(5):
        wr, wi = cmul(wr, wi, wr, wi)
    seg_r, seg_i = wr * pe, wi * pe
    one_row = jnp.ones((1, GN), F32)
    no_row = jnp.zeros((1, GN), F32)
    total = (one_row, no_row, no_row, no_row)
    before = []
    for j in range(SEGS):
        before.append(total)
        total = link(total, (seg_r[j : j + 1], seg_i[j : j + 1], end_r[j : j + 1], end_i[j : j + 1]))
    put_row(ra_ref, 0, 0, total[2])
    put_row(ra_ref, 0, 1, total[3])

    to_all(ra_ref, peers_a, 1)
    weights.own_along(0, weights.core, 1)
    loaded(dn_ref.at[own], 9)
    weights.own_along(1, weights.core, None)
    weights.hand(1, 0, 0)
    for h in range(2):
        ch = slice(h * 256, (h + 1) * 256)
        read_ref[h, 0] = spread(maps_ref[2, ch, :])
        read_ref[h, 1] = spread(-maps_ref[3, ch, :])
    w_r, w_i = to_block(wr), to_block(wi)
    for _ in range(3):
        w_r, w_i = cmul(w_r, w_i, w_r, w_i)
    v_r, v_i = w_r, w_i
    for _ in range(3):
        v_r, v_i = cmul(v_r, v_i, v_r, v_i)
    from_all(ea_ref, peers_a, 0)
    eb = ea_ref[0]
    for d in range(1, 8):
        eb = eb * ea_ref[d]
    eb_ref[0] = eb
    to_all(eb_ref, peers_b, 2)
    from_all(ra_ref, peers_a, 1)
    unit = jnp.ones((16, 128), F32)
    null = jnp.zeros((16, 128), F32)

    def stretch(e, pr, pi, ref, slot):
        block = ref[slot].astype(F32)
        decay = e[slot]
        return pr * decay, pi * decay, block[:16], block[16:]

    run = (unit, null, null, null)
    pre_a = run
    for k in range(8):
        pre_a = choose(q == k, run, pre_a)
        run = link(run, stretch(ea_ref, w_r, w_i, ra_ref, (q - k + 8) % 8))
    rb_ref[0, :16] = run[2].astype(BF16)
    rb_ref[0, 16:] = run[3].astype(BF16)
    to_all(rb_ref, peers_b, 3)
    weights.own_along(1, 1 - weights.core, None)
    weights.beyond_f_next()
    weights.beyond_f_prev()
    weights.along_s(0, 1)
    weights.along_s(0, 2)
    from_all(eb_ref, peers_b, 2)
    from_all(rb_ref, peers_b, 3)
    run = (unit, null, null, null)
    pre_b = run
    for k in range(4):
        pre_b = choose(z == k, run, pre_b)
        run = link(run, stretch(eb_ref, v_r, v_i, rb_ref, (z - k + 4) % 4))
    carry = link(pre_b, pre_a)
    cr, ci = to_row(carry[2]), to_row(carry[3])
    starts = []
    for k in range(SEGS):
        pr, pi, sr, si = before[k]
        tr, ti = cmul(pr, pi, cr, ci)
        starts.append((tr + sr, ti + si))
    init = [jnp.concatenate([s[k] for s in starts], axis=0) for k in range(2)]
    scan_pass((base_r, base_i), e_ref, dr_ref, di_ref, init, True)

    for h in range(2):
        gn = slice(h * 1024, (h + 1) * 1024)
        y = dot_nt(dr_ref[:, gn].astype(BF16), read_ref[h, 0])
        y = y + dot_nt(di_ref[:, gn].astype(BF16), read_ref[h, 1])
        act_ref[:, h * 256 : (h + 1) * 256] = jax.nn.gelu(y).astype(BF16)
    act = dot(one_hot(perm, BF16), act_ref[...]).astype(BF16)
    loaded(wo_ref, 6)
    for g in range(2):
        out = dot(act, wo_ref[:, g * HALF : (g + 1) * HALF]).astype(BF16)
        mix_part[g, 0] = out[:, :QUARTER]
        mix_part[g, 1] = out[:, QUARTER:]
        across.start_relay(0, g, mix_part, mix_relay)
        across.start_own(0, g, mix_part, mix_landed)
    weights.beyond_s_own()
    across.pass_on(0, 0, mix_part, mix_relay, mix_landed)
    weights.opposite_f(0)
    weights.along_s(0, 3)
    across.pass_on(0, 1, mix_part, mix_relay, mix_landed)
    weights.beyond_s(0, 1)
    weights.beyond_f(1)
    mixed = jnp.concatenate(
        across.total(0, 0, mix_part, mix_landed)
        + across.total(0, 1, mix_part, mix_landed), axis=1)
    loaded(res_ref, 7)
    loaded(gains_ref, 8)
    middle = (res_ref[...].astype(F32) + rms_scale(mixed, gains_ref[0])).astype(BF16)
    res_ref[...] = middle
    normed = rms_scale(middle.astype(F32), gains_ref[1]).astype(BF16)
    rows_ref[across.rows(tp), :] = normed
    across.share(rows_ref)
    weights.beyond_s(0, 2)
    across.share_on(rows_ref)
    weights.beyond_s(0, 3)
    weights.along_s(1, 1)
    weights.along_s(1, 2)
    weights.opposite_f(1)
    weights.along_s(1, 3)
    weights.beyond_s(1, 0)
    across.shared(rows_ref)
    for k in range(4):
        weights.opposite_s(0, k)
    weights.handed(0, 11, 16)
    def hidden_tile(gate, up, first):
        hidden = gate / (1.0 + jnp.exp(-gate)) * up
        hid_ref[first : first + gate.shape[1], :] = hidden.T.astype(BF16)

    for first in range(0, F - 128, 256):
        tile = [gu_ref[:, side * F + first : side * F + first + 256] for side in range(2)]
        hidden_tile(dot(rows_ref[...], tile[0]), dot(rows_ref[...], tile[1]), first)
        if first in (0, 768):
            weights.beyond_s(1, 1 if first == 0 else 2)
    both = dot(rows_ref[...], jnp.concatenate([gu_ref[:, F - 128 : F], gu_ref[:, 2 * F - 128 :]], axis=1))
    hidden_tile(both[:, :128], both[:, 128:], F - 128)

    def down(g):
        weights.handed_group(g)
        block = jnp.concatenate(
            [dn_ref[pl.ds(weights.columns(k, m), 128), :] for k, m in CHIPS[g]], axis=0)
        out = dot(block, hid_ref[...])
        for i in range(4):
            out_part[g, i // 2, :, (i % 2) * 128 : (i % 2 + 1) * 128] = (
                out[i * 128 : (i + 1) * 128].T.astype(BF16))
        across.start_relay(1, g, out_part, out_relay)
        across.start_own(1, g, out_part, out_landed)

    down(0)
    weights.beyond_s(1, 3)
    down(1)
    weights.opposite_s(1, 0)
    weights.opposite_s(1, 1)
    down(2)
    weights.opposite_s(1, 2)
    weights.opposite_s(1, 3)
    across.pass_on(1, 0, out_part, out_relay, out_landed)
    down(3)
    across.pass_on(1, 1, out_part, out_relay, out_landed)
    across.pass_on(1, 2, out_part, out_relay, out_landed)
    across.pass_on(1, 3, out_part, out_relay, out_landed)
    for g, chips in enumerate(CHIPS):
        sums = across.total(1, g, out_part, out_landed)
        for j, (k, m) in enumerate(chips):
            piece = sums[j // 2][:, (j % 2) * 128 : (j % 2 + 1) * 128]
            sum_ref[:, pl.ds(weights.columns(k, m), 128)] = piece
    merged = res_ref[...].astype(F32) + 0.5 * rms_scale(sum_ref[...], gains_ref[2])
    out_ref[...] = merged.astype(BF16)
    weights.drain()
    across.drain(0, mix_part.at[:, :, pl.ds(0, 192)])
    across.drain(1, out_part.at[:, :, pl.ds(0, 192)])
    across.drain(2, rows_ref.at[pl.ds(0, 192)])


def layer(arrays):
    hbm = pl.BlockSpec(memory_space=pl.ANY)
    dma = pltpu.SemaphoreType.DMA
    return pl.pallas_call(
        layer_kernel,
        out_shape=pltpu.VMEM((ROWS, D), BF16),
        in_specs=[hbm] * len(arrays),
        out_specs=pl.BlockSpec(memory_space=pltpu.VMEM),
        scratch_shapes=[
            pltpu.VMEM((T, 512), BF16),
            pltpu.VMEM((G, T), F32),
            pltpu.VMEM((2, G, N), F32),
            pltpu.VMEM((1, G), F32),
            pltpu.VMEM((4, 512, N), F32),
            pltpu.VMEM((3, 1, D), F32),
            pltpu.VMEM((512, D), BF16),
            pltpu.VMEM((ROWS, D), BF16),
            pltpu.VMEM((T, GN), F32),
            pltpu.VMEM((T, GN), F32),
            pltpu.VMEM((T, GN), F32),
            pltpu.VMEM((T, 512), BF16),
            pltpu.VMEM((2, 2, 256, 1024), BF16),
            pltpu.VMEM((8, 16, 128), F32),
            pltpu.VMEM((4, 16, 128), F32),
            pltpu.VMEM((8, 32, 128), BF16),
            pltpu.VMEM((4, 32, 128), BF16),
            pltpu.VMEM((D, 2 * F), BF16),
            pltpu.VMEM((D, F), BF16),
            pltpu.VMEM((2, 2, T, QUARTER), BF16),
            pltpu.VMEM((4, 2, T, QUARTER // 2), BF16),
            pltpu.VMEM((2, 2, ROWS, QUARTER), BF16),
            pltpu.VMEM((4, 2, ROWS, QUARTER // 2), BF16),
            pltpu.VMEM((2, 2, 2, ROWS, QUARTER), BF16),
            pltpu.VMEM((4, 2, 2, ROWS, QUARTER // 2), BF16),
            pltpu.VMEM((T, D), BF16),
            pltpu.VMEM((F, T), BF16),
            pltpu.VMEM((ROWS, D), F32),
            dma((4,)), dma((4,)), dma((2,)), dma((2, 15)), dma((3,)), dma((15,)), dma((10,)),
        ],
        compiler_params=pltpu.CompilerParams(
            collective_id=0, has_side_effects=True, vmem_limit_bytes=60000000
        ),
        name="layer",
    )(*arrays)


def shards(
    residual, ssm_input, pole_real, pole_imaginary, step_log, input_real, entry_map_quadrature,
    output_real, output_imaginary, added_log_decay, out_weight, mix_gain, gate_weight, up_weight,
    down_weight, pre_gain, post_gain,
):
    small = (
        ssm_input, added_log_decay.T, pole_real, pole_imaginary, step_log.reshape(1, G),
        input_real.transpose(0, 2, 1).reshape(512, N),
        entry_map_quadrature.transpose(0, 2, 1).reshape(512, N),
        output_real.reshape(512, N), output_imaginary.reshape(512, N),
        mix_gain.reshape(1, D), pre_gain.reshape(1, D), post_gain.reshape(1, D),
    )
    return layer(small + (out_weight, residual, gate_weight, up_weight, down_weight))


def solution(mesh):
    return jax.shard_map(
        shards,
        mesh=mesh,
        in_specs=(
            P(("sp", "tp"), None), P("sp", "tp"), P("tp", None), P("tp", None), P("tp"),
            P("tp", None, None), P("tp", None, None), P("tp", None, None), P("tp", None, None),
            P("sp", "tp"), P("tp", None), P(), P("sp", "tp"), P("sp", "tp"), P("sp", "tp"),
            P(), P(),
        ),
        out_specs=P(("sp", "tp"), None),
        check_vma=False,
    )
```

```python
import functools

import jax
import jax.numpy as jnp
from jax import lax
from jax.experimental import pallas as pl
from jax.experimental.pallas import tpu as pltpu
from jax.sharding import PartitionSpec as P

EPSILON = 1e-06
EXACT = lax.Precision.HIGHEST
MESH = pl.DeviceIdType.MESH
F32 = jnp.float32
BF16 = jnp.bfloat16
T = 256
G = 32
N = 64
C = 16
GN = G * N
SEGS = 8
STEPS = T // SEGS
D = 2048
F = 1408
ROWS = 64
HALF = D // 2
TILES = F // 128


def dot(a, b, **kw):
    return jnp.dot(a, b, preferred_element_type=F32, **kw)


def dot_nt(a, b):
    return lax.dot_general(a, b, (((1,), (1,)), ((), ())), preferred_element_type=F32)


def iota(shape, dim):
    return lax.broadcasted_iota(jnp.int32, shape, dim)


def one_hot(mask, dtype):
    return jnp.where(mask, 1.0, 0.0).astype(dtype)


def cmul(ar, ai, br, bi):
    return ar * br - ai * bi, ar * bi + ai * br


def split(v):
    hi = v.astype(BF16)
    return hi, (v - hi.astype(F32)).astype(BF16)


def expm1(x):
    p = 1.0 / 40320.0
    for k in (5040.0, 720.0, 120.0, 24.0, 6.0, 2.0, 1.0):
        p = p * x + 1.0 / k
    return jnp.where(x > -0.5, p * x, jnp.exp(x) - 1.0)


def lanes_of(v, count):
    pair = jnp.concatenate([v, v], axis=1)
    return jnp.concatenate([pair] * (count // 128), axis=1)


def step_rows(pr, pi, sl, row):
    same = iota((G, G), 0) == iota((G, G), 1)
    column = jnp.sum(jnp.where(same, jnp.broadcast_to(sl, (G, G)), 0.0), axis=1, keepdims=True)
    pr, pi, step = row(lanes_of(pr, GN)), row(lanes_of(pi, GN)), jnp.exp(row(column))
    log_size = pr * step
    angle = pi * step
    cosine, sine = jnp.cos(angle), jnp.sin(angle)
    size = jnp.exp(log_size)
    half = jnp.sin(0.5 * angle)
    lift_r = expm1(log_size) * cosine - 2.0 * half * half
    lift_i = size * sine
    inv = 1.0 / (pr * pr + pi * pi)
    ratio_r = (lift_r * pr + lift_i * pi) * inv
    ratio_i = (lift_i * pr - lift_r * pi) * inv
    return size * cosine, size * sine, ratio_r, ratio_i


def thirds(v):
    hi = v.astype(BF16)
    rest = v - hi.astype(F32)
    mid = rest.astype(BF16)
    return jnp.concatenate([hi, mid, (rest - mid.astype(F32)).astype(BF16)], axis=0)


def scan_pass(base, e_ref, dr_ref, di_ref, init, store):
    ends = []
    width = GN // 4
    for lc in range(4):
        sl = slice(lc * width, (lc + 1) * width)
        br = jnp.broadcast_to(base[0][:, sl], (SEGS, width))
        bi = jnp.broadcast_to(base[1][:, sl], (SEGS, width))

        def body(i, st):
            sr, si, pe = st
            rows = pl.ds(pl.multiple_of(i * SEGS, SEGS), SEGS)
            e = e_ref[rows, sl]
            ar, ai = br * e, bi * e
            nr = ar * sr - ai * si + dr_ref[rows, sl]
            ni = ar * si + ai * sr + di_ref[rows, sl]
            if store:
                dr_ref[rows, sl] = nr
                di_ref[rows, sl] = ni
                return nr, ni, pe
            return nr, ni, pe * e

        st = (init[0][:, sl], init[1][:, sl], jnp.ones((SEGS, width), F32))
        ends.append(lax.fori_loop(0, STEPS, body, st, unroll=4))
    return [jnp.concatenate([p[k] for p in ends], axis=1) for k in range(3)]


def put_row(ref, slot, part, row):
    for k in range(16):
        ref[slot, part * 16 + k : part * 16 + k + 1, :] = row[:, k * 128 : (k + 1) * 128].astype(ref.dtype)


def to_block(row):
    return jnp.concatenate([row[:, k * 128 : (k + 1) * 128] for k in range(16)], axis=0)


def to_row(block):
    return jnp.concatenate([block[k : k + 1, :] for k in range(16)], axis=1)


def link(first, then):
    ar, ai, sr, si = first
    br, bi, tr, ti = then
    pr, pi = cmul(br, bi, ar, ai)
    ur, ui = cmul(br, bi, sr, si)
    return pr, pi, ur + tr, ui + ti


def choose(cond, a, b):
    return tuple(jnp.where(cond, x, y) for x, y in zip(a, b))


def rms_scale(values, gain):
    return values * lax.rsqrt(jnp.mean(values * values, axis=-1, keepdims=True) + EPSILON) * gain


CHIPS = (
    ((0, 0), (0, 1), (1, 0), (0, 2)),
    ((2, 0), (1, 1), (1, 2), (2, 1)),
    ((2, 2), (3, 0), (0, 3), (1, 3)),
    ((3, 1), (2, 3), (3, 2), (3, 3)),
)
GROUP_SEMS = (11, 1, 12, 13)


class Gather:
    def __init__(self, refs, send, recv, sp):
        self.refs, self.send_sem, self.recv_sem = refs, send, recv
        core, y, z = sp % 2, (sp // 2) % 4, sp // 8
        self.core = core
        self.fm, self.sm = 1 + 3 * core, 4 - 3 * core
        f = y + core * (z - y)
        s = z + core * (y - z)
        self.fk = [f, (f + 3) % 4, (f + 1) % 4, (f + 2) % 4]
        self.sk = [s, (s + 3) % 4, (s + 1) % 4, (s + 2) % 4]
        self.f_next, self.f_prev = self.place(2, 0), self.place(1, 0)
        self.s_next, self.s_prev = self.place(0, 2), self.place(0, 1)
        self.partner = sp + 1 - 2 * core

    def place(self, k, m):
        return 2 * (self.fk[k] * self.fm + self.sk[m] * self.sm) + self.core

    def block(self, p, k, m, half=None):
        start = self.place(k, m) * ROWS
        return self.rows(p, start, half)

    def rows(self, p, start, half):
        if half is None:
            return self.refs[p].at[pl.ds(pl.multiple_of(start, ROWS), ROWS)]
        return self.refs[p].at[pl.ds(pl.multiple_of(start + half * 32, 32), 32)]

    def copy(self, p, sem, ref, dev):
        return pltpu.make_async_remote_copy(
            ref, ref, self.send_sem.at[p], self.recv_sem.at[p, sem],
            device_id={"sp": dev}, device_id_type=MESH)

    def send(self, p, sem, ref, dev):
        self.copy(p, sem, ref, dev).start()

    def arrive(self, p, sem, rows):
        self.copy(p, sem, self.refs[p].at[pl.ds(0, rows)], self.partner).wait_recv()

    def drain(self):
        for p in range(2):
            self.copy(p, 0, self.refs[p].at[pl.ds(0, 1984)], self.partner).wait_send()

    def hand(self, p, k, m):
        group = next(g for g in range(4) if (m, k) in CHIPS[g])
        self.send(p, GROUP_SEMS[group] if p == 1 else 11, self.block(p, k, m), self.partner)

    def handed_group(self, g):
        self.arrive(1, GROUP_SEMS[g], 4 * ROWS)

    def handed(self, p, sem, count):
        self.arrive(p, sem, count * ROWS)

    def own_along(self, p, turn, half):
        own = self.block(p, 0, 0, half)
        nexts, prevs = (self.f_next, self.s_next), (self.f_prev, self.s_prev)
        for side, (f_dev, s_dev) in enumerate((nexts, prevs)):
            f_sem = 0 if p == 1 or (half == 0 and side == 0) else 1
            self.send(p, f_sem + turn * (3 - f_sem), own, f_dev + turn * (s_dev - f_dev))

    def beyond_f(self, p):
        self.arrive(p, 0, 128)
        self.send(p, 2, self.block(p, 1, 0, 0), self.f_next)
        self.send(p, 2, self.block(p, 2, 0, 1), self.f_prev)

    def beyond_f_next(self):
        self.arrive(0, 0, 32)
        self.send(0, 2, self.block(0, 1, 0, 0), self.f_next)

    def beyond_f_prev(self):
        self.arrive(0, 1, 96)
        self.send(0, 2, self.block(0, 2, 0, 1), self.f_prev)

    def opposite_f(self, p):
        self.arrive(p, 2, 64)

    def beyond_s_own(self):
        self.beyond_s(0, 0)

    def along_s(self, p, k):
        ref = self.block(p, k, 0)
        self.send(p, 3 + k, ref, self.s_next)
        self.send(p, 3 + k, ref, self.s_prev)
        self.hand(p, k, 0)

    def beyond_s(self, p, k):
        self.arrive(p, 3 + k, 128)
        self.send(p, 7 + k, self.block(p, k, 1, 0), self.s_next)
        self.send(p, 7 + k, self.block(p, k, 2, 1), self.s_prev)
        self.hand(p, k, 1)
        self.hand(p, k, 2)

    def opposite_s(self, p, k):
        self.arrive(p, 7 + k, 64)
        self.hand(p, k, 3)

    def columns(self, k, m):
        return pl.multiple_of((self.fk[k] * self.fm + self.sk[m] * self.sm) * 128, 128)


class Across:
    def __init__(self, x, send, recv):
        self.x, self.send_sem, self.recv_sem = x, send, recv
        self.next, self.prev, self.far = (x + 1) % 4, (x + 3) % 4, (x + 2) % 4

    def copy(self, phase, sem, src, dst, dev):
        return pltpu.make_async_remote_copy(
            src, dst, self.send_sem.at[phase], self.recv_sem.at[(0, 4, 12)[phase] + sem],
            device_id={"tp": dev}, device_id_type=MESH)

    def send(self, phase, sem, src, dst, dev):
        self.copy(phase, sem, src, dst, dev).start()

    def arrive(self, phase, sem, ref):
        self.copy(phase, sem, ref, ref, self.next).wait_recv()

    def drain(self, phase, ref):
        self.copy(phase, 0, ref, ref, self.next).wait_send()

    def rows(self, x, half=None):
        if half is None:
            return pl.ds(pl.multiple_of(x * ROWS, ROWS), ROWS)
        return pl.ds(pl.multiple_of(x * ROWS + half * 32, 32), 32)

    def start_relay(self, phase, g, side, part, relay):
        dev = (self.next, self.prev)[side]
        self.send(phase, g, part.at[g, side, self.rows(self.far)], relay.at[g, side], dev)

    def start_own(self, phase, g, part, landed):
        self.send(
            phase, part.shape[0] + g, part.at[g, 1, self.rows(self.next)], landed.at[g, 0, 1], self.next)
        self.send(
            phase, part.shape[0] + g, part.at[g, 0, self.rows(self.prev)], landed.at[g, 1, 0], self.prev)

    def pass_on(self, phase, g, part, relay, landed):
        self.arrive(phase, g, relay.at[g])
        for side, dev in ((0, self.next), (1, self.prev)):
            total = relay[g, side].astype(F32) + part[g, side, self.rows(dev)].astype(F32)
            relay[g, side] = total.astype(BF16)
            self.send(phase, part.shape[0] + g, relay.at[g, side], landed.at[g, side, side], dev)

    def total(self, phase, g, part, landed):
        self.arrive(phase, part.shape[0] + g, landed.at[g])
        return [
            part[g, sub, self.rows(self.x)].astype(F32)
            + landed[g, 0, sub].astype(F32)
            + landed[g, 1, sub].astype(F32)
            for sub in range(2)
        ]

    def share(self, ref):
        top, bottom = (ref.at[self.rows(self.x, half)] for half in range(2))
        self.send(2, 0, top, top, self.next)
        self.send(2, 1, bottom, bottom, self.prev)
        self.send(2, 2, bottom, bottom, self.next)
        self.send(2, 2, top, top, self.prev)

    def share_on(self, ref):
        top, bottom = ref.at[self.rows(self.prev, 0)], ref.at[self.rows(self.next, 1)]
        self.arrive(2, 0, top)
        self.send(2, 2, top, top, self.next)
        self.arrive(2, 1, bottom)
        self.send(2, 2, bottom, bottom, self.prev)

    def shared(self, ref):
        self.arrive(2, 2, ref.at[pl.ds(0, 128)])


QUARTER = D // 4
def layer_kernel(
    u_hbm, a_hbm, pr_hbm, pi_hbm, sl_hbm, bre_hbm, bim_hbm, cre_hbm, cim_hbm,
    mix_gain_hbm, pre_gain_hbm, post_gain_hbm, wo_hbm, res_hbm, gate_hbm, up_hbm, down_hbm,
    out_ref,
    u_ref, a_ref, poles_ref, sl_ref, maps_ref, gains_ref, wo_ref, res_ref,
    e_ref, dr_ref, di_ref, act_ref, read_ref, ea_ref, eb_ref, ra_ref, rb_ref, gu_ref, dn_ref,
    mix_part, out_part, mix_relay, out_relay, mix_landed, out_landed, rows_ref, hid_ref, sum_ref,
    cs, cq, ws, wq, xs, xq, ls,
):
    sp = lax.axis_index("sp")
    tp = lax.axis_index("tp")
    q = sp % 8
    z = sp // 8
    peers_a = [z * 8 + (q + d) % 8 for d in range(1, 8)]
    peers_b = [((z + d) % 4) * 8 + q for d in range(1, 4)]
    weights = Gather((gu_ref, dn_ref), ws, wq, sp)
    across = Across(tp, xs, xq)
    own = pl.ds(pl.multiple_of(sp * ROWS, ROWS), ROWS)
    for side, hbm in enumerate((gate_hbm, up_hbm)):
        pltpu.make_async_copy(hbm, gu_ref.at[own, pl.ds(side * F, F)], ls.at[0]).start()
    barrier = pltpu.get_barrier_semaphore()
    for peer in peers_a + peers_b:
        pl.semaphore_signal(barrier, inc=1, device_id={"sp": peer}, device_id_type=MESH)
    for peer in (across.next, across.prev):
        pl.semaphore_signal(barrier, inc=1, device_id={"tp": peer}, device_id_type=MESH)
    pairs = (
        (a_hbm, a_ref, 1), (pr_hbm, poles_ref.at[0], 2), (pi_hbm, poles_ref.at[1], 2),
        (sl_hbm, sl_ref, 3), (u_hbm, u_ref, 4),
        (bre_hbm, maps_ref.at[0], 5), (bim_hbm, maps_ref.at[1], 5),
        (cre_hbm, maps_ref.at[2], 5), (cim_hbm, maps_ref.at[3], 5),
        (wo_hbm, wo_ref, 6), (res_hbm, res_ref, 7), (mix_gain_hbm, gains_ref.at[0], 8),
        (pre_gain_hbm, gains_ref.at[1], 8), (post_gain_hbm, gains_ref.at[2], 8),
        (down_hbm, dn_ref.at[own], 9),
    )
    for src, dst, sem in pairs:
        pltpu.make_async_copy(src, dst, ls.at[sem]).start()

    def loaded(ref, sem):
        pltpu.make_async_copy(ref, ref, ls.at[sem]).wait()

    mine = iota((G, GN), 1) // N == iota((G, GN), 0)

    def row(v):
        return jnp.sum(jnp.where(mine, v, 0.0), axis=0, keepdims=True)

    loaded(a_ref, 1)
    put_row(ea_ref, 0, 0, jnp.exp(row(jnp.sum(a_ref[...], axis=1, keepdims=True))))
    loaded(gu_ref.at[own], 0)
    pl.semaphore_wait(barrier, 12)

    def to_all(ref, peers, sem):
        for d, peer in enumerate(peers, 1):
            pltpu.make_async_remote_copy(
                ref.at[0], ref.at[d], cs.at[sem], cq.at[sem],
                device_id={"sp": peer}, device_id_type=MESH).start()

    def from_all(ref, peers, sem):
        others = ref.at[pl.ds(1, len(peers))]
        pltpu.make_async_remote_copy(
            others, others, cs.at[sem], cq.at[sem],
            device_id={"sp": peers[0]}, device_id_type=MESH).wait()

    to_all(ea_ref, peers_a, 0)
    weights.own_along(0, weights.core, 0)
    weights.own_along(0, 1 - weights.core, 0)
    weights.own_along(0, 1 - weights.core, 1)
    weights.hand(0, 0, 0)
    loaded(poles_ref, 2)
    loaded(sl_ref, 3)

    base_r, base_i, ratio_r, ratio_i = step_rows(poles_ref[0], poles_ref[1], sl_ref[...], row)

    perm = iota((T, T), 0) == (iota((T, T), 1) % SEGS) * STEPS + iota((T, T), 1) // SEGS
    order = iota((T, T), 1) == (iota((T, T), 0) % SEGS) * STEPS + iota((T, T), 0) // SEGS
    e_small = dot(thirds(jnp.exp(a_ref[...])), one_hot(perm, BF16)).astype(BF16)
    groups = one_hot(mine, BF16)
    e_ref[...] = lax.dot_general(
        e_small, jnp.concatenate([groups] * 3, axis=0), (((0,), (0,)), ((), ())),
        preferred_element_type=F32)
    loaded(u_ref, 4)
    loaded(maps_ref, 5)
    u = dot(one_hot(order, BF16), u_ref[...]).astype(BF16)
    inside = iota((256, 1024), 0) // C == iota((256, 1024), 1) // N

    def spread(v):
        return jnp.where(inside, lanes_of(v, 1024), 0.0).astype(BF16)

    for h in range(2):
        gn = slice(h * 1024, (h + 1) * 1024)
        ch = slice(h * 256, (h + 1) * 256)
        raw_r = dot(u[:, ch], spread(maps_ref[0, ch, :]))
        raw_i = dot(u[:, ch], spread(maps_ref[1, ch, :]))
        rr, ri = ratio_r[:, gn], ratio_i[:, gn]
        dr_ref[:, gn] = rr * raw_r - ri * raw_i
        di_ref[:, gn] = rr * raw_i + ri * raw_r

    zero = jnp.zeros((SEGS, GN), F32)
    end_r, end_i, pe = scan_pass((base_r, base_i), e_ref, dr_ref, di_ref, (zero, zero), False)
    wr, wi = base_r, base_i
    for _ in range(5):
        wr, wi = cmul(wr, wi, wr, wi)
    seg_r, seg_i = wr * pe, wi * pe
    one_row = jnp.ones((1, GN), F32)
    no_row = jnp.zeros((1, GN), F32)
    total = (one_row, no_row, no_row, no_row)
    before = []
    for j in range(SEGS):
        before.append(total)
        total = link(total, (seg_r[j : j + 1], seg_i[j : j + 1], end_r[j : j + 1], end_i[j : j + 1]))
    put_row(ra_ref, 0, 0, total[2])
    put_row(ra_ref, 0, 1, total[3])

    to_all(ra_ref, peers_a, 1)
    weights.own_along(0, weights.core, 1)
    loaded(dn_ref.at[own], 9)
    weights.own_along(1, weights.core, None)
    weights.hand(1, 0, 0)
    for h in range(2):
        ch = slice(h * 256, (h + 1) * 256)
        read_ref[h, 0] = spread(maps_ref[2, ch, :])
        read_ref[h, 1] = spread(-maps_ref[3, ch, :])
    w_r, w_i = to_block(wr), to_block(wi)
    for _ in range(3):
        w_r, w_i = cmul(w_r, w_i, w_r, w_i)
    v_r, v_i = w_r, w_i
    for _ in range(3):
        v_r, v_i = cmul(v_r, v_i, v_r, v_i)
    from_all(ea_ref, peers_a, 0)
    eb = ea_ref[0]
    for d in range(1, 8):
        eb = eb * ea_ref[d]
    eb_ref[0] = eb
    to_all(eb_ref, peers_b, 2)
    from_all(ra_ref, peers_a, 1)
    unit = jnp.ones((16, 128), F32)
    null = jnp.zeros((16, 128), F32)

    def stretch(e, pr, pi, ref, slot):
        block = ref[slot].astype(F32)
        decay = e[slot]
        return pr * decay, pi * decay, block[:16], block[16:]

    run = (unit, null, null, null)
    pre_a = run
    for k in range(8):
        pre_a = choose(q == k, run, pre_a)
        run = link(run, stretch(ea_ref, w_r, w_i, ra_ref, (q - k + 8) % 8))
    rb_ref[0, :16] = run[2].astype(BF16)
    rb_ref[0, 16:] = run[3].astype(BF16)
    to_all(rb_ref, peers_b, 3)
    weights.own_along(1, 1 - weights.core, None)
    weights.beyond_f_next()
    weights.beyond_f_prev()
    weights.along_s(0, 1)
    weights.along_s(0, 2)
    from_all(eb_ref, peers_b, 2)
    from_all(rb_ref, peers_b, 3)
    run = (unit, null, null, null)
    pre_b = run
    for k in range(4):
        pre_b = choose(z == k, run, pre_b)
        run = link(run, stretch(eb_ref, v_r, v_i, rb_ref, (z - k + 4) % 4))
    carry = link(pre_b, pre_a)
    cr, ci = to_row(carry[2]), to_row(carry[3])
    starts = []
    for k in range(SEGS):
        pr, pi, sr, si = before[k]
        tr, ti = cmul(pr, pi, cr, ci)
        starts.append((tr + sr, ti + si))
    init = [jnp.concatenate([s[k] for s in starts], axis=0) for k in range(2)]
    scan_pass((base_r, base_i), e_ref, dr_ref, di_ref, init, True)

    for h in range(2):
        gn = slice(h * 1024, (h + 1) * 1024)
        y = dot_nt(dr_ref[:, gn].astype(BF16), read_ref[h, 0])
        y = y + dot_nt(di_ref[:, gn].astype(BF16), read_ref[h, 1])
        act_ref[:, h * 256 : (h + 1) * 256] = jax.nn.gelu(y).astype(BF16)
    act = dot(one_hot(perm, BF16), act_ref[...]).astype(BF16)
    loaded(wo_ref, 6)
    for g in range(2):
        out = dot(act, wo_ref[:, g * HALF : (g + 1) * HALF]).astype(BF16)
        mix_part[g, 0] = out[:, :QUARTER]
        mix_part[g, 1] = out[:, QUARTER:]
        for side in range(2):
            across.start_relay(0, g, side, mix_part, mix_relay)
        across.start_own(0, g, mix_part, mix_landed)
    weights.beyond_s_own()
    across.pass_on(0, 0, mix_part, mix_relay, mix_landed)
    weights.opposite_f(0)
    weights.along_s(0, 3)
    across.pass_on(0, 1, mix_part, mix_relay, mix_landed)
    weights.beyond_s(0, 1)
    weights.beyond_f(1)
    mixed = jnp.concatenate(
        across.total(0, 0, mix_part, mix_landed)
        + across.total(0, 1, mix_part, mix_landed), axis=1)
    loaded(res_ref, 7)
    loaded(gains_ref, 8)
    middle = (res_ref[...].astype(F32) + rms_scale(mixed, gains_ref[0])).astype(BF16)
    res_ref[...] = middle
    normed = rms_scale(middle.astype(F32), gains_ref[1]).astype(BF16)
    rows_ref[across.rows(tp), :] = normed
    across.share(rows_ref)
    weights.beyond_s(0, 2)
    across.share_on(rows_ref)
    weights.beyond_s(0, 3)
    weights.along_s(1, 1)
    weights.along_s(1, 2)
    weights.opposite_f(1)
    weights.along_s(1, 3)
    weights.beyond_s(1, 0)
    across.shared(rows_ref)
    for k in range(4):
        weights.opposite_s(0, k)
    weights.handed(0, 11, 16)
    def hidden_tile(gate, up, first):
        hidden = gate / (1.0 + jnp.exp(-gate)) * up
        hid_ref[first : first + gate.shape[1], :] = hidden.T.astype(BF16)

    for first in range(0, F - 128, 256):
        tile = [gu_ref[:, side * F + first : side * F + first + 256] for side in range(2)]
        hidden_tile(dot(rows_ref[...], tile[0]), dot(rows_ref[...], tile[1]), first)
        if first in (256, 1024):
            weights.beyond_s(1, 1 if first == 256 else 2)
    both = dot(rows_ref[...], jnp.concatenate([gu_ref[:, F - 128 : F], gu_ref[:, 2 * F - 128 :]], axis=1))
    hidden_tile(both[:, :128], both[:, 128:], F - 128)

    def down(g):
        weights.handed_group(g)
        size = 2 if g == 3 else 4
        for start in range(0, 4, size):
            block = jnp.concatenate(
                [dn_ref[pl.ds(weights.columns(k, m), 128), :]
                 for k, m in CHIPS[g][start : start + size]], axis=0)
            out = dot(block, hid_ref[...])
            for i in range(start, start + size):
                out_part[g, i // 2, :, (i % 2) * 128 : (i % 2 + 1) * 128] = (
                    out[(i - start) * 128 : (i - start + 1) * 128].T.astype(BF16))
            for side in range(start // 2, (start + size) // 2):
                across.start_relay(1, g, side, out_part, out_relay)
        across.start_own(1, g, out_part, out_landed)

    down(0)
    weights.beyond_s(1, 3)
    down(1)
    weights.opposite_s(1, 0)
    weights.opposite_s(1, 1)
    down(2)
    weights.opposite_s(1, 2)
    weights.opposite_s(1, 3)
    across.pass_on(1, 0, out_part, out_relay, out_landed)
    down(3)
    across.pass_on(1, 1, out_part, out_relay, out_landed)
    across.pass_on(1, 2, out_part, out_relay, out_landed)
    across.pass_on(1, 3, out_part, out_relay, out_landed)
    for g, chips in enumerate(CHIPS):
        sums = across.total(1, g, out_part, out_landed)
        for j, (k, m) in enumerate(chips):
            piece = sums[j // 2][:, (j % 2) * 128 : (j % 2 + 1) * 128]
            sum_ref[:, pl.ds(weights.columns(k, m), 128)] = piece
    merged = res_ref[...].astype(F32) + 0.5 * rms_scale(sum_ref[...], gains_ref[2])
    out_ref[...] = merged.astype(BF16)
    weights.drain()
    across.drain(0, mix_part.at[:, :, pl.ds(0, 192)])
    across.drain(1, out_part.at[:, :, pl.ds(0, 192)])
    across.drain(2, rows_ref.at[pl.ds(0, 192)])


def layer(arrays):
    hbm = pl.BlockSpec(memory_space=pl.ANY)
    dma = pltpu.SemaphoreType.DMA
    return pl.pallas_call(
        layer_kernel,
        out_shape=pltpu.VMEM((ROWS, D), BF16),
        in_specs=[hbm] * len(arrays),
        out_specs=pl.BlockSpec(memory_space=pltpu.VMEM),
        scratch_shapes=[
            pltpu.VMEM((T, 512), BF16),
            pltpu.VMEM((G, T), F32),
            pltpu.VMEM((2, G, N), F32),
            pltpu.VMEM((1, G), F32),
            pltpu.VMEM((4, 512, N), F32),
            pltpu.VMEM((3, 1, D), F32),
            pltpu.VMEM((512, D), BF16),
            pltpu.VMEM((ROWS, D), BF16),
            pltpu.VMEM((T, GN), F32),
            pltpu.VMEM((T, GN), F32),
            pltpu.VMEM((T, GN), F32),
            pltpu.VMEM((T, 512), BF16),
            pltpu.VMEM((2, 2, 256, 1024), BF16),
            pltpu.VMEM((8, 16, 128), F32),
            pltpu.VMEM((4, 16, 128), F32),
            pltpu.VMEM((8, 32, 128), BF16),
            pltpu.VMEM((4, 32, 128), BF16),
            pltpu.VMEM((D, 2 * F), BF16),
            pltpu.VMEM((D, F), BF16),
            pltpu.VMEM((2, 2, T, QUARTER), BF16),
            pltpu.VMEM((4, 2, T, QUARTER // 2), BF16),
            pltpu.VMEM((2, 2, ROWS, QUARTER), BF16),
            pltpu.VMEM((4, 2, ROWS, QUARTER // 2), BF16),
            pltpu.VMEM((2, 2, 2, ROWS, QUARTER), BF16),
            pltpu.VMEM((4, 2, 2, ROWS, QUARTER // 2), BF16),
            pltpu.VMEM((T, D), BF16),
            pltpu.VMEM((F, T), BF16),
            pltpu.VMEM((ROWS, D), F32),
            dma((4,)), dma((4,)), dma((2,)), dma((2, 14)), dma((3,)), dma((15,)), dma((10,)),
        ],
        compiler_params=pltpu.CompilerParams(
            collective_id=0, has_side_effects=True, vmem_limit_bytes=60000000
        ),
        name="layer",
    )(*arrays)


def shards(
    residual, ssm_input, pole_real, pole_imaginary, step_log, input_real, entry_map_quadrature,
    output_real, output_imaginary, added_log_decay, out_weight, mix_gain, gate_weight, up_weight,
    down_weight, pre_gain, post_gain,
):
    small = (
        ssm_input, added_log_decay.T, pole_real, pole_imaginary, step_log.reshape(1, G),
        input_real.transpose(0, 2, 1).reshape(512, N),
        entry_map_quadrature.transpose(0, 2, 1).reshape(512, N),
        output_real.reshape(512, N), output_imaginary.reshape(512, N),
        mix_gain.reshape(1, D), pre_gain.reshape(1, D), post_gain.reshape(1, D),
    )
    return layer(small + (out_weight, residual, gate_weight, up_weight, down_weight))


def solution(mesh):
    return jax.shard_map(
        shards,
        mesh=mesh,
        in_specs=(
            P(("sp", "tp"), None), P("sp", "tp"), P("tp", None), P("tp", None), P("tp"),
            P("tp", None, None), P("tp", None, None), P("tp", None, None), P("tp", None, None),
            P("sp", "tp"), P("tp", None), P(), P("sp", "tp"), P("sp", "tp"), P("sp", "tp"),
            P(), P(),
        ),
        out_specs=P(("sp", "tp"), None),
        check_vma=False,
    )
```
